128 devices in a mesh: sp: 32 (over z, y, core), tp: 4 (over x).
Axes of the slice: x: 4, y: 4, z: 4, core: 2. Of those that a mesh axis runs over, the one named last changes fastest.
Arguments:
- d_out: bfloat16 [16384, 2048], P('sp'), may hold values from -6 to 6
- route_expert: int32 [16384, 2], P('sp'), may hold values from 0 to 31, all different within a row; in each aligned block of 512 rows (0 to 511, 512 to 1023, ...) at most 36 rows name the same one
- route_weight: float32 [16384, 2], P('sp'), may hold values from 0.2 to 1
- expert_inputs: bfloat16 [32, 1152, 2048], P('sp'), may hold values from -6 to 6
- w_gate: bfloat16 [32, 2048, 2816], P('sp', None, 'tp'), may hold values from -0.125 to 0.125
- w_up: bfloat16 [32, 2048, 2816], P('sp', None, 'tp'), may hold values from -0.125 to 0.125
- w_down: bfloat16 [32, 2816, 2048], P('sp', 'tp'), may hold values from -0.109375 to 0.109375
- w_out: bfloat16 [2048, 1024], P(None, 'tp'), may hold values from -0.1875 to 0.1875
- queries: bfloat16 [16384, 4, 128], P('sp', 'tp'), may hold values from -6 to 6
- keys: bfloat16 [16384, 4, 128], P('sp', 'tp'), may hold values from -1.25 to 1.25
- values: bfloat16 [16384, 4, 256], P('sp', 'tp'), may hold values from -6 to 6
- log_decay: float32 [16384, 4, 128], P('sp', 'tp'), may hold values from -1 to 0
Outputs:
- grad_gate: bfloat16 [32, 2048, 2816], P('sp', None, 'tp')
- grad_up: bfloat16 [32, 2048, 2816], P('sp', None, 'tp')
- grad_down: bfloat16 [32, 2816, 2048], P('sp', 'tp')
- grad_proj: float32 [2048, 1024], P('sp', 'tp')
- grad_queries: bfloat16 [16384, 4, 128], P('sp', 'tp')
- grad_keys: bfloat16 [16384, 4, 128], P('sp', 'tp')
- grad_values: bfloat16 [16384, 4, 256], P('sp', 'tp')
- grad_log_decay: float32 [16384, 4, 128], P('sp', 'tp')
The draws below stay inside these ranges and needn't reach their ends.
Inputs may be any that keep to these rules, and one draw needn't show every extreme that they name: `route_expert`: the two experts of a token differ. Among the rows of one device no expert is named more than 36 times, and in every draw some device names some expert exactly 36 times.
All inputs are finite; a program needn't handle non-finite values.
Results may differ from the reference program's by a relative error of at most 0.02.
Values may be sent and summed in bfloat16 or wider, within the bound.
No kernel may reach another device: no remote copies, remote signals or barrier semaphores. Data moves between devices by JAX's collectives and lax.ppermute only.
A program may use at most 128 MiB of HBM per device.

```python
import math
import jax
import jax.numpy as jnp
import numpy as np
from jax import lax

D = 2048
FF = 2816
MIXER_HEADS = 4
KEY_CHANNELS = 128
DV = 256
BLK = 64
TOK_DEV = 512
SEQUENCE_TOKENS = 16384
EXPERTS = 32
CAP = 36
N_SP = 32
N_TP = 4


def draw_log_decay(key, part):
    every_head_keys = jax.random.split(jax.random.fold_in(key, 11), 7)
    slow_share = 0.5
    gradual_decay_mask = jax.random.bernoulli(every_head_keys[0], slow_share, (MIXER_HEADS, KEY_CHANNELS))
    slow_rate = jnp.exp(jax.random.uniform(every_head_keys[1], (MIXER_HEADS, KEY_CHANNELS), jnp.float32, jnp.log(0.05), jnp.log(0.5))) / SEQUENCE_TOKENS
    fast_rate = jnp.exp(jax.random.uniform(every_head_keys[2], (MIXER_HEADS, KEY_CHANNELS), jnp.float32, jnp.log(0.01), jnp.log(0.033)))
    base_rate = jnp.where(gradual_decay_mask, slow_rate, fast_rate)
    segment_count = SEQUENCE_TOKENS // TOK_DEV
    device_factor = jnp.exp(jax.random.uniform(every_head_keys[3], (segment_count, 1, 1, 1), jnp.float32, jnp.log(0.5), jnp.log(2.0)))
    device_factor = jnp.broadcast_to(device_factor, (segment_count, TOK_DEV, 1, 1)).reshape(SEQUENCE_TOKENS, 1, 1)
    roughness = jax.random.uniform(every_head_keys[4], (SEQUENCE_TOKENS, MIXER_HEADS, KEY_CHANNELS), jnp.float32, 0.5, 1.5)
    spike_position = jax.random.randint(every_head_keys[5], (4,), 0, SEQUENCE_TOKENS)
    spike_token_rows = jnp.any(jnp.arange(SEQUENCE_TOKENS)[:, None] == spike_position[None, :], axis=1)
    spike_penalty = jnp.log(jax.random.uniform(every_head_keys[6], (SEQUENCE_TOKENS, MIXER_HEADS, KEY_CHANNELS), jnp.float32, 0.5, 0.8))
    channel_decay_logs = -base_rate[None] * device_factor * roughness
    channel_decay_logs = channel_decay_logs + jnp.where(spike_token_rows[:, None, None] & gradual_decay_mask[None], spike_penalty, 0.0)
    return channel_decay_logs.astype(jnp.float32)


def with_spikes(drawn, own_key, source, target, shards_of, factor):
    def block_of(position):
        return (jnp.arange(drawn.shape[position]) // (drawn.shape[position] // shards_of)).reshape((-1,) + (1,) * (drawn.ndim - 1 - position))

    near = jax.random.permutation(own_key, shards_of)[block_of(target)]
    far = (block_of(target) + shards_of // 2) % shards_of
    return jnp.where((block_of(source) == near) | (block_of(source) == far), factor * drawn, drawn)


def levels(rng, dims, shards, least, largest):
    loudness = 1.0
    for dim, shards_of in shards:
        steps = jax.random.uniform(jax.random.fold_in(jax.random.fold_in(rng, 6), dim), (shards_of,), jnp.float32, least / len(shards), largest / len(shards))
        loudness = loudness * jnp.repeat(jnp.exp(steps), dims[dim] // shards_of).reshape((-1,) + (1,) * (len(dims) - 1 - dim))
    return loudness


def assign_block(own_key, own, number, rows, amount, top, reach, skew):
    ranking = jax.random.permutation(own_key, amount)
    crowded, ordinary = load_shares(amount, rows * top, reach, skew, True), load_shares(amount, rows * top, reach, skew, False)
    places = jnp.arange(amount)

    def named(sizes, turn):
        used = int((sizes > 0).sum())
        fixed = max(1, used // 4)
        passed = fixed + (places - fixed + turn * (used - fixed)) % max(1, amount - fixed)
        return jnp.zeros((amount,), jnp.int32).at[ranking[jnp.where(places < fixed, places, passed)]].set(jnp.asarray(sizes, jnp.int32))

    sizes = jnp.where(number % 4 == 0, named(crowded, number // 4), named(ordinary, number - number // 4 - 1))
    mixed = jax.random.permutation(jax.random.fold_in(own, 3), amount)
    giver, receiver = mixed[0:amount // 2 * 2:2], mixed[1:amount // 2 * 2:2]
    slack = jnp.minimum(sizes[giver] - 1, reach - sizes[receiver]) // 2
    slack = jnp.where((giver == ranking[0]) | (receiver == ranking[0]) | (sizes[receiver] == 0), 0, jnp.maximum(slack, 0))
    passed = jax.random.randint(jax.random.fold_in(own, 4), (amount // 2,), 0, 1 << 20) % (slack + 1)
    sizes = sizes.at[giver].add(-passed).at[receiver].add(passed)
    members = jnp.searchsorted(jnp.cumsum(sizes), jnp.arange(rows * top), side="right").astype(jnp.int32)
    grid = members.reshape(top, rows).T
    grid = grid[jax.random.permutation(jax.random.fold_in(own, 1), rows)]
    turn = jax.random.randint(jax.random.fold_in(own, 2), (rows, 1), 0, top)
    return jnp.take_along_axis(grid, (jnp.arange(top)[None, :] + turn) % top, axis=1)


def load_shares(amount, total, reach, lean, full):
    weights = [(1 << 20) // math.isqrt(grade ** lean) + 1 for grade in range(1, amount + 1)]
    largest = reach if full else min(reach, max(-(-total // amount), total * weights[0] // sum(weights)))
    least = 1 if total - largest >= amount - 1 else 0
    given, surplus = [largest] + [least] * (amount - 1), total - largest - least * (amount - 1)
    while surplus > 0:
        movable = [i for i in range(1, amount) if given[i] < largest] or [i for i in range(1, amount) if given[i] < reach]
        mass, budget = sum([weights[i] for i in movable]), surplus
        for i in movable:
            extra = min(reach - given[i], max(1, budget * weights[i] // mass), surplus)
            given[i] = given[i] + extra
            surplus = surplus - extra
    return np.array(given)


def gaussian(stream_key, shape, width, limit, shards=(), kind=jnp.bfloat16):
    loudness = levels(stream_key, shape, shards, -0.22, 0.18) if shards else 1.0
    entries = jax.random.normal(stream_key, shape, jnp.float32) * width * loudness
    return jnp.minimum(jnp.maximum(entries, -limit), limit).astype(kind)


def gaussian_with(rng, dims, scale, bound, cuts, heavy, kind=jnp.bfloat16):
    values = scale * jax.random.normal(rng, dims, jnp.float32)
    if cuts:
        values = values * levels(rng, dims, cuts, -0.22, 0.18)
    return jnp.clip(with_spikes(values, jax.random.fold_in(rng, 3), *heavy), -bound, bound).astype(kind)


def setup_inputs(seed: int = 0) -> dict:
    splits = jax.random.split(jax.random.key(seed), 13)
    d_out = gaussian_with(splits[0], (SEQUENCE_TOKENS, D), 1.0, 6.0, ((0, 32),), (0, 1, 32, 2.75))
    route_expert_keys = jax.random.split(jax.random.fold_in(splits[1], 1), SEQUENCE_TOKENS // TOK_DEV)
    route_expert_turns = jax.random.permutation(jax.random.fold_in(splits[1], 3), SEQUENCE_TOKENS // TOK_DEV)
    route_expert = jax.vmap(lambda own, number: assign_block(jax.random.fold_in(splits[1], 2), own, number, TOK_DEV, EXPERTS, 2, CAP, 0))(route_expert_keys, route_expert_turns).reshape((SEQUENCE_TOKENS, 2))
    route_weight = jnp.clip(0.2 + 0.8 * jax.random.uniform(splits[2], (SEQUENCE_TOKENS, 2), jnp.float32) ** levels(splits[2], (SEQUENCE_TOKENS, 2), ((0, 32),), -0.2, 0.2), 0.2, 1.0)
    expert_inputs = gaussian(splits[3], (EXPERTS, EXPERTS * CAP, D), 1.0, 6.0, ((0, 32),))
    w_gate = gaussian(splits[4], (EXPERTS, D, FF), D ** -0.5, 0.125, ((0, 32), (2, 4)))
    w_up = gaussian(splits[5], (EXPERTS, D, FF), D ** -0.5, 0.125, ((0, 32), (2, 4)))
    w_down = gaussian(splits[6], (EXPERTS, FF, D), FF ** -0.5, 0.109375, ((0, 32), (1, 4)))
    w_out = gaussian(splits[7], (D, MIXER_HEADS * DV), (MIXER_HEADS * DV) ** -0.5, 0.1875, ((1, 4),))
    queries = gaussian(splits[8], (SEQUENCE_TOKENS, MIXER_HEADS, KEY_CHANNELS), 1.0, 6.0, ((0, 32), (1, 4)))
    keys = gaussian(splits[9], (SEQUENCE_TOKENS, MIXER_HEADS, KEY_CHANNELS), (SEQUENCE_TOKENS ** -0.25), 1.25, ((0, 32), (1, 4)))
    values = gaussian(splits[10], (SEQUENCE_TOKENS, MIXER_HEADS, DV), 1.0, 6.0, ((0, 32), (1, 4)))
    log_decay = draw_log_decay(jax.random.fold_in(splits[12], 71), 0)
    return dict(d_out=d_out, route_expert=route_expert, route_weight=route_weight, expert_inputs=expert_inputs, w_gate=w_gate, w_up=w_up, w_down=w_down, w_out=w_out, queries=queries, keys=keys, values=values, log_decay=log_decay)


precise = lax.Precision.HIGHEST

def block_mixer(scaled_queries, keys_in, values_in, decay_in, initial):
    length, head_count, _ = scaled_queries.shape
    value_width = values_in.shape[-1]
    count_blocks = length // BLK

    def to_blocks(tensor):
        return tensor.reshape(count_blocks, BLK, head_count, tensor.shape[-1]).transpose(0, 2, 1, 3)
    causal = jnp.tril(jnp.ones((BLK, BLK), dtype=bool))[:, :, None]

    def advance(carry_state, inputs):
        query_block, key_block, value_block, decay_block = inputs
        cumulative = jnp.cumsum(decay_block, axis=1)
        ending = cumulative[:, -1, :]
        carried = jnp.einsum('hcd,hde->hce', query_block * jnp.exp(cumulative), carry_state, precision=precise)
        within = jnp.where(causal, jnp.exp(cumulative[:, :, None, :] - cumulative[:, None, :, :]), 0.0)
        scores = jnp.einsum('hid,hjd,hijd->hij', query_block, key_block, within, precision=precise)
        inner_part = jnp.einsum('hij,hje->hie', scores, value_block, precision=precise)
        faded_keys = key_block * jnp.exp(ending[:, None, :] - cumulative)
        carry_state = carry_state * jnp.exp(ending)[:, :, None] + jnp.einsum('hcd,hce->hde', faded_keys, value_block, precision=precise)
        return (carry_state, carried + inner_part)
    final_state, blocks_out = lax.scan(jax.checkpoint(advance), initial, (to_blocks(scaled_queries), to_blocks(keys_in), to_blocks(values_in), to_blocks(decay_in)))
    return (blocks_out.transpose(0, 2, 1, 3).reshape(length, head_count, value_width), final_state)

def expert_pass(rows_in, routed_rows, gate_w, up_w, down_w):
    gate_pre = jnp.dot(rows_in, gate_w, preferred_element_type=jnp.float32)
    up_pre = jnp.dot(rows_in, up_w, preferred_element_type=jnp.float32)
    sigmoid_gate = jax.nn.sigmoid(gate_pre)
    active = gate_pre * sigmoid_gate
    hidden = (active * up_pre).astype(jnp.bfloat16)
    d_hidden = lax.dot_general(routed_rows, down_w, (((1,), (1,)), ((), ())), preferred_element_type=jnp.float32)
    d_gate = (d_hidden * up_pre * sigmoid_gate * (1.0 + gate_pre * (1.0 - sigmoid_gate))).astype(jnp.bfloat16)
    d_up = (d_hidden * active).astype(jnp.bfloat16)
    rows_first = (((0,), (0,)), ((), ()))
    grad_gate = lax.dot_general(rows_in, d_gate, rows_first, preferred_element_type=jnp.float32).astype(jnp.bfloat16)
    grad_up = lax.dot_general(rows_in, d_up, rows_first, preferred_element_type=jnp.float32).astype(jnp.bfloat16)
    grad_down = lax.dot_general(hidden, routed_rows, rows_first, preferred_element_type=jnp.float32).astype(jnp.bfloat16)
    return (grad_gate, grad_up, grad_down, d_gate, d_up)

def reference(d_out, route_expert, route_weight, expert_inputs, w_gate, w_up, w_down, w_out, queries, keys, values, log_decay):
    per_block = route_expert.reshape(N_SP, 2 * TOK_DEV).astype(jnp.int32)
    onehot = (per_block[:, :, None] == jnp.arange(EXPERTS, dtype=jnp.int32)[None, None, :]).astype(jnp.int32)
    before = jnp.cumsum(onehot, axis=1) - onehot
    rank_slot = lax.optimization_barrier(jnp.sum(before * onehot, axis=2))
    source_dev = jnp.arange(N_SP, dtype=jnp.int32)[:, None]
    slot_index = (per_block * (N_SP * CAP) + source_dev * CAP + rank_slot).reshape(-1).astype(jnp.int32)
    scaled = (jnp.repeat(d_out, 2, axis=0).astype(jnp.float32) * route_weight.reshape(-1)[:, None]).astype(jnp.bfloat16)
    routed = jnp.zeros((EXPERTS * N_SP * CAP, D), jnp.bfloat16).at[slot_index].set(scaled).reshape(EXPERTS, N_SP * CAP, D)
    part_width = FF // N_TP

    def one_expert(operands):
        rows_in, routed_rows, gate_w, up_w, down_w = operands
        grad_gate, grad_up, grad_down, d_gate, d_up = expert_pass(rows_in, routed_rows, gate_w, up_w, down_w)
        total = jnp.zeros((rows_in.shape[0], D), jnp.float32)
        for piece in range(N_TP):
            lower = piece * part_width
            term = lax.dot_general(d_gate[:, lower:lower + part_width], gate_w[:, lower:lower + part_width], (((1,), (1,)), ((), ())), preferred_element_type=jnp.float32)
            term = term + lax.dot_general(d_up[:, lower:lower + part_width], up_w[:, lower:lower + part_width], (((1,), (1,)), ((), ())), preferred_element_type=jnp.float32)
            total = total + lax.optimization_barrier(term.astype(jnp.bfloat16)).astype(jnp.float32)
        return (grad_gate, grad_up, grad_down, total.astype(jnp.bfloat16))
    grad_gate, grad_up, grad_down, row_grads = lax.map(one_expert, (expert_inputs, routed, w_gate, w_up, w_down))
    picked = row_grads.reshape(-1, D)[slot_index].astype(jnp.float32).reshape(SEQUENCE_TOKENS, 2, D).sum(axis=1)
    mix_grad = (d_out.astype(jnp.float32) + picked).astype(jnp.bfloat16)
    scale_q = KEY_CHANNELS ** (-0.5)
    initial = jnp.zeros((MIXER_HEADS, KEY_CHANNELS, DV), jnp.float32)

    def mixer_map(query_x, key_x, value_x, decay_x):
        return block_mixer(query_x * scale_q, key_x, value_x, decay_x, initial)[0]
    mixer_out, pullback = jax.vjp(mixer_map, queries.astype(jnp.float32), keys.astype(jnp.float32), values.astype(jnp.float32), log_decay)
    mixed = mixer_out.reshape(SEQUENCE_TOKENS, MIXER_HEADS * DV).astype(jnp.bfloat16)
    grad_proj = lax.dot_general(mix_grad, mixed, (((0,), (0,)), ((), ())), preferred_element_type=jnp.float32)
    d_mixed = jnp.dot(mix_grad, w_out, preferred_element_type=jnp.float32).reshape(SEQUENCE_TOKENS, MIXER_HEADS, DV)
    grad_q, grad_k, grad_v, grad_g = pullback(d_mixed)
    return (grad_gate, grad_up, grad_down, grad_proj, grad_q.astype(jnp.bfloat16), grad_k.astype(jnp.bfloat16), grad_v.astype(jnp.bfloat16), grad_g)
```

```python
import jax
import jax.numpy as jnp
from jax import lax
from jax.experimental import pallas as pl
from jax.experimental.pallas import tpu as pltpu
from jax.sharding import Mesh
from jax.sharding import PartitionSpec as P

BLK = 64
PAD = 8
SP = ("sp_0", "sp_1", "sp_2")
INNER = ("sp_1", "sp_2")
OUTER = "sp_0"
F32 = jnp.float32
BF16 = jnp.bfloat16

NN = (((1,), (0,)), ((), ()))
NT = (((1,), (1,)), ((), ()))
TN = (((0,), (0,)), ((), ()))


def dot(a, b, dims):
    return lax.dot_general(a, b, dims, preferred_element_type=F32)


def halves(x):
    high = x.astype(BF16)
    return high, (x - high.astype(F32)).astype(BF16)


def thirds(x):
    high = x.astype(BF16)
    rest = x - high.astype(F32)
    middle = rest.astype(BF16)
    return high, middle, (rest - middle.astype(F32)).astype(BF16)


def dot_parts(a, b, dims):
    out = dot(a[0], b[0], dims)
    if len(a) > 1:
        out = out + dot(a[1], b[0], dims)
    if len(b) > 1:
        out = out + dot(a[0], b[1], dims)
    return out


def dot_exact(mask, x, dims):
    high, middle, low = thirds(x)
    return dot(mask, high, dims) + (dot(mask, middle, dims) + dot(mask, low, dims))


def grid_of(shape, dim):
    return lax.broadcasted_iota(jnp.int32, shape, dim)


def vmem_call(kernel, outs, **options):
    return pl.pallas_call(
        kernel,
        out_shape=outs,
        compiler_params=pltpu.CompilerParams(vmem_limit_bytes=56 * 1024 * 1024),
        **options,
    )


def route_body(d_out, experts_t, weight, outbox, pick):
    tokens = d_out.shape[0]
    slots, experts = outbox.shape[0], lax.axis_size(SP)
    stride = slots // experts
    first, second = experts_t[0:1, :], experts_t[1:2, :]
    ids = grid_of((experts, tokens), 0)
    is_first, is_second = ids == first, ids == second
    chosen = jnp.where(is_first | is_second, 1.0, 0.0).astype(BF16)
    earlier = jnp.where(
        grid_of((tokens, tokens), 0) < grid_of((tokens, tokens), 1), 1.0, 0.0
    ).astype(BF16)
    before = dot(chosen, earlier, NN)
    rank_a = jnp.sum(jnp.where(is_first, before, 0.0), axis=0, keepdims=True).astype(jnp.int32)
    rank_b = jnp.sum(jnp.where(is_second, before, 0.0), axis=0, keepdims=True).astype(jnp.int32)
    slot_a = first * stride + rank_a
    slot_b = second * stride + rank_b
    weights_a = jnp.concatenate(thirds(weight[:, 0:1]), axis=1)
    weights_b = jnp.concatenate(thirds(weight[:, 1:2]), axis=1)
    rows = d_out[...]
    step = 256
    for start in range(0, slots, step):
        slot = grid_of((step, tokens), 0) + start
        one_a = jnp.where(slot == slot_a, 1.0, 0.0).astype(BF16)
        one_b = jnp.where(slot == slot_b, 1.0, 0.0).astype(BF16)
        both = one_a + one_b
        factor = jnp.sum(dot(one_a, weights_a, NN) + dot(one_b, weights_b, NN), axis=1, keepdims=True)
        pick[start : start + step, :] = both
        outbox[start : start + step, :] = (dot(both, rows, NN) * factor).astype(BF16)


def expert_body(routed, active, slope, down_w, gate_w, up_w, d_gate, d_up, partial):
    d_hidden = dot(routed[...], down_w[...], NT)
    to_gate = (d_hidden * slope[...]).astype(BF16)
    to_up = (d_hidden * active[...]).astype(BF16)
    d_gate[...] = to_gate
    d_up[...] = to_up
    parts, _, width = partial.shape
    for part in range(parts):
        cols = slice(part * width, (part + 1) * width)
        term = dot(to_gate, gate_w[cols, :], NT) + dot(to_up, up_w[cols, :], NT)
        partial[part] = term.astype(BF16)


def expert_cotangents(routed, active, slope, down_w, gate_w, up_w, parts):
    rows, width = routed.shape
    units = down_w.shape[0]
    step = 256
    quarter = width // parts
    by_row = lambda i: (i, 0)
    whole = lambda i: (0, 0)
    return pl.pallas_call(
        expert_body,
        grid=(rows // step,),
        in_specs=[
            pl.BlockSpec((step, width), by_row),
            pl.BlockSpec((step, units), by_row),
            pl.BlockSpec((step, units), by_row),
            pl.BlockSpec((units, width), whole),
            pl.BlockSpec((width, units), whole),
            pl.BlockSpec((width, units), whole),
        ],
        out_specs=[
            pl.BlockSpec((step, units), by_row),
            pl.BlockSpec((step, units), by_row),
            pl.BlockSpec((parts, step, quarter), lambda i: (0, i, 0)),
        ],
        out_shape=[
            jax.ShapeDtypeStruct((rows, units), BF16),
            jax.ShapeDtypeStruct((rows, units), BF16),
            jax.ShapeDtypeStruct((parts, rows, quarter), BF16),
        ],
        compiler_params=pltpu.CompilerParams(vmem_limit_bytes=56 * 1024 * 1024),
    )(routed, active, slope, down_w, gate_w, up_w)


def triangle(reverse):
    row, col = grid_of((BLK, BLK), 0), grid_of((BLK, BLK), 1)
    return jnp.where((row <= col) if reverse else (row >= col), 1.0, 0.0).astype(BF16)


def local_state_body(keys, values, decay, cumulative, ends, gain, produced, ending):
    blocks = gain.shape[0]
    lower = triangle(False)
    for c in range(blocks):
        rows = slice(c * BLK, (c + 1) * BLK)
        cum = dot_exact(lower, decay[rows, :], NN)
        cumulative[rows, :] = cum
        end = cum[BLK - 1 : BLK, :]
        ends[c : c + 1, :] = end
        faded = keys[rows, :].astype(F32) * jnp.exp(end - cum)
        gain[c] = dot_parts((values[rows, :],), halves(faded), TN)
    state = gain[0]
    total = ends[0:1, :]
    for c in range(1, blocks):
        state = state * jnp.exp(ends[c : c + 1, :]) + gain[c]
        total = total + ends[c : c + 1, :]
    produced[...] = state.astype(BF16)
    ending[...] = total


def local_states(keys, values, decay):
    tokens, channels = keys.shape
    width = values.shape[1]
    blocks = tokens // BLK
    return vmem_call(
        local_state_body,
        [
            jax.ShapeDtypeStruct((tokens, channels), F32),
            jax.ShapeDtypeStruct((blocks, channels), F32),
            jax.ShapeDtypeStruct((blocks, width, channels), F32),
            jax.ShapeDtypeStruct((width, channels), BF16),
            jax.ShapeDtypeStruct((1, channels), F32),
        ],
    )(keys, values, decay)


def forward_body(queries, keys, values, cumulative, ends, gain, start, mixed, states, scores):
    blocks = gain.shape[0]
    scale = queries.shape[1] ** (-0.5)
    causal = grid_of((BLK, BLK), 0) >= grid_of((BLK, BLK), 1)
    state = start[...]
    for c in range(blocks):
        rows = slice(c * BLK, (c + 1) * BLK)
        cum = cumulative[rows, :]
        middle = cum[BLK // 2 - 1 : BLK // 2, :]
        query = queries[rows, :].astype(F32) * scale
        near_q = halves(query * jnp.exp(cum - middle))
        near_k = halves(keys[rows, :].astype(F32) * jnp.exp(middle - cum))
        score = jnp.where(causal, dot_parts(near_q, near_k, NT), 0.0)
        scores[rows, :] = score
        states[c] = state
        out = dot_parts(halves(query * jnp.exp(cum)), halves(state), NT)
        out = out + dot_parts(halves(score), (values[rows, :],), NN)
        mixed[rows, :] = out.astype(BF16)
        state = state * jnp.exp(ends[c : c + 1, :]) + gain[c]
    states[blocks] = state


def forward(queries, keys, values, cumulative, ends, gain, start):
    tokens, channels = keys.shape
    width = values.shape[1]
    blocks = tokens // BLK
    return vmem_call(
        forward_body,
        [
            jax.ShapeDtypeStruct((tokens, width), BF16),
            jax.ShapeDtypeStruct((blocks + 1, width, channels), F32),
            jax.ShapeDtypeStruct((tokens, BLK), F32),
        ],
    )(queries, keys, values, cumulative, ends, gain, start)


def cotangent_body(tiles, w_out, queries, cumulative, ends, d_mixed, back, own):
    blocks = back.shape[0]
    scale = queries.shape[1] ** (-0.5)
    quarter = tiles.shape[2]
    total = dot(tiles[0], w_out[0:quarter, :], NN)
    for part in range(1, tiles.shape[0]):
        total = total + dot(tiles[part], w_out[part * quarter : (part + 1) * quarter, :], NN)
    d_mixed[...] = total
    for c in range(blocks):
        rows = slice(c * BLK, (c + 1) * BLK)
        query = queries[rows, :].astype(F32) * (scale * jnp.exp(cumulative[rows, :]))
        back[c] = dot_parts(halves(d_mixed[rows, :]), halves(query), TN)
    state = back[blocks - 1]
    for c in reversed(range(blocks - 1)):
        state = state * jnp.exp(ends[c : c + 1, :]) + back[c]
    own[...] = state.astype(BF16)


def cotangents(tiles, w_out, queries, cumulative, ends):
    tokens, channels = queries.shape
    width = w_out.shape[1]
    blocks = tokens // BLK
    return vmem_call(
        cotangent_body,
        [
            jax.ShapeDtypeStruct((tokens, width), F32),
            jax.ShapeDtypeStruct((blocks, width, channels), F32),
            jax.ShapeDtypeStruct((width, channels), BF16),
        ],
    )(tiles, w_out, queries, cumulative, ends)


def inside_body(queries, keys, values, cumulative, scores, d_mixed, to_q, to_k, to_v):
    blocks = queries.shape[0] // BLK
    scale = queries.shape[1] ** (-0.5)
    causal = grid_of((BLK, BLK), 0) >= grid_of((BLK, BLK), 1)
    for c in range(blocks):
        rows = slice(c * BLK, (c + 1) * BLK)
        cum = cumulative[rows, :]
        middle = cum[BLK // 2 - 1 : BLK // 2, :]
        rising, falling = jnp.exp(cum - middle), jnp.exp(middle - cum)
        near_q = halves(queries[rows, :].astype(F32) * scale * rising)
        near_k = halves(keys[rows, :].astype(F32) * falling)
        incoming = halves(d_mixed[rows, :])
        d_score = jnp.where(causal, dot_parts(incoming, (values[rows, :],), NT), 0.0)
        d_score = halves(d_score)
        to_q[rows, :] = rising * dot_parts(d_score, near_k, NN)
        to_k[rows, :] = falling * dot_parts(d_score, near_q, TN)
        to_v[rows, :] = dot_parts(halves(scores[rows, :]), incoming, TN)


def inside_blocks(queries, keys, values, cumulative, scores, d_mixed):
    tokens, channels = queries.shape
    return vmem_call(
        inside_body,
        [
            jax.ShapeDtypeStruct((tokens, channels), F32),
            jax.ShapeDtypeStruct((tokens, channels), F32),
            jax.ShapeDtypeStruct(values.shape, F32),
        ],
    )(queries, keys, values, cumulative, scores, d_mixed)


def backward_body(
    queries, keys, values, cumulative, ends, d_mixed, states, back, to_q, to_k, to_v, later,
    grad_q, grad_k, grad_v, grad_g,
):
    blocks = back.shape[0]
    scale = queries.shape[1] ** (-0.5)
    upper = triangle(True)
    after = later[...]
    carry = jnp.sum(after * states[blocks], axis=0, keepdims=True)
    for c in reversed(range(blocks)):
        rows = slice(c * BLK, (c + 1) * BLK)
        cum = cumulative[rows, :]
        end = ends[c : c + 1, :]
        fading = jnp.exp(end - cum)
        key = keys[rows, :].astype(F32)
        after_parts = halves(after)
        d_query = jnp.exp(cum) * dot_parts(halves(d_mixed[rows, :]), halves(states[c]), NN)
        d_query = (d_query + to_q[rows, :]) * scale
        d_key = fading * dot_parts((values[rows, :],), after_parts, NN) + to_k[rows, :]
        d_value = dot_parts(halves(key * fading), after_parts, NT) + to_v[rows, :]
        grad_q[rows, :] = d_query.astype(BF16)
        grad_k[rows, :] = d_key.astype(BF16)
        grad_v[rows, :] = d_value.astype(BF16)
        change = queries[rows, :].astype(F32) * d_query - key * d_key
        summed = dot_exact(upper, change, NN) + carry
        grad_g[rows, :] = summed
        carry = summed[0:1, :]
        after = after * jnp.exp(end) + back[c]


def backward(queries, keys, values, cumulative, ends, d_mixed, states, back, inside, later):
    return vmem_call(
        backward_body,
        [
            jax.ShapeDtypeStruct(queries.shape, BF16),
            jax.ShapeDtypeStruct(keys.shape, BF16),
            jax.ShapeDtypeStruct(values.shape, BF16),
            jax.ShapeDtypeStruct(queries.shape, F32),
        ],
    )(queries, keys, values, cumulative, ends, d_mixed, states, back, *inside, later)


def sent_to_all(x, axis):
    count = lax.axis_size(axis)
    return lax.all_to_all(jnp.broadcast_to(x[None], (count, *x.shape)), axis, 0, 0, tiled=True)


def masked_sums(logs, mask):
    return jnp.sum(jnp.where(mask[:, :, None], logs[None], 0.0), axis=1)


def between(logs, index, reverse):
    count = logs.shape[0]
    row, col = grid_of((count, count), 0), grid_of((count, count), 1)
    if reverse:
        inner, outer = (col > index) & (col < row), col < row
        passed = jnp.arange(count) > index
        own = jnp.arange(count) > index
    else:
        inner, outer = (col < index) & (col > row), col > row
        passed = jnp.arange(count) < index
        own = jnp.arange(count) < index
    near = jnp.where(passed[:, None], jnp.exp(masked_sums(logs, inner)), 0.0)
    whole = jnp.exp(masked_sums(logs, outer))
    own = jnp.exp(jnp.sum(jnp.where(own[:, None], logs, 0.0), axis=0))
    return near, whole, own


def state_weights(endings, reverse):
    inner, outer = lax.axis_size(INNER), lax.axis_size(OUTER)
    grouped = endings.reshape(outer, inner, -1)
    place = lax.axis_index(OUTER)
    mine = jnp.sum(
        jnp.where((jnp.arange(outer) == place)[:, None, None], grouped, 0.0), axis=0
    )
    near, whole, own = between(mine, lax.axis_index(INNER), reverse)
    far, _, _ = between(jnp.sum(grouped, axis=1), place, reverse)
    return near, whole, own, far


def state_from_others(part, weights):
    near, whole, own, far = weights
    pieces = sent_to_all(part, INNER).astype(F32)
    group = jnp.sum(pieces * whole[:, None, :], axis=0).astype(BF16)
    inside = jnp.sum(pieces * near[:, None, :], axis=0)
    groups = sent_to_all(group, OUTER).astype(F32)
    return inside + own[None] * jnp.sum(groups * far[:, None, :], axis=0)


def local(
    d_out,
    route_expert,
    route_weight,
    expert_inputs,
    w_gate,
    w_up,
    w_down,
    w_out,
    queries,
    keys,
    values,
    log_decay,
):
    tok_rows, model_width = d_out.shape
    experts = lax.axis_size(SP)
    tp = lax.axis_size("tp")
    capacity = expert_inputs.shape[1] // experts
    stride = -(-capacity // PAD) * PAD
    slots = experts * stride
    quarter = model_width // tp

    outbox, pick = vmem_call(
        route_body,
        [
            jax.ShapeDtypeStruct((slots, model_width), BF16),
            jax.ShapeDtypeStruct((slots, tok_rows), BF16),
        ],
    )(d_out, route_expert.T, route_weight)
    routed = lax.all_to_all(
        outbox.reshape(experts, stride, model_width), SP, split_axis=0, concat_axis=0, tiled=True
    ).reshape(slots, model_width)

    query, key, value, decay = queries[:, 0], keys[:, 0], values[:, 0], log_decay[:, 0]
    cumulative, ends, gain, produced, ending = local_states(key, value, decay)
    endings = lax.all_gather(ending[0], SP)
    start = state_from_others(produced, state_weights(endings, False))
    mixed, states, scores = forward(query, key, value, cumulative, ends, gain, start)

    rows_in = expert_inputs[0].reshape(experts, capacity, model_width)
    rows_in = jnp.pad(rows_in, ((0, 0), (0, stride - capacity), (0, 0))).reshape(
        slots, model_width
    )
    gate_w, up_w, down_w = w_gate[0], w_up[0], w_down[0]
    gate_pre = dot(rows_in, gate_w, NN)
    up_pre = dot(rows_in, up_w, NN)
    sigmoid_gate = jax.nn.sigmoid(gate_pre)
    active = gate_pre * sigmoid_gate
    hidden = (active * up_pre).astype(BF16)
    slope = up_pre * sigmoid_gate * (1.0 + gate_pre * (1.0 - sigmoid_gate))
    d_gate, d_up, partial = expert_cotangents(routed, active, slope, down_w, gate_w, up_w, tp)
    arrived = lax.all_to_all(partial, "tp", 0, 0, tiled=True)
    grad_gate = dot(rows_in, d_gate, TN).astype(BF16)
    grad_up = dot(rows_in, d_up, TN).astype(BF16)
    grad_down = dot(hidden, routed, TN).astype(BF16)
    summed = jnp.sum(arrived.astype(F32), axis=0).astype(BF16)
    returned = lax.all_to_all(
        summed.reshape(experts, stride, quarter), SP, split_axis=0, concat_axis=0, tiled=True
    ).reshape(slots, quarter)

    own_cols = lax.dynamic_slice_in_dim(d_out, lax.axis_index("tp") * quarter, quarter, 1)
    mix_cols = (own_cols.astype(F32) + dot(pick, returned, TN)).astype(BF16)
    tiles = sent_to_all(mix_cols, "tp")

    d_mixed, back, own_term = cotangents(tiles, w_out, query, cumulative, ends)
    later = state_from_others(own_term, state_weights(endings, True))
    inside = inside_blocks(query, key, value, cumulative, scores, d_mixed)
    grad_q, grad_k, grad_v, grad_g = backward(
        query, key, value, cumulative, ends, d_mixed, states, back, inside, later
    )

    proj = jnp.einsum("ptc,te->pce", tiles, mixed, preferred_element_type=F32).astype(BF16)
    proj = proj.reshape(experts, model_width // experts, -1)
    grad_proj = jnp.sum(lax.all_to_all(proj, SP, 0, 0, tiled=True).astype(F32), axis=0)
    return (
        grad_gate[None],
        grad_up[None],
        grad_down[None],
        grad_proj,
        grad_q[:, None],
        grad_k[:, None],
        grad_v[:, None],
        grad_g[:, None],
    )


def solution(mesh):
    finer = Mesh(mesh.devices.reshape(4, 4, 2, mesh.shape["tp"]), ("sp_0", "sp_1", "sp_2", "tp"))
    return jax.shard_map(
        local,
        mesh=finer,
        in_specs=(
            P(SP, None),
            P(SP, None),
            P(SP, None),
            P(SP, None, None),
            P(SP, None, "tp"),
            P(SP, None, "tp"),
            P(SP, "tp", None),
            P(None, "tp"),
            P(SP, "tp", None),
            P(SP, "tp", None),
            P(SP, "tp", None),
            P(SP, "tp", None),
        ),
        out_specs=(
            P(SP, None, "tp"),
            P(SP, None, "tp"),
            P(SP, "tp", None),
            P(SP, "tp"),
            P(SP, "tp", None),
            P(SP, "tp", None),
            P(SP, "tp", None),
            P(SP, "tp", None),
        ),
        check_vma=False,
    )
```

```python
import functools

import jax
import jax.numpy as jnp
from jax import lax
from jax.experimental import pallas as pl
from jax.experimental.pallas import tpu as pltpu
from jax.sharding import Mesh
from jax.sharding import PartitionSpec as P


BLK = 64
PAD = 8
SP = ("sp_0", "sp_1", "sp_2")
F32 = jnp.float32
BF16 = jnp.bfloat16

NN = (((1,), (0,)), ((), ()))
NT = (((1,), (1,)), ((), ()))
TN = (((0,), (0,)), ((), ()))


def dot(a, b, dims):
    return lax.dot_general(a, b, dims, preferred_element_type=F32)


def halves(x):
    high = x.astype(BF16)
    return high, (x - high.astype(F32)).astype(BF16)


def thirds(x):
    high = x.astype(BF16)
    rest = x - high.astype(F32)
    middle = rest.astype(BF16)
    return high, middle, (rest - middle.astype(F32)).astype(BF16)


def dot_parts(a, b, dims):
    out = dot(a[0], b[0], dims)
    if len(a) > 1:
        out = out + dot(a[1], b[0], dims)
    if len(b) > 1:
        out = out + dot(a[0], b[1], dims)
    return out


def dot_exact(mask, x, dims):
    high, middle, low = thirds(x)
    return dot(mask, high, dims) + (dot(mask, middle, dims) + dot(mask, low, dims))


def grid_of(shape, dim):
    return lax.broadcasted_iota(jnp.int32, shape, dim)


def vmem_call(kernel, outs, **options):
    return pl.pallas_call(
        kernel,
        out_shape=outs,
        compiler_params=pltpu.CompilerParams(vmem_limit_bytes=56 * 1024 * 1024),
        **options,
    )


def fill_outbox(d_out, weight, slot_a, slot_b, outbox, pick):
    slots, tokens = pick.shape
    weights_a = jnp.concatenate(thirds(weight[0:1, :]), axis=0)
    weights_b = jnp.concatenate(thirds(weight[1:2, :]), axis=0)
    rows = d_out[...]
    step = 256
    for start in range(0, slots, step):
        slot = grid_of((step, tokens), 0) + start
        one_a = jnp.where(slot == slot_a, 1.0, 0.0).astype(BF16)
        one_b = jnp.where(slot == slot_b, 1.0, 0.0).astype(BF16)
        both = one_a + one_b
        factor = dot(one_a, weights_a, NT) + dot(one_b, weights_b, NT)
        factor = jnp.sum(factor, axis=1, keepdims=True)
        pick[start : start + step, :] = both
        outbox[start : start + step, :] = (dot(both, rows, NN) * factor).astype(BF16)


def slots_of(chosen, ranks, least, most, stride):
    inside = (ranks >= least) & (ranks < most)
    return jnp.where(inside, chosen * stride + ranks - least, -1)


def route_body(d_out, chosen, weight, outbox, pick, ranks, *, experts, most, stride):
    tokens = d_out.shape[0]
    first, second = chosen[0:1, :], chosen[1:2, :]
    ids = grid_of((experts, tokens), 0)
    is_first, is_second = ids == first, ids == second
    named = jnp.where(is_first | is_second, 1.0, 0.0).astype(BF16)
    earlier = jnp.where(
        grid_of((tokens, tokens), 0) < grid_of((tokens, tokens), 1), 1.0, 0.0
    ).astype(BF16)
    before = dot(named, earlier, NN)
    rank_a = jnp.sum(jnp.where(is_first, before, 0.0), axis=0, keepdims=True).astype(jnp.int32)
    rank_b = jnp.sum(jnp.where(is_second, before, 0.0), axis=0, keepdims=True).astype(jnp.int32)
    ranks[0:1, :] = rank_a
    ranks[1:2, :] = rank_b
    slot_a = slots_of(first, rank_a, 0, most, stride)
    slot_b = slots_of(second, rank_b, 0, most, stride)
    fill_outbox(d_out, weight, slot_a, slot_b, outbox, pick)


def refill_body(d_out, chosen, weight, ranks, outbox, pick, *, least, most, stride):
    slot_a = slots_of(chosen[0:1, :], ranks[0:1, :], least, most, stride)
    slot_b = slots_of(chosen[1:2, :], ranks[1:2, :], least, most, stride)
    fill_outbox(d_out, weight, slot_a, slot_b, outbox, pick)


def expert_body(place, routed, active, slope, down_w, gate_w, up_w, *refs):
    d_gate, d_up, keep_a, send_a, keep_b, send_b = refs[-6:]
    d_hidden = dot(routed[...], down_w[...], NT)
    to_gate = (d_hidden * slope[...]).astype(BF16)
    to_up = (d_hidden * active[...]).astype(BF16)
    d_gate[...] = to_gate
    d_up[...] = to_up
    half = keep_a.shape[2]
    homes = (
        ((keep_a, 0), (keep_b, 0)),
        ((send_a, 0), (keep_b, 1)),
        ((send_a, 1), (send_b, 1)),
        ((keep_a, 1), (send_b, 0)),
    )
    for k, (home_a, home_b) in enumerate(homes):
        start = pl.multiple_of((place[0] ^ k) * (2 * half), 2 * half)
        cols = pl.ds(start, 2 * half)
        term = dot(to_gate, gate_w[:, cols], NN) + dot(to_up, up_w[:, cols], NN)
        term = term.astype(BF16)
        home_a[0][home_a[1]] = term[:, :half]
        home_b[0][home_b[1]] = term[:, half:]


def expert_cotangents(place, routed, active, slope, down_w, gate_w, up_w, first_row, earlier):
    rows, width = routed.shape
    units = down_w.shape[0]
    step = 256
    half = width // 8
    skipped = first_row // step
    by_row = lambda i, *_: (i, 0)
    later_row = lambda i, *_: (i + skipped, 0)
    whole = lambda i, *_: (0, 0)
    in_specs = [
        pl.BlockSpec((step, width), by_row),
        pl.BlockSpec((step, units), later_row),
        pl.BlockSpec((step, units), later_row),
        pl.BlockSpec((units, width), whole),
        pl.BlockSpec((units, width), whole),
        pl.BlockSpec((units, width), whole),
    ]
    in_specs += [pl.BlockSpec(memory_space=pl.ANY)] * len(earlier)
    pair = pl.BlockSpec((2, step, half), lambda i, *_: (0, i, 0))
    return pl.pallas_call(
        expert_body,
        grid_spec=pltpu.PrefetchScalarGridSpec(
            num_scalar_prefetch=1,
            grid=(rows // step,),
            in_specs=in_specs,
            out_specs=[pl.BlockSpec((step, units), later_row)] * 2 + [pair] * 4,
        ),
        out_shape=[jax.ShapeDtypeStruct(active.shape, BF16)] * 2
        + [jax.ShapeDtypeStruct((2, rows, half), BF16)] * 4,
        input_output_aliases={7 + i: i for i in range(len(earlier))},
        compiler_params=pltpu.CompilerParams(vmem_limit_bytes=56 * 1024 * 1024),
    )(place, routed, active, slope, down_w, gate_w, up_w, *earlier)


def swapped(x, flip):
    count = lax.axis_size("tp")
    return lax.ppermute(x, "tp", [(i, i ^ flip) for i in range(count)])


def plus(*terms):
    total = terms[0].astype(F32)
    for term in terms[1:]:
        total = total + term.astype(F32)
    return total.astype(BF16)


def summed_over_tp(keep_a, send_a, keep_b, send_b):
    got_a = swapped(send_a, 1)
    got_b = swapped(send_b, 3)
    last_a, last_b = plus(keep_a[1], got_a[1]), plus(keep_b[1], got_b[1])
    last_a = swapped(last_a, 3)
    last_b = swapped(last_b, 1)
    return jnp.concatenate(
        [plus(keep_a[0], got_a[0], last_a), plus(keep_b[0], got_b[0], last_b)], axis=1
    )


def shifted(x, axis, by):
    count = lax.axis_size(axis)
    return lax.ppermute(x, axis, [(i, (i + by) % count) for i in range(count)])


def gathered_ring(x):
    half = x.shape[0] // 2
    below, above = shifted(x, "tp", 1), shifted(x, "tp", -1)
    across = jnp.concatenate(
        [shifted(below[:half], "tp", 1), shifted(above[half:], "tp", -1)], axis=0
    )
    return x, below, above, across


def triangle(reverse):
    row, col = grid_of((BLK, BLK), 0), grid_of((BLK, BLK), 1)
    return jnp.where((row <= col) if reverse else (row >= col), 1.0, 0.0).astype(BF16)


def local_state_body(keys, values, decay, cumulative, ends, gain, produced):
    blocks = gain.shape[0]
    lower = triangle(False)
    for c in range(blocks):
        rows = slice(c * BLK, (c + 1) * BLK)
        cum = dot_exact(lower, decay[rows, :], NN)
        cumulative[rows, :] = cum
        end = cum[BLK - 1 : BLK, :]
        ends[c : c + 1, :] = end
        faded = keys[rows, :].astype(F32) * jnp.exp(end - cum)
        gain[c] = dot_parts((values[rows, :],), halves(faded), TN)
    state = gain[0]
    total = ends[0:1, :]
    for c in range(1, blocks):
        state = state * jnp.exp(ends[c : c + 1, :]) + gain[c]
        total = total + ends[c : c + 1, :]
    width = state.shape[0]
    produced[0:width, :] = state
    spare = produced.shape[0] - width
    produced[width:, :] = jnp.where(grid_of((spare, total.shape[1]), 0) == 0, total, 0.0)


def local_states(keys, values, decay):
    tokens, channels = keys.shape
    width = values.shape[1]
    blocks = tokens // BLK
    return vmem_call(
        local_state_body,
        [
            jax.ShapeDtypeStruct((tokens, channels), F32),
            jax.ShapeDtypeStruct((blocks, channels), F32),
            jax.ShapeDtypeStruct((blocks, width, channels), F32),
            jax.ShapeDtypeStruct((width + 8, channels), F32),
        ],
    )(keys, values, decay)


def forward_body(queries, keys, values, cumulative, ends, gain, start, mixed, states, scores):
    blocks = gain.shape[0]
    scale = queries.shape[1] ** (-0.5)
    causal = grid_of((BLK, BLK), 0) >= grid_of((BLK, BLK), 1)
    state = start[...]
    for c in range(blocks):
        rows = slice(c * BLK, (c + 1) * BLK)
        cum = cumulative[rows, :]
        middle = cum[BLK // 2 - 1 : BLK // 2, :]
        query = queries[rows, :].astype(F32) * scale
        near_q = halves(query * jnp.exp(cum - middle))
        near_k = halves(keys[rows, :].astype(F32) * jnp.exp(middle - cum))
        score = jnp.where(causal, dot_parts(near_q, near_k, NT), 0.0)
        scores[rows, :] = score
        states[c] = state
        out = dot_parts(halves(query * jnp.exp(cum)), halves(state), NT)
        out = out + dot_parts(halves(score), (values[rows, :],), NN)
        mixed[rows, :] = out.astype(BF16)
        state = state * jnp.exp(ends[c : c + 1, :]) + gain[c]
    states[blocks] = state


def forward(queries, keys, values, cumulative, ends, gain, start):
    tokens, channels = keys.shape
    width = values.shape[1]
    blocks = tokens // BLK
    return vmem_call(
        forward_body,
        [
            jax.ShapeDtypeStruct((tokens, width), BF16),
            jax.ShapeDtypeStruct((blocks + 1, width, channels), F32),
            jax.ShapeDtypeStruct((tokens, BLK), F32),
        ],
    )(queries, keys, values, cumulative, ends, gain, start)


def cotangent_body(place, a, b, c, d, w_out, queries, cumulative, ends, d_mixed, back, own):
    blocks = back.shape[0]
    scale = queries.shape[1] ** (-0.5)
    quarter = a.shape[1]
    total = None
    for tile, offset in ((a, 0), (b, 3), (c, 1), (d, 2)):
        start = pl.multiple_of(((place[0] + offset) & 3) * quarter, quarter)
        term = dot(tile[...], w_out[pl.ds(start, quarter), :], NN)
        total = term if total is None else total + term
    d_mixed[...] = total
    for c in range(blocks):
        rows = slice(c * BLK, (c + 1) * BLK)
        query = queries[rows, :].astype(F32) * (scale * jnp.exp(cumulative[rows, :]))
        back[c] = dot_parts(halves(d_mixed[rows, :]), halves(query), TN)
    state = back[blocks - 1]
    for c in reversed(range(blocks - 1)):
        state = state * jnp.exp(ends[c : c + 1, :]) + back[c]
    own[...] = state.astype(BF16)


SMEM = pl.BlockSpec(memory_space=pltpu.SMEM)
VMEM = pl.BlockSpec(memory_space=pltpu.VMEM)


def cotangents(place, tiles, w_out, queries, cumulative, ends):
    tokens, channels = queries.shape
    width = w_out.shape[1]
    blocks = tokens // BLK
    return vmem_call(
        cotangent_body,
        [
            jax.ShapeDtypeStruct((tokens, width), F32),
            jax.ShapeDtypeStruct((blocks, width, channels), F32),
            jax.ShapeDtypeStruct((width, channels), BF16),
        ],
        in_specs=[SMEM] + [VMEM] * 8,
    )(place, *tiles, w_out, queries, cumulative, ends)


def projection_body(place, a, b, c, d, mixed, out):
    quarter = a.shape[1]
    for tile, offset in ((a, 0), (b, 3), (c, 1), (d, 2)):
        start = pl.multiple_of(((place[0] + offset) & 3) * quarter, quarter)
        out[pl.ds(start, quarter), :] = dot(tile[...], mixed[...], TN).astype(BF16)


def projection(place, tiles, mixed):
    return vmem_call(
        projection_body,
        jax.ShapeDtypeStruct((4 * tiles[0].shape[1], mixed.shape[1]), BF16),
        in_specs=[SMEM] + [VMEM] * 5,
    )(place, *tiles, mixed)


def inside_body(queries, keys, values, cumulative, scores, d_mixed, to_q, to_k, to_v):
    blocks = queries.shape[0] // BLK
    scale = queries.shape[1] ** (-0.5)
    causal = grid_of((BLK, BLK), 0) >= grid_of((BLK, BLK), 1)
    for c in range(blocks):
        rows = slice(c * BLK, (c + 1) * BLK)
        cum = cumulative[rows, :]
        middle = cum[BLK // 2 - 1 : BLK // 2, :]
        rising, falling = jnp.exp(cum - middle), jnp.exp(middle - cum)
        near_q = halves(queries[rows, :].astype(F32) * scale * rising)
        near_k = halves(keys[rows, :].astype(F32) * falling)
        incoming = halves(d_mixed[rows, :])
        d_score = jnp.where(causal, dot_parts(incoming, (values[rows, :],), NT), 0.0)
        d_score = halves(d_score)
        to_q[rows, :] = rising * dot_parts(d_score, near_k, NN)
        to_k[rows, :] = falling * dot_parts(d_score, near_q, TN)
        to_v[rows, :] = dot_parts(halves(scores[rows, :]), incoming, TN)


def inside_blocks(queries, keys, values, cumulative, scores, d_mixed):
    tokens, channels = queries.shape
    return vmem_call(
        inside_body,
        [
            jax.ShapeDtypeStruct((tokens, channels), F32),
            jax.ShapeDtypeStruct((tokens, channels), F32),
            jax.ShapeDtypeStruct(values.shape, F32),
        ],
    )(queries, keys, values, cumulative, scores, d_mixed)


def backward_body(
    queries, keys, values, cumulative, ends, d_mixed, states, back, to_q, to_k, to_v, later,
    grad_q, grad_k, grad_v, grad_g,
):
    blocks = back.shape[0]
    scale = queries.shape[1] ** (-0.5)
    upper = triangle(True)
    after = later[...]
    carry = jnp.sum(after * states[blocks], axis=0, keepdims=True)
    for c in reversed(range(blocks)):
        rows = slice(c * BLK, (c + 1) * BLK)
        cum = cumulative[rows, :]
        end = ends[c : c + 1, :]
        fading = jnp.exp(end - cum)
        key = keys[rows, :].astype(F32)
        after_parts = halves(after)
        d_query = jnp.exp(cum) * dot_parts(halves(d_mixed[rows, :]), halves(states[c]), NN)
        d_query = (d_query + to_q[rows, :]) * scale
        d_key = fading * dot_parts((values[rows, :],), after_parts, NN) + to_k[rows, :]
        d_value = dot_parts(halves(key * fading), after_parts, NT) + to_v[rows, :]
        grad_q[rows, :] = d_query.astype(BF16)
        grad_k[rows, :] = d_key.astype(BF16)
        grad_v[rows, :] = d_value.astype(BF16)
        change = queries[rows, :].astype(F32) * d_query - key * d_key
        summed = dot_exact(upper, change, NN) + carry
        grad_g[rows, :] = summed
        carry = summed[0:1, :]
        after = after * jnp.exp(end) + back[c]


def backward(queries, keys, values, cumulative, ends, d_mixed, states, back, inside, later):
    return vmem_call(
        backward_body,
        [
            jax.ShapeDtypeStruct(queries.shape, BF16),
            jax.ShapeDtypeStruct(keys.shape, BF16),
            jax.ShapeDtypeStruct(values.shape, BF16),
            jax.ShapeDtypeStruct(queries.shape, F32),
        ],
    )(queries, keys, values, cumulative, ends, d_mixed, states, back, *inside, later)


def order_weights(logs, index, reverse):
    count = logs.shape[0]
    place = lax.rem(index - jnp.arange(count, dtype=jnp.int32) + count, count)
    row, col = place[:, None], place[None, :]
    if reverse:
        inner, outer, passed = (col < row) & (col > index), col < row, place > index
    else:
        inner, outer, passed = (col > row) & (col < index), col > row, place < index
    masked = lambda mask: jnp.sum(jnp.where(mask[:, :, None], logs[None], 0.0), axis=1)
    near = jnp.where(passed[:, None], jnp.exp(masked(inner)), 0.0)
    whole = jnp.exp(masked(outer))
    own = jnp.exp(jnp.sum(jnp.where(passed[:, None], logs, 0.0), axis=0))
    return near, whole, own


def everyone(x, axis):
    return [x] + [shifted(x, axis, k) for k in range(1, lax.axis_size(axis))]


def weighted(pieces, weights):
    total = 0.0
    for k, piece in enumerate(pieces):
        total = total + piece.astype(F32) * weights[k][None, :]
    return total


def states_before(payload):
    width = payload.shape[0] - 8
    levels, kept = [], []
    for axis in reversed(SP):
        pieces = everyone(payload, axis)
        logs = jnp.stack([piece[width] for piece in pieces])
        index = lax.axis_index(axis)
        near, whole, own = order_weights(logs, index, False)
        states = [piece[:width] for piece in pieces]
        levels.append((weighted(states, near), own))
        kept.append(order_weights(logs, index, True))
        if axis != SP[0]:
            row = jnp.sum(logs, axis=0)[None]
            row = jnp.pad(row, ((0, 7), (0, 0)))
            payload = jnp.concatenate([weighted(states, whole), row], axis=0)
    return chained(levels), kept


def chained(levels):
    state = levels[-1][0]
    for inside, own in reversed(levels[:-1]):
        state = inside + own[None] * state
    return state


def states_after(part, kept):
    levels = []
    for axis, (near, whole, own) in zip(reversed(SP), kept):
        pieces = everyone(part, axis)
        levels.append((weighted(pieces, near), own))
        if axis != SP[0]:
            part = weighted(pieces, whole).astype(BF16)
    return chained(levels)


def local(
    d_out,
    route_expert,
    route_weight,
    expert_inputs,
    w_gate,
    w_up,
    w_down,
    w_out,
    queries,
    keys,
    values,
    log_decay,
):
    tok_rows, model_width = d_out.shape
    experts = lax.axis_size(SP)
    capacity = expert_inputs.shape[1] // experts
    cut = capacity * 2 // 3 // PAD * PAD
    tail = -(-(capacity - cut) // PAD) * PAD
    quarter = model_width // lax.axis_size("tp")
    place = lax.axis_index("tp").reshape(1)
    chosen, weight = route_expert.T, route_weight.T

    def exchanged(box, stride):
        box = box.reshape(experts, stride, box.shape[1])
        box = lax.all_to_all(box, SP, split_axis=0, concat_axis=0, tiled=True)
        return box.reshape(experts * stride, box.shape[2])

    outbox_a, pick_a, ranks = vmem_call(
        functools.partial(route_body, experts=experts, most=cut, stride=cut),
        [
            jax.ShapeDtypeStruct((experts * cut, model_width), BF16),
            jax.ShapeDtypeStruct((experts * cut, tok_rows), BF16),
            jax.ShapeDtypeStruct((2, tok_rows), jnp.int32),
        ],
    )(d_out, chosen, weight)
    routed_a = exchanged(outbox_a, cut)
    outbox_b, pick_b = vmem_call(
        functools.partial(refill_body, least=cut, most=capacity, stride=tail),
        [
            jax.ShapeDtypeStruct((experts * tail, model_width), BF16),
            jax.ShapeDtypeStruct((experts * tail, tok_rows), BF16),
        ],
    )(d_out, chosen, weight, ranks)
    routed_b = exchanged(outbox_b, tail)

    rows_in = expert_inputs[0].reshape(experts, capacity, model_width)
    rows_a = rows_in[:, :cut].reshape(experts * cut, model_width)
    rows_b = jnp.pad(rows_in[:, cut:], ((0, 0), (0, cut + tail - capacity), (0, 0)))
    rows_in = jnp.concatenate([rows_a, rows_b.reshape(experts * tail, model_width)], axis=0)
    gate_w, up_w, down_w = w_gate[0].T, w_up[0].T, w_down[0]
    gate_pre = dot(rows_in, gate_w, NT)
    up_pre = dot(rows_in, up_w, NT)
    sigmoid_gate = jax.nn.sigmoid(gate_pre)
    active = gate_pre * sigmoid_gate
    hidden = (active * up_pre).astype(BF16)
    slope = up_pre * sigmoid_gate * (1.0 + gate_pre * (1.0 - sigmoid_gate))

    query, key, value, decay = queries[:, 0], keys[:, 0], values[:, 0], log_decay[:, 0]
    cumulative, ends, gain, produced = local_states(key, value, decay)
    start, kept = states_before(produced)
    mixed, states, scores = forward(query, key, value, cumulative, ends, gain, start)

    weights = (active, slope, down_w, gate_w, up_w)
    d_gate, d_up, *parts_a = expert_cotangents(place, routed_a, *weights, 0, ())
    d_gate, d_up, *parts_b = expert_cotangents(
        place, routed_b, *weights, experts * cut, (d_gate, d_up)
    )
    returned_a = exchanged(summed_over_tp(*parts_a), cut)
    returned_b = exchanged(summed_over_tp(*parts_b), tail)
    routed = jnp.concatenate([routed_a, routed_b], axis=0)
    grad_gate = dot(d_gate, rows_in, TN).astype(BF16).T
    grad_up = dot(d_up, rows_in, TN).astype(BF16).T
    grad_down = dot(hidden, routed, TN).astype(BF16)

    own_cols = lax.dynamic_slice_in_dim(d_out, place[0] * quarter, quarter, 1)
    picked = own_cols.astype(F32) + dot(pick_a, returned_a, TN)
    picked = picked + dot(pick_b, returned_b, TN)
    tiles = gathered_ring(picked.astype(BF16))

    d_mixed, back, own_term = cotangents(place, tiles, w_out, query, cumulative, ends)
    later = states_after(own_term, kept)
    inside = inside_blocks(query, key, value, cumulative, scores, d_mixed)
    grad_q, grad_k, grad_v, grad_g = backward(
        query, key, value, cumulative, ends, d_mixed, states, back, inside, later
    )

    proj = projection(place, tiles, mixed).reshape(experts, model_width // experts, -1)
    grad_proj = jnp.sum(lax.all_to_all(proj, SP, 0, 0, tiled=True).astype(F32), axis=0)
    return (
        grad_gate[None],
        grad_up[None],
        grad_down[None],
        grad_proj,
        grad_q[:, None],
        grad_k[:, None],
        grad_v[:, None],
        grad_g[:, None],
    )


def solution(mesh):
    finer = Mesh(mesh.devices.reshape(4, 4, 2, mesh.shape["tp"]), ("sp_0", "sp_1", "sp_2", "tp"))
    return jax.shard_map(
        local,
        mesh=finer,
        in_specs=(
            P(SP, None),
            P(SP, None),
            P(SP, None),
            P(SP, None, None),
            P(SP, None, "tp"),
            P(SP, None, "tp"),
            P(SP, "tp", None),
            P(None, "tp"),
            P(SP, "tp", None),
            P(SP, "tp", None),
            P(SP, "tp", None),
            P(SP, "tp", None),
        ),
        out_specs=(
            P(SP, None, "tp"),
            P(SP, None, "tp"),
            P(SP, "tp", None),
            P(SP, "tp"),
            P(SP, "tp", None),
            P(SP, "tp", None),
            P(SP, "tp", None),
            P(SP, "tp", None),
        ),
        check_vma=False,
    )
```

```python
import functools

import jax
import jax.numpy as jnp
from jax import lax
from jax.experimental import pallas as pl
from jax.experimental.pallas import tpu as pltpu
from jax.sharding import Mesh
from jax.sharding import PartitionSpec as P


BLK = 64
PAD = 8
SP = ("sp_0", "sp_1", "sp_2")
F32 = jnp.float32
BF16 = jnp.bfloat16

NN = (((1,), (0,)), ((), ()))
NT = (((1,), (1,)), ((), ()))
TN = (((0,), (0,)), ((), ()))


def dot(a, b, dims):
    return lax.dot_general(a, b, dims, preferred_element_type=F32)


def halves(x):
    high = x.astype(BF16)
    return high, (x - high.astype(F32)).astype(BF16)


def thirds(x):
    high = x.astype(BF16)
    rest = x - high.astype(F32)
    middle = rest.astype(BF16)
    return high, middle, (rest - middle.astype(F32)).astype(BF16)


def dot_parts(a, b, dims):
    out = dot(a[0], b[0], dims)
    if len(a) > 1:
        out = out + dot(a[1], b[0], dims)
    if len(b) > 1:
        out = out + dot(a[0], b[1], dims)
    return out


def dot_exact(mask, x, dims):
    high, middle, low = thirds(x)
    return dot(mask, high, dims) + (dot(mask, middle, dims) + dot(mask, low, dims))


def grid_of(shape, dim):
    return lax.broadcasted_iota(jnp.int32, shape, dim)


SMEM = pl.BlockSpec(memory_space=pltpu.SMEM)
VMEM = pl.BlockSpec(memory_space=pltpu.VMEM)


def limit(mebibytes):
    return pltpu.CompilerParams(vmem_limit_bytes=mebibytes * 1024 * 1024)


def vmem_call(kernel, outs, mebibytes=12, **options):
    return pl.pallas_call(kernel, out_shape=outs, compiler_params=limit(mebibytes), **options)


def fill_outbox(d_out, weight, slot_a, slot_b, outbox, pick):
    slots, tokens = pick.shape
    weights_a = jnp.concatenate(thirds(weight[0:1, :]), axis=0)
    weights_b = jnp.concatenate(thirds(weight[1:2, :]), axis=0)
    rows = d_out[...]
    step = 256
    for start in range(0, slots, step):
        slot = grid_of((step, tokens), 0) + start
        one_a = jnp.where(slot == slot_a, 1.0, 0.0).astype(BF16)
        one_b = jnp.where(slot == slot_b, 1.0, 0.0).astype(BF16)
        both = one_a + one_b
        factor = dot(one_a, weights_a, NT) + dot(one_b, weights_b, NT)
        factor = jnp.sum(factor, axis=1, keepdims=True)
        pick[start : start + step, :] = both
        outbox[start : start + step, :] = (dot(both, rows, NN) * factor).astype(BF16)


def slots_of(chosen, ranks, least, most, stride):
    inside = (ranks >= least) & (ranks < most)
    return jnp.where(inside, chosen * stride + ranks - least, -1)


def route_body(d_out, chosen, weight, outbox, pick, ranks, *, experts, most, stride):
    tokens = d_out.shape[0]
    first, second = chosen[0:1, :], chosen[1:2, :]
    ids = grid_of((experts, tokens), 0)
    is_first, is_second = ids == first, ids == second
    named = jnp.where(is_first | is_second, 1.0, 0.0).astype(BF16)
    earlier = jnp.where(
        grid_of((tokens, tokens), 0) < grid_of((tokens, tokens), 1), 1.0, 0.0
    ).astype(BF16)
    before = dot(named, earlier, NN)
    rank_a = jnp.sum(jnp.where(is_first, before, 0.0), axis=0, keepdims=True).astype(jnp.int32)
    rank_b = jnp.sum(jnp.where(is_second, before, 0.0), axis=0, keepdims=True).astype(jnp.int32)
    ranks[0:1, :] = rank_a
    ranks[1:2, :] = rank_b
    slot_a = slots_of(first, rank_a, 0, most, stride)
    slot_b = slots_of(second, rank_b, 0, most, stride)
    fill_outbox(d_out, weight, slot_a, slot_b, outbox, pick)


def refill_body(d_out, chosen, weight, ranks, outbox, pick, *, least, most, stride):
    slot_a = slots_of(chosen[0:1, :], ranks[0:1, :], least, most, stride)
    slot_b = slots_of(chosen[1:2, :], ranks[1:2, :], least, most, stride)
    fill_outbox(d_out, weight, slot_a, slot_b, outbox, pick)


def slot_order(group, capacity, cut, tail):
    def placed(rows, stride, width, first):
        row, col = grid_of((rows, group * capacity), 0), grid_of((rows, group * capacity), 1)
        found = row < 0
        for source in range(group):
            start = source * stride
            here = (row >= start) & (row < start + width)
            found = found | (here & (col == row + (source * capacity + first - start)))
        return jnp.where(found, 1.0, 0.0).astype(BF16)

    return placed(group * cut, cut, cut, 0), placed(group * tail, tail, capacity - cut, cut)


def expert_forward_body(
    inputs, gate_w, up_w, rows_in, active, slope, hidden, *, experts, capacity, cut, tail
):
    group = 8
    orders = slot_order(group, capacity, cut, tail)
    for step in range(experts // group):
        block = inputs[step * group * capacity : (step + 1) * group * capacity, :]
        for order, start in zip(orders, (step * group * cut, experts * cut + step * group * tail)):
            rows_in[start : start + order.shape[0], :] = dot(order, block, NN).astype(BF16)
    units = gate_w.shape[0]
    step = rows_in.shape[0] // 2
    for first in range(0, units, 256):
        cols = slice(first, min(first + 256, units))
        for start in range(0, rows_in.shape[0], step):
            rows = slice(start, start + step)
            gate = dot(rows_in[rows, :], gate_w[cols, :], NT)
            up = dot(rows_in[rows, :], up_w[cols, :], NT)
            sigmoid = 1.0 / (1.0 + jnp.exp(-gate))
            silu = gate * sigmoid
            hidden[rows, cols] = (silu * up).astype(BF16)
            active[rows, cols] = silu.astype(BF16)
            slope[rows, cols] = (up * sigmoid * (1.0 + gate * (1.0 - sigmoid))).astype(BF16)


def expert_forward(inputs, gate_w, up_w, experts, capacity, cut, tail):
    slots = experts * (cut + tail)
    units = gate_w.shape[0]
    return vmem_call(
        functools.partial(
            expert_forward_body, experts=experts, capacity=capacity, cut=cut, tail=tail
        ),
        [jax.ShapeDtypeStruct((slots, inputs.shape[1]), BF16)]
        + [jax.ShapeDtypeStruct((slots, units), BF16)] * 3,
        mebibytes=56,
    )(inputs, gate_w, up_w)


def expert_body(place, routed, active, slope, down_w, gate_w, up_w, *refs):
    routed_out, d_gate, d_up, keep_a, send_a, keep_b, send_b = refs[-7:]
    routed_out[...] = routed[...]
    d_hidden = dot(routed[...], down_w[...], NT)
    to_gate = (d_hidden * slope[...].astype(F32)).astype(BF16)
    to_up = (d_hidden * active[...].astype(F32)).astype(BF16)
    d_gate[...] = to_gate
    d_up[...] = to_up
    half = keep_a.shape[2]
    homes = (
        ((keep_a, 0), (keep_b, 0)),
        ((send_a, 0), (keep_b, 1)),
        ((send_a, 1), (send_b, 1)),
        ((keep_a, 1), (send_b, 0)),
    )
    for k, (home_a, home_b) in enumerate(homes):
        start = pl.multiple_of((place[0] ^ k) * (2 * half), 2 * half)
        cols = pl.ds(start, 2 * half)
        term = dot(to_gate, gate_w[:, cols], NN) + dot(to_up, up_w[:, cols], NN)
        term = term.astype(BF16)
        home_a[0][home_a[1]] = term[:, :half]
        home_b[0][home_b[1]] = term[:, half:]


def expert_cotangents(place, routed, active, slope, down_w, gate_w, up_w, first_row, earlier):
    rows, width = routed.shape
    units = down_w.shape[0]
    step = 256
    half = width // 8
    skipped = first_row // step
    by_row = lambda i, *_: (i, 0)
    later_row = lambda i, *_: (i + skipped, 0)
    whole = lambda i, *_: (0, 0)
    in_specs = [
        pl.BlockSpec((step, width), by_row),
        pl.BlockSpec((step, units), later_row),
        pl.BlockSpec((step, units), later_row),
        pl.BlockSpec((units, width), whole),
        pl.BlockSpec((units, width), whole),
        pl.BlockSpec((units, width), whole),
    ]
    in_specs += [pl.BlockSpec(memory_space=pl.ANY)] * len(earlier)
    pair = pl.BlockSpec((2, step, half), lambda i, *_: (0, i, 0))
    return pl.pallas_call(
        expert_body,
        grid_spec=pltpu.PrefetchScalarGridSpec(
            num_scalar_prefetch=1,
            grid=(rows // step,),
            in_specs=in_specs,
            out_specs=[pl.BlockSpec((step, width), later_row)]
            + [pl.BlockSpec((step, units), later_row)] * 2
            + [pair] * 4,
        ),
        out_shape=[jax.ShapeDtypeStruct((active.shape[0], width), BF16)]
        + [jax.ShapeDtypeStruct(active.shape, BF16)] * 2
        + [jax.ShapeDtypeStruct((2, rows, half), BF16)] * 4,
        input_output_aliases={7 + i: i for i in range(len(earlier))},
        compiler_params=limit(56),
    )(place, routed, active, slope, down_w, gate_w, up_w, *earlier)


def swapped(x, flip):
    count = lax.axis_size("tp")
    return lax.ppermute(x, "tp", [(i, i ^ flip) for i in range(count)])


def plus(*terms):
    total = terms[0].astype(F32)
    for term in terms[1:]:
        total = total + term.astype(F32)
    return total.astype(BF16)


def summed_over_tp(keep_a, send_a, keep_b, send_b):
    got_a = swapped(send_a, 1)
    got_b = swapped(send_b, 3)
    last_a, last_b = plus(keep_a[1], got_a[1]), plus(keep_b[1], got_b[1])
    last_a = swapped(last_a, 3)
    last_b = swapped(last_b, 1)
    return jnp.concatenate(
        [plus(keep_a[0], got_a[0], last_a), plus(keep_b[0], got_b[0], last_b)], axis=1
    )


def shifted(x, axis, by):
    count = lax.axis_size(axis)
    return lax.ppermute(x, axis, [(i, (i + by) % count) for i in range(count)])


def gathered_ring(x):
    half = x.shape[0] // 2
    below = shifted(x, "tp", 1)
    above = shifted(x, "tp", -1)
    across = jnp.concatenate(
        [shifted(below[:half], "tp", 1), shifted(above[half:], "tp", -1)], axis=0
    )
    return x, below, above, across


def triangle(reverse):
    row, col = grid_of((BLK, BLK), 0), grid_of((BLK, BLK), 1)
    return jnp.where((row <= col) if reverse else (row >= col), 1.0, 0.0).astype(BF16)


def local_state_body(keys, values, decay, cumulative, ends, gain, produced):
    blocks = gain.shape[0]
    lower = triangle(False)
    for c in range(blocks):
        rows = slice(c * BLK, (c + 1) * BLK)
        cum = dot_exact(lower, decay[rows, :], NN)
        cumulative[rows, :] = cum
        end = cum[BLK - 1 : BLK, :]
        ends[c : c + 1, :] = end
        faded = keys[rows, :].astype(F32) * jnp.exp(end - cum)
        gain[c] = dot_parts((values[rows, :],), halves(faded), TN)
    state = gain[0]
    total = ends[0:1, :]
    for c in range(1, blocks):
        state = state * jnp.exp(ends[c : c + 1, :]) + gain[c]
        total = total + ends[c : c + 1, :]
    width = state.shape[0]
    produced[0:width, :] = state
    spare = produced.shape[0] - width
    produced[width:, :] = jnp.where(grid_of((spare, total.shape[1]), 0) == 0, total, 0.0)


def local_states(keys, values, decay):
    tokens, channels = keys.shape
    width = values.shape[1]
    blocks = tokens // BLK
    return vmem_call(
        local_state_body,
        [
            jax.ShapeDtypeStruct((tokens, channels), F32),
            jax.ShapeDtypeStruct((blocks, channels), F32),
            jax.ShapeDtypeStruct((blocks, width, channels), F32),
            jax.ShapeDtypeStruct((width + 8, channels), F32),
        ],
    )(keys, values, decay)


def forward_body(index, queries, keys, values, cumulative, ends, gain, *refs):
    *pieces, inside_0, inside_1, book_0, book_1, mixed, states, scores, book = refs
    blocks = gain.shape[0]
    far, _, (near, _, _) = opened(pieces, index[0], book)
    own = slice(BOOK_OWN + 1, BOOK_OWN + 2)
    start = inside_0[...] + book_0[own, :] * (inside_1[...] + book_1[own, :] * weighted(far, near))
    scale = queries.shape[1] ** (-0.5)
    causal = grid_of((BLK, BLK), 0) >= grid_of((BLK, BLK), 1)
    state = start
    for c in range(blocks):
        rows = slice(c * BLK, (c + 1) * BLK)
        cum = cumulative[rows, :]
        middle = cum[BLK // 2 - 1 : BLK // 2, :]
        query = queries[rows, :].astype(F32) * scale
        near_q = halves(query * jnp.exp(cum - middle))
        near_k = halves(keys[rows, :].astype(F32) * jnp.exp(middle - cum))
        score = jnp.where(causal, dot_parts(near_q, near_k, NT), 0.0)
        scores[rows, :] = score
        states[c] = state
        out = dot_parts(halves(query * jnp.exp(cum)), halves(state), NT)
        out = out + dot_parts(halves(score), (values[rows, :],), NN)
        mixed[rows, :] = out.astype(BF16)
        state = state * jnp.exp(ends[c : c + 1, :]) + gain[c]
    states[blocks] = state


def forward(queries, keys, values, cumulative, ends, gain, before):
    pieces, index, insides, books = before
    tokens, channels = keys.shape
    width = values.shape[1]
    blocks = tokens // BLK
    operands = (*pieces, *insides, *books)
    return vmem_call(
        forward_body,
        [
            jax.ShapeDtypeStruct((tokens, width), BF16),
            jax.ShapeDtypeStruct((blocks + 1, width, channels), F32),
            jax.ShapeDtypeStruct((tokens, BLK), F32),
            jax.ShapeDtypeStruct((BOOK_ROWS, channels), F32),
        ],
        in_specs=[SMEM] + [VMEM] * (6 + len(operands)),
    )(index, queries, keys, values, cumulative, ends, gain, *operands)


def cotangent_body(place, a, b, c, d, w_out, queries, cumulative, ends, d_mixed, back, own):
    blocks = back.shape[0]
    scale = queries.shape[1] ** (-0.5)
    quarter = a.shape[1]
    total = None
    for tile, offset in ((a, 0), (b, 3), (c, 1), (d, 2)):
        start = pl.multiple_of(((place[0] + offset) & 3) * quarter, quarter)
        term = dot(tile[...], w_out[pl.ds(start, quarter), :], NN)
        total = term if total is None else total + term
    d_mixed[...] = total
    for c in range(blocks):
        rows = slice(c * BLK, (c + 1) * BLK)
        query = queries[rows, :].astype(F32) * (scale * jnp.exp(cumulative[rows, :]))
        back[c] = dot_parts(halves(d_mixed[rows, :]), halves(query), TN)
    state = back[blocks - 1]
    for c in reversed(range(blocks - 1)):
        state = state * jnp.exp(ends[c : c + 1, :]) + back[c]
    own[...] = state.astype(BF16)


def cotangents(place, tiles, w_out, queries, cumulative, ends):
    tokens, channels = queries.shape
    width = w_out.shape[1]
    blocks = tokens // BLK
    return vmem_call(
        cotangent_body,
        [
            jax.ShapeDtypeStruct((tokens, width), F32),
            jax.ShapeDtypeStruct((blocks, width, channels), F32),
            jax.ShapeDtypeStruct((width, channels), BF16),
        ],
        in_specs=[SMEM] + [VMEM] * 8,
    )(place, *tiles, w_out, queries, cumulative, ends)


def projection_body(place, a, b, c, d, mixed, out):
    quarter = a.shape[1]
    for tile, offset in ((a, 0), (b, 3), (c, 1), (d, 2)):
        start = pl.multiple_of(((place[0] + offset) & 3) * quarter, quarter)
        out[pl.ds(start, quarter), :] = dot(tile[...], mixed[...], TN).astype(BF16)


def projection(place, tiles, mixed):
    return vmem_call(
        projection_body,
        jax.ShapeDtypeStruct((4 * tiles[0].shape[1], mixed.shape[1]), BF16),
        in_specs=[SMEM] + [VMEM] * 5,
    )(place, *tiles, mixed)


def inside_body(queries, keys, values, cumulative, scores, d_mixed, to_q, to_k, to_v):
    blocks = queries.shape[0] // BLK
    scale = queries.shape[1] ** (-0.5)
    causal = grid_of((BLK, BLK), 0) >= grid_of((BLK, BLK), 1)
    for c in range(blocks):
        rows = slice(c * BLK, (c + 1) * BLK)
        cum = cumulative[rows, :]
        middle = cum[BLK // 2 - 1 : BLK // 2, :]
        rising, falling = jnp.exp(cum - middle), jnp.exp(middle - cum)
        near_q = halves(queries[rows, :].astype(F32) * scale * rising)
        near_k = halves(keys[rows, :].astype(F32) * falling)
        incoming = halves(d_mixed[rows, :])
        d_score = jnp.where(causal, dot_parts(incoming, (values[rows, :],), NT), 0.0)
        d_score = halves(d_score)
        to_q[rows, :] = rising * dot_parts(d_score, near_k, NN)
        to_k[rows, :] = falling * dot_parts(d_score, near_q, TN)
        to_v[rows, :] = dot_parts(halves(scores[rows, :]), incoming, TN)


def inside_blocks(queries, keys, values, cumulative, scores, d_mixed):
    tokens, channels = queries.shape
    return vmem_call(
        inside_body,
        [
            jax.ShapeDtypeStruct((tokens, channels), F32),
            jax.ShapeDtypeStruct((tokens, channels), F32),
            jax.ShapeDtypeStruct(values.shape, F32),
        ],
    )(queries, keys, values, cumulative, scores, d_mixed)


def backward_body(
    queries, keys, values, cumulative, ends, d_mixed, states, back, to_q, to_k, to_v, *refs
):
    *pieces, inside_0, inside_1, book_0, book_1, book, grad_q, grad_k, grad_v, grad_g = refs
    own = slice(BOOK_OWN, BOOK_OWN + 1)
    later = weighted([x[...] for x in pieces], [book[k : k + 1, :] for k in range(len(pieces))])
    later = inside_0[...] + book_0[own, :] * (inside_1[...] + book_1[own, :] * later)
    blocks = back.shape[0]
    scale = queries.shape[1] ** (-0.5)
    upper = triangle(True)
    after = later
    carry = jnp.sum(after * states[blocks], axis=0, keepdims=True)
    for c in reversed(range(blocks)):
        rows = slice(c * BLK, (c + 1) * BLK)
        cum = cumulative[rows, :]
        end = ends[c : c + 1, :]
        fading = jnp.exp(end - cum)
        key = keys[rows, :].astype(F32)
        after_parts = halves(after)
        d_query = jnp.exp(cum) * dot_parts(halves(d_mixed[rows, :]), halves(states[c]), NN)
        d_query = (d_query + to_q[rows, :]) * scale
        d_key = fading * dot_parts((values[rows, :],), after_parts, NN) + to_k[rows, :]
        d_value = dot_parts(halves(key * fading), after_parts, NT) + to_v[rows, :]
        grad_q[rows, :] = d_query.astype(BF16)
        grad_k[rows, :] = d_key.astype(BF16)
        grad_v[rows, :] = d_value.astype(BF16)
        change = queries[rows, :].astype(F32) * d_query - key * d_key
        summed = dot_exact(upper, change, NN) + carry
        grad_g[rows, :] = summed
        carry = summed[0:1, :]
        after = after * jnp.exp(end) + back[c]


def backward(
    queries, keys, values, cumulative, ends, d_mixed, states, back, inside, after, books
):
    pieces, insides = after
    return vmem_call(
        backward_body,
        [
            jax.ShapeDtypeStruct(queries.shape, BF16),
            jax.ShapeDtypeStruct(keys.shape, BF16),
            jax.ShapeDtypeStruct(values.shape, BF16),
            jax.ShapeDtypeStruct(queries.shape, F32),
        ],
    )(queries, keys, values, cumulative, ends, d_mixed, states, back, *inside, *pieces, *insides, *books)


BOOK_WHOLE, BOOK_OWN, BOOK_ROWS = 8, 16, 24


def stage_weights(logs, index, reverse):
    count = len(logs)
    place = [lax.rem(index - k + count, count) for k in range(count)]
    none = jnp.zeros_like(logs[0])

    def summed(condition):
        total = none
        for log, at in zip(logs, place):
            total = total + jnp.where(condition(at), log, 0.0)
        return total

    if reverse:
        passed = lambda at: at > index
        inner = lambda start: lambda at: (at < start) & (at > index)
        outer = lambda start: lambda at: at < start
    else:
        passed = lambda at: at < index
        inner = lambda start: lambda at: (at > start) & (at < index)
        outer = lambda start: lambda at: at > start
    near = [jnp.where(passed(at), jnp.exp(summed(inner(at))), 0.0) for at in place]
    whole = [jnp.exp(summed(outer(at))) for at in place]
    return near, whole, jnp.exp(summed(passed))


def weighted(pieces, weights):
    total = pieces[0].astype(F32) * weights[0]
    for piece, weight in zip(pieces[1:], weights[1:]):
        total = total + piece.astype(F32) * weight
    return total


def opened(pieces, index, book):
    width = pieces[0].shape[0] - 8
    logs = [piece[width : width + 1, :] for piece in pieces]
    states = [piece[0:width, :] for piece in pieces]
    near, whole, own = stage_weights(logs, index, True)
    for k in range(len(logs)):
        book[k : k + 1, :] = near[k]
        book[BOOK_WHOLE + k : BOOK_WHOLE + k + 1, :] = whole[k]
    book[BOOK_OWN : BOOK_OWN + 1, :] = own
    return states, logs, stage_weights(logs, index, False)


def stage_before_body(index, *refs):
    *pieces, inside, payload, book = refs
    states, logs, (near, whole, own) = opened(pieces, index[0], book)
    width = inside.shape[0]
    book[BOOK_OWN + 1 : BOOK_OWN + 2, :] = own
    inside[...] = weighted(states, near)
    payload[0:width, :] = weighted(states, whole)
    total = logs[0]
    for log in logs[1:]:
        total = total + log
    payload[width:, :] = jnp.where(grid_of((8, total.shape[1]), 0) == 0, total, 0.0)


def stage_after_body(*refs):
    *pieces, book, inside, total = refs
    pieces = [piece[...] for piece in pieces]
    inside[...] = weighted(pieces, [book[k : k + 1, :] for k in range(len(pieces))])
    wholes = [book[BOOK_WHOLE + k : BOOK_WHOLE + k + 1, :] for k in range(len(pieces))]
    total[...] = weighted(pieces, wholes).astype(BF16)


def everyone(x, axis):
    return [x] + [shifted(x, axis, k) for k in range(1, lax.axis_size(axis))]


def states_before(payload):
    rows, channels = payload.shape
    insides, books = [], []
    for axis in reversed(SP):
        pieces = everyone(payload, axis)
        index = lax.axis_index(axis).reshape(1)
        if axis == SP[0]:
            return pieces, index, insides, books
        inside, payload, book = vmem_call(
            stage_before_body,
            [
                jax.ShapeDtypeStruct((rows - 8, channels), F32),
                jax.ShapeDtypeStruct((rows, channels), F32),
                jax.ShapeDtypeStruct((BOOK_ROWS, channels), F32),
            ],
            in_specs=[SMEM] + [VMEM] * len(pieces),
        )(index, *pieces)
        insides.append(inside)
        books.append(book)


def states_after(part, books):
    insides = []
    for axis, book in zip(reversed(SP), books):
        pieces = everyone(part, axis)
        if axis == SP[0]:
            return pieces, insides
        inside, part = vmem_call(
            stage_after_body,
            [jax.ShapeDtypeStruct(part.shape, F32), jax.ShapeDtypeStruct(part.shape, BF16)],
        )(*pieces, book)
        insides.append(inside)


def local(
    d_out,
    route_expert,
    route_weight,
    expert_inputs,
    w_gate,
    w_up,
    w_down,
    w_out,
    queries,
    keys,
    values,
    log_decay,
):
    tok_rows, model_width = d_out.shape
    experts = lax.axis_size(SP)
    capacity = expert_inputs.shape[1] // experts
    cut = capacity * 2 // 3 // PAD * PAD
    tail = -(-(capacity - cut) // PAD) * PAD
    quarter = model_width // lax.axis_size("tp")
    place = lax.axis_index("tp").reshape(1)
    chosen, weight = route_expert.T, route_weight.T

    def exchanged(box, stride):
        box = box.reshape(experts, stride, box.shape[1])
        box = lax.all_to_all(box, SP, split_axis=0, concat_axis=0, tiled=True)
        return box.reshape(experts * stride, box.shape[2])

    outbox_a, pick_a, ranks = vmem_call(
        functools.partial(route_body, experts=experts, most=cut, stride=cut),
        [
            jax.ShapeDtypeStruct((experts * cut, model_width), BF16),
            jax.ShapeDtypeStruct((experts * cut, tok_rows), BF16),
            jax.ShapeDtypeStruct((2, tok_rows), jnp.int32),
        ],
        mebibytes=20,
    )(d_out, chosen, weight)
    routed_a = exchanged(outbox_a, cut)
    outbox_b, pick_b = vmem_call(
        functools.partial(refill_body, least=cut, most=capacity, stride=tail),
        [
            jax.ShapeDtypeStruct((experts * tail, model_width), BF16),
            jax.ShapeDtypeStruct((experts * tail, tok_rows), BF16),
        ],
        mebibytes=20,
    )(d_out, chosen, weight, ranks)
    routed_b = exchanged(outbox_b, tail)

    gate_w, up_w, down_w = w_gate[0].T, w_up[0].T, w_down[0]
    rows_in, active, slope, hidden = expert_forward(
        expert_inputs[0], gate_w, up_w, experts, capacity, cut, tail
    )

    query, key, value, decay = queries[:, 0], keys[:, 0], values[:, 0], log_decay[:, 0]
    cumulative, ends, gain, produced = local_states(key, value, decay)
    before = states_before(produced)
    mixed, states, scores, book = forward(query, key, value, cumulative, ends, gain, before)
    books = (*before[3], book)

    weights = (active, slope, down_w, gate_w, up_w)
    *whole, keep_a, send_a, keep_b, send_b = expert_cotangents(
        place, routed_a, *weights, 0, ()
    )
    parts_a = (keep_a, send_a, keep_b, send_b)
    routed, d_gate, d_up, *parts_b = expert_cotangents(
        place, routed_b, *weights, experts * cut, whole
    )
    returned_a = exchanged(summed_over_tp(*parts_a), cut)
    returned_b = exchanged(summed_over_tp(*parts_b), tail)
    grad_gate = dot(d_gate, rows_in, TN).astype(BF16).T
    grad_up = dot(d_up, rows_in, TN).astype(BF16).T
    grad_down = dot(hidden, routed, TN).astype(BF16)

    own_cols = lax.dynamic_slice_in_dim(d_out, place[0] * quarter, quarter, 1)
    picked = own_cols.astype(F32) + dot(pick_a, returned_a, TN)
    picked = picked + dot(pick_b, returned_b, TN)
    tiles = gathered_ring(picked.astype(BF16))

    d_mixed, back, own_term = cotangents(place, tiles, w_out, query, cumulative, ends)
    after = states_after(own_term, books)
    inside = inside_blocks(query, key, value, cumulative, scores, d_mixed)
    grad_q, grad_k, grad_v, grad_g = backward(
        query, key, value, cumulative, ends, d_mixed, states, back, inside, after, books
    )

    proj = projection(place, tiles, mixed).reshape(experts, model_width // experts, -1)
    proj = lax.all_to_all(proj, SP, 0, 0, tiled=True)
    grad_proj = jnp.sum(proj.astype(F32), axis=0)
    return (
        grad_gate[None],
        grad_up[None],
        grad_down[None],
        grad_proj,
        grad_q[:, None],
        grad_k[:, None],
        grad_v[:, None],
        grad_g[:, None],
    )


def solution(mesh):
    finer = Mesh(mesh.devices.reshape(4, 4, 2, mesh.shape["tp"]), ("sp_0", "sp_1", "sp_2", "tp"))
    return jax.shard_map(
        local,
        mesh=finer,
        in_specs=(
            P(SP, None),
            P(SP, None),
            P(SP, None),
            P(SP, None, None),
            P(SP, None, "tp"),
            P(SP, None, "tp"),
            P(SP, "tp", None),
            P(None, "tp"),
            P(SP, "tp", None),
            P(SP, "tp", None),
            P(SP, "tp", None),
            P(SP, "tp", None),
        ),
        out_specs=(
            P(SP, None, "tp"),
            P(SP, None, "tp"),
            P(SP, "tp", None),
            P(SP, "tp"),
            P(SP, "tp", None),
            P(SP, "tp", None),
            P(SP, "tp", None),
            P(SP, "tp", None),
        ),
        check_vma=False,
    )
```

```python
import functools

import jax
import jax.numpy as jnp
from jax import lax
from jax.experimental import pallas as pl
from jax.experimental.pallas import tpu as pltpu
from jax.sharding import Mesh
from jax.sharding import PartitionSpec as P


BLK = 64
PAD = 8
SP = ("sp_0", "sp_1", "sp_2")
F32 = jnp.float32
BF16 = jnp.bfloat16

NN = (((1,), (0,)), ((), ()))
NT = (((1,), (1,)), ((), ()))
TN = (((0,), (0,)), ((), ()))


def dot(a, b, dims):
    return lax.dot_general(a, b, dims, preferred_element_type=F32)


def halves(x):
    high = x.astype(BF16)
    return high, (x - high.astype(F32)).astype(BF16)


def thirds(x):
    high = x.astype(BF16)
    rest = x - high.astype(F32)
    middle = rest.astype(BF16)
    return high, middle, (rest - middle.astype(F32)).astype(BF16)


def dot_parts(a, b, dims):
    out = dot(a[0], b[0], dims)
    if len(a) > 1:
        out = out + dot(a[1], b[0], dims)
    if len(b) > 1:
        out = out + dot(a[0], b[1], dims)
    return out


def dot_exact(mask, x, dims):
    high, middle, low = thirds(x)
    return dot(mask, high, dims) + (dot(mask, middle, dims) + dot(mask, low, dims))


def grid_of(shape, dim):
    return lax.broadcasted_iota(jnp.int32, shape, dim)


SMEM = pl.BlockSpec(memory_space=pltpu.SMEM)
VMEM = pl.BlockSpec(memory_space=pltpu.VMEM)


def limit(mebibytes):
    return pltpu.CompilerParams(vmem_limit_bytes=mebibytes * 1024 * 1024)


def vmem_call(kernel, outs, mebibytes=12, **options):
    return pl.pallas_call(kernel, out_shape=outs, compiler_params=limit(mebibytes), **options)


def fill_outbox(rows, weight, slot_a, slot_b, outbox):
    weights_a = jnp.concatenate(thirds(weight[0:1, :]), axis=0)
    weights_b = jnp.concatenate(thirds(weight[1:2, :]), axis=0)
    step = 256
    for start in range(0, outbox.shape[0], step):
        slot = grid_of((step, rows.shape[0]), 0) + start
        one_a = jnp.where(slot == slot_a, 1.0, 0.0).astype(BF16)
        one_b = jnp.where(slot == slot_b, 1.0, 0.0).astype(BF16)
        factor = dot(one_a, weights_a, NT) + dot(one_b, weights_b, NT)
        factor = jnp.sum(factor, axis=1, keepdims=True)
        outbox[start : start + step, :] = (dot(one_a + one_b, rows, NN) * factor).astype(BF16)


def slots_of(chosen, ranks, least, most, stride):
    inside = (ranks >= least) & (ranks < most)
    return jnp.where(inside, chosen * stride + ranks - least, -1)


def route_body(place, d_out, chosen, weight, outbox, ranks, *, experts, most):
    tokens = d_out.shape[0]
    first, second = chosen[0:1, :], chosen[1:2, :]
    ids = grid_of((experts, tokens), 0)
    is_first, is_second = ids == first, ids == second
    named = jnp.where(is_first | is_second, 1.0, 0.0).astype(BF16)
    earlier = jnp.where(
        grid_of((tokens, tokens), 0) < grid_of((tokens, tokens), 1), 1.0, 0.0
    ).astype(BF16)
    before = dot(named, earlier, NN)
    rank_a = jnp.sum(jnp.where(is_first, before, 0.0), axis=0, keepdims=True).astype(jnp.int32)
    rank_b = jnp.sum(jnp.where(is_second, before, 0.0), axis=0, keepdims=True).astype(jnp.int32)
    ranks[0:1, :] = rank_a
    ranks[1:2, :] = rank_b
    slot_a = slots_of(first, rank_a, 0, most, most)
    slot_b = slots_of(second, rank_b, 0, most, most)
    width = outbox.shape[1]
    rows = d_out[:, pl.ds(pl.multiple_of(place[0] * width, width), width)]
    fill_outbox(rows, weight, slot_a, slot_b, outbox)


def refill_body(d_out, chosen, weight, ranks, outbox, pick, *, least, most, tail):
    first, second = chosen[0:1, :], chosen[1:2, :]
    rank_a, rank_b = ranks[0:1, :], ranks[1:2, :]
    slot_a = slots_of(first, rank_a, least, most, tail)
    slot_b = slots_of(second, rank_b, least, most, tail)
    fill_outbox(d_out[...], weight, slot_a, slot_b, outbox)
    slot_a = first * (least + tail) + rank_a
    slot_b = second * (least + tail) + rank_b
    step = 256
    for start in range(0, pick.shape[0], step):
        slot = grid_of((step, pick.shape[1]), 0) + start
        found = (slot == slot_a) | (slot == slot_b)
        pick[start : start + step, :] = jnp.where(found, 1.0, 0.0).astype(BF16)


def slot_order(group, capacity, cut, tail):
    def placed(rows, stride, width, first):
        row, col = grid_of((rows, group * capacity), 0), grid_of((rows, group * capacity), 1)
        found = row < 0
        for source in range(group):
            start = source * stride
            here = (row >= start) & (row < start + width)
            found = found | (here & (col == row + (source * capacity + first - start)))
        return jnp.where(found, 1.0, 0.0).astype(BF16)

    return placed(group * cut, cut, cut, 0), placed(group * tail, tail, capacity - cut, cut)


def expert_forward_body(
    inputs, gate_w, up_w, rows_in, active, slope, hidden, *, experts, capacity, cut, tail
):
    group = 8
    orders = slot_order(group, capacity, cut, tail)
    for step in range(experts // group):
        block = inputs[step * group * capacity : (step + 1) * group * capacity, :]
        for order, start in zip(orders, (step * group * cut, experts * cut + step * group * tail)):
            rows_in[start : start + order.shape[0], :] = dot(order, block, NN).astype(BF16)
    units = gate_w.shape[0]
    step = rows_in.shape[0] // 2
    for first in range(0, units, 256):
        cols = slice(first, min(first + 256, units))
        for start in range(0, rows_in.shape[0], step):
            rows = slice(start, start + step)
            gate = dot(rows_in[rows, :], gate_w[cols, :], NT)
            up = dot(rows_in[rows, :], up_w[cols, :], NT)
            sigmoid = 1.0 / (1.0 + jnp.exp(-gate))
            silu = gate * sigmoid
            hidden[rows, cols] = (silu * up).astype(BF16)
            active[rows, cols] = silu.astype(BF16)
            slope[rows, cols] = (up * sigmoid * (1.0 + gate * (1.0 - sigmoid))).astype(BF16)


def expert_forward(inputs, gate_w, up_w, experts, capacity, cut, tail):
    slots = experts * (cut + tail)
    units = gate_w.shape[0]
    return vmem_call(
        functools.partial(
            expert_forward_body, experts=experts, capacity=capacity, cut=cut, tail=tail
        ),
        [jax.ShapeDtypeStruct((slots, inputs.shape[1]), BF16)]
        + [jax.ShapeDtypeStruct((slots, units), BF16)] * 3,
        mebibytes=56,
    )(inputs, gate_w, up_w)


def expert_body(place, *refs, tiles):
    routed, (active, slope, down_w, gate_w, up_w) = refs[:tiles], refs[tiles : tiles + 5]
    routed_out, d_gate, d_up, keep_a, send_a, keep_b, send_b = refs[-11:-4]
    down_v, gate_v, up_v, loaded = refs[-4:]
    copies = [
        pltpu.make_async_copy(source, target, loaded.at[i])
        for i, (source, target) in enumerate(((down_w, down_v), (gate_w, gate_v), (up_w, up_v)))
    ]

    @pl.when(pl.program_id(0) == 0)
    def _():
        for copy in copies:
            copy.start()
        copies[0].wait()

    d_hidden = 0.0
    for k, tile in enumerate(routed):
        wide = tile.shape[1]
        cols = slice(None)
        if tiles > 1:
            cols = pl.ds(pl.multiple_of(((place[0] + tiles - k) & (tiles - 1)) * wide, wide), wide)
        routed_out[:, cols] = tile[...]
        d_hidden = d_hidden + dot(tile[...], down_v[:, cols], NT)

    @pl.when(pl.program_id(0) == 0)
    def _():
        copies[1].wait()
        copies[2].wait()

    to_gate = (d_hidden * slope[...].astype(F32)).astype(BF16)
    to_up = (d_hidden * active[...].astype(F32)).astype(BF16)
    d_gate[...] = to_gate
    d_up[...] = to_up
    half = keep_a.shape[2]
    homes = (
        ((keep_a, 0), (keep_b, 0)),
        ((send_a, 0), (keep_b, 1)),
        ((send_a, 1), (send_b, 1)),
        ((keep_a, 1), (send_b, 0)),
    )
    for k, (home_a, home_b) in enumerate(homes):
        start = pl.multiple_of((place[0] ^ k) * (2 * half), 2 * half)
        cols = pl.ds(start, 2 * half)
        term = dot(to_gate, gate_v[:, cols], NN) + dot(to_up, up_v[:, cols], NN)
        term = term.astype(BF16)
        home_a[0][home_a[1]] = term[:, :half]
        home_b[0][home_b[1]] = term[:, half:]


def expert_cotangents(place, routed, active, slope, down_w, gate_w, up_w, first_row, earlier):
    rows, wide = routed[0].shape
    tiles = len(routed)
    units, width = down_w.shape
    step = 256
    half = width // 8
    skipped = first_row // step
    by_row = lambda i, *_: (i, 0)
    later_row = lambda i, *_: (i + skipped, 0)
    in_specs = [pl.BlockSpec((step, wide), by_row)] * tiles + [
        pl.BlockSpec((step, units), later_row),
        pl.BlockSpec((step, units), later_row),
    ]
    in_specs += [pl.BlockSpec(memory_space=pl.ANY)] * (3 + len(earlier))
    pair = pl.BlockSpec((2, step, half), lambda i, *_: (0, i, 0))
    return pl.pallas_call(
        functools.partial(expert_body, tiles=tiles),
        grid_spec=pltpu.PrefetchScalarGridSpec(
            num_scalar_prefetch=1,
            grid=(rows // step,),
            in_specs=in_specs,
            out_specs=[pl.BlockSpec((step, width), later_row)]
            + [pl.BlockSpec((step, units), later_row)] * 2
            + [pair] * 4,
            scratch_shapes=[pltpu.VMEM((units, width), BF16)] * 3
            + [pltpu.SemaphoreType.DMA((3,))],
        ),
        out_shape=[jax.ShapeDtypeStruct((active.shape[0], width), BF16)]
        + [jax.ShapeDtypeStruct(active.shape, BF16)] * 2
        + [jax.ShapeDtypeStruct((2, rows, half), BF16)] * 4,
        input_output_aliases={6 + tiles + i: i for i in range(len(earlier))},
        compiler_params=limit(56),
    )(place, *routed, active, slope, down_w, gate_w, up_w, *earlier)


def weight_grads_body(d_gate, d_up, rows_in, for_gate, for_up):
    rows = rows_in[...]
    for_gate[...] = dot(d_gate[...], rows, TN).astype(BF16)
    for_up[...] = dot(d_up[...], rows, TN).astype(BF16)


def weight_grads(d_gate, d_up, rows_in):
    rows, width = rows_in.shape
    units = d_gate.shape[1]
    step = 512
    whole = pl.BlockSpec((rows, units), lambda i: (0, 0))
    by_col = lambda i: (0, i)
    return pl.pallas_call(
        weight_grads_body,
        grid=(width // step,),
        in_specs=[whole, whole, pl.BlockSpec((rows, step), by_col)],
        out_specs=[pl.BlockSpec((units, step), by_col)] * 2,
        out_shape=[jax.ShapeDtypeStruct((units, width), BF16)] * 2,
        compiler_params=limit(48),
    )(d_gate, d_up, rows_in)


def swapped(x, flip):
    count = lax.axis_size("tp")
    return lax.ppermute(x, "tp", [(i, i ^ flip) for i in range(count)])


def plus(*terms):
    total = terms[0].astype(F32)
    for term in terms[1:]:
        total = total + term.astype(F32)
    return total.astype(BF16)


def final_sum_body(keep_a, got_a, last_a, keep_b, got_b, last_b, out):
    half = keep_a.shape[2]
    for start, keep, got, last in ((0, keep_a, got_a, last_a), (half, keep_b, got_b, last_b)):
        total = keep[0].astype(F32) + got[0].astype(F32) + last[...].astype(F32)
        out[:, start : start + half] = total.astype(BF16)


def final_sum(keep_a, got_a, last_a, keep_b, got_b, last_b):
    _, rows, half = keep_a.shape
    first = pl.BlockSpec((1, rows, half), lambda i: (0, 0, 0))
    whole = pl.BlockSpec((rows, half), lambda i: (0, 0))
    return pl.pallas_call(
        final_sum_body,
        grid=(1,),
        in_specs=[first, first, whole] * 2,
        out_specs=pl.BlockSpec((rows, 2 * half), lambda i: (0, 0)),
        out_shape=jax.ShapeDtypeStruct((rows, 2 * half), BF16),
        compiler_params=limit(12),
    )(keep_a, got_a, last_a, keep_b, got_b, last_b)


def summed_over_tp(keep_a, send_a, keep_b, send_b):
    got_a = swapped(send_a, 1)
    got_b = swapped(send_b, 3)
    last_a, last_b = plus(keep_a[1], got_a[1]), plus(keep_b[1], got_b[1])
    last_a = swapped(last_a, 3)
    last_b = swapped(last_b, 1)
    return final_sum(keep_a, got_a, last_a, keep_b, got_b, last_b)


def shifted(x, axis, by):
    count = lax.axis_size(axis)
    return lax.ppermute(x, axis, [(i, (i + by) % count) for i in range(count)])


def gathered_ring(x):
    half = x.shape[0] // 2
    below = shifted(x, "tp", 1)
    above = shifted(x, "tp", -1)
    across = jnp.concatenate(
        [shifted(below[:half], "tp", 1), shifted(above[half:], "tp", -1)], axis=0
    )
    return x, below, above, across


def triangle(reverse):
    row, col = grid_of((BLK, BLK), 0), grid_of((BLK, BLK), 1)
    return jnp.where((row <= col) if reverse else (row >= col), 1.0, 0.0).astype(BF16)


def local_state_body(keys, values, decay, cumulative, ends, gain, produced):
    blocks = gain.shape[0]
    lower = triangle(False)
    for c in range(blocks):
        rows = slice(c * BLK, (c + 1) * BLK)
        cum = dot_exact(lower, decay[rows, :], NN)
        cumulative[rows, :] = cum
        end = cum[BLK - 1 : BLK, :]
        ends[c : c + 1, :] = end
        faded = keys[rows, :].astype(F32) * jnp.exp(end - cum)
        gain[c] = dot_parts((values[rows, :],), halves(faded), TN)
    state = gain[0]
    total = ends[0:1, :]
    for c in range(1, blocks):
        state = state * jnp.exp(ends[c : c + 1, :]) + gain[c]
        total = total + ends[c : c + 1, :]
    width = state.shape[0]
    produced[0:width, :] = state
    spare = produced.shape[0] - width
    produced[width:, :] = jnp.where(grid_of((spare, total.shape[1]), 0) == 0, total, 0.0)


def local_states(keys, values, decay):
    tokens, channels = keys.shape
    width = values.shape[1]
    blocks = tokens // BLK
    return vmem_call(
        local_state_body,
        [
            jax.ShapeDtypeStruct((tokens, channels), F32),
            jax.ShapeDtypeStruct((blocks, channels), F32),
            jax.ShapeDtypeStruct((blocks, width, channels), F32),
            jax.ShapeDtypeStruct((width + 8, channels), F32),
        ],
    )(keys, values, decay)


def forward_body(index, queries, keys, values, cumulative, ends, gain, *refs):
    *pieces, inside_0, inside_1, book_0, book_1, mixed, states, scores, book = refs
    blocks = gain.shape[0]
    far, _, (near, _, _) = opened(pieces, index[0], book)
    own = slice(BOOK_OWN + 1, BOOK_OWN + 2)
    start = inside_0[...] + book_0[own, :] * (inside_1[...] + book_1[own, :] * weighted(far, near))
    scale = queries.shape[1] ** (-0.5)
    causal = grid_of((BLK, BLK), 0) >= grid_of((BLK, BLK), 1)
    state = start
    for c in range(blocks):
        rows = slice(c * BLK, (c + 1) * BLK)
        cum = cumulative[rows, :]
        middle = cum[BLK // 2 - 1 : BLK // 2, :]
        query = queries[rows, :].astype(F32) * scale
        near_q = halves(query * jnp.exp(cum - middle))
        near_k = halves(keys[rows, :].astype(F32) * jnp.exp(middle - cum))
        score = jnp.where(causal, dot_parts(near_q, near_k, NT), 0.0)
        scores[rows, :] = score
        states[c] = state
        out = dot_parts(halves(query * jnp.exp(cum)), halves(state), NT)
        out = out + dot_parts(halves(score), (values[rows, :],), NN)
        mixed[rows, :] = out.astype(BF16)
        state = state * jnp.exp(ends[c : c + 1, :]) + gain[c]
    states[blocks] = state


def forward(queries, keys, values, cumulative, ends, gain, before):
    pieces, index, insides, books = before
    tokens, channels = keys.shape
    width = values.shape[1]
    blocks = tokens // BLK
    operands = (*pieces, *insides, *books)
    return vmem_call(
        forward_body,
        [
            jax.ShapeDtypeStruct((tokens, width), BF16),
            jax.ShapeDtypeStruct((blocks + 1, width, channels), F32),
            jax.ShapeDtypeStruct((tokens, BLK), F32),
            jax.ShapeDtypeStruct((BOOK_ROWS, channels), F32),
        ],
        in_specs=[SMEM] + [VMEM] * (6 + len(operands)),
    )(index, queries, keys, values, cumulative, ends, gain, *operands)


def cotangent_body(place, a, b, c, d, w_out, queries, cumulative, ends, d_mixed, back, own):
    blocks = back.shape[0]
    scale = queries.shape[1] ** (-0.5)
    quarter = a.shape[1]
    total = None
    for tile, offset in ((a, 0), (b, 3), (c, 1), (d, 2)):
        start = pl.multiple_of(((place[0] + offset) & 3) * quarter, quarter)
        term = dot(tile[...], w_out[pl.ds(start, quarter), :], NN)
        total = term if total is None else total + term
    d_mixed[...] = total
    for c in range(blocks):
        rows = slice(c * BLK, (c + 1) * BLK)
        query = queries[rows, :].astype(F32) * (scale * jnp.exp(cumulative[rows, :]))
        back[c] = dot_parts(halves(d_mixed[rows, :]), halves(query), TN)
    state = back[blocks - 1]
    for c in reversed(range(blocks - 1)):
        state = state * jnp.exp(ends[c : c + 1, :]) + back[c]
    own[...] = state.astype(BF16)


def cotangents(place, tiles, w_out, queries, cumulative, ends):
    tokens, channels = queries.shape
    width = w_out.shape[1]
    blocks = tokens // BLK
    return vmem_call(
        cotangent_body,
        [
            jax.ShapeDtypeStruct((tokens, width), F32),
            jax.ShapeDtypeStruct((blocks, width, channels), F32),
            jax.ShapeDtypeStruct((width, channels), BF16),
        ],
        in_specs=[SMEM] + [VMEM] * 8,
    )(place, *tiles, w_out, queries, cumulative, ends)


def projection_body(place, a, b, c, d, mixed, out):
    quarter = a.shape[1]
    for tile, offset in ((a, 0), (b, 3), (c, 1), (d, 2)):
        start = pl.multiple_of(((place[0] + offset) & 3) * quarter, quarter)
        out[pl.ds(start, quarter), :] = dot(tile[...], mixed[...], TN).astype(BF16)


def projection(place, tiles, mixed):
    return vmem_call(
        projection_body,
        jax.ShapeDtypeStruct((4 * tiles[0].shape[1], mixed.shape[1]), BF16),
        in_specs=[SMEM] + [VMEM] * 5,
    )(place, *tiles, mixed)


def inside_body(queries, keys, values, cumulative, scores, d_mixed, to_q, to_k, to_v):
    blocks = queries.shape[0] // BLK
    scale = queries.shape[1] ** (-0.5)
    causal = grid_of((BLK, BLK), 0) >= grid_of((BLK, BLK), 1)
    for c in range(blocks):
        rows = slice(c * BLK, (c + 1) * BLK)
        cum = cumulative[rows, :]
        middle = cum[BLK // 2 - 1 : BLK // 2, :]
        rising, falling = jnp.exp(cum - middle), jnp.exp(middle - cum)
        near_q = halves(queries[rows, :].astype(F32) * scale * rising)
        near_k = halves(keys[rows, :].astype(F32) * falling)
        incoming = halves(d_mixed[rows, :])
        d_score = jnp.where(causal, dot_parts(incoming, (values[rows, :],), NT), 0.0)
        d_score = halves(d_score)
        to_q[rows, :] = rising * dot_parts(d_score, near_k, NN)
        to_k[rows, :] = falling * dot_parts(d_score, near_q, TN)
        to_v[rows, :] = dot_parts(halves(scores[rows, :]), incoming, TN)


def inside_blocks(queries, keys, values, cumulative, scores, d_mixed):
    tokens, channels = queries.shape
    return vmem_call(
        inside_body,
        [
            jax.ShapeDtypeStruct((tokens, channels), F32),
            jax.ShapeDtypeStruct((tokens, channels), F32),
            jax.ShapeDtypeStruct(values.shape, F32),
        ],
    )(queries, keys, values, cumulative, scores, d_mixed)


def backward_body(
    queries, keys, values, cumulative, ends, d_mixed, states, back, to_q, to_k, to_v, *refs
):
    *pieces, inside_0, inside_1, book_0, book_1, book, grad_q, grad_k, grad_v, grad_g = refs
    own = slice(BOOK_OWN, BOOK_OWN + 1)
    later = weighted([x[...] for x in pieces], [book[k : k + 1, :] for k in range(len(pieces))])
    later = inside_0[...] + book_0[own, :] * (inside_1[...] + book_1[own, :] * later)
    blocks = back.shape[0]
    scale = queries.shape[1] ** (-0.5)
    upper = triangle(True)
    after = later
    carry = jnp.sum(after * states[blocks], axis=0, keepdims=True)
    for c in reversed(range(blocks)):
        rows = slice(c * BLK, (c + 1) * BLK)
        cum = cumulative[rows, :]
        end = ends[c : c + 1, :]
        fading = jnp.exp(end - cum)
        key = keys[rows, :].astype(F32)
        after_parts = halves(after)
        d_query = jnp.exp(cum) * dot_parts(halves(d_mixed[rows, :]), halves(states[c]), NN)
        d_query = (d_query + to_q[rows, :]) * scale
        d_key = fading * dot_parts((values[rows, :],), after_parts, NN) + to_k[rows, :]
        d_value = dot_parts(halves(key * fading), after_parts, NT) + to_v[rows, :]
        grad_q[rows, :] = d_query.astype(BF16)
        grad_k[rows, :] = d_key.astype(BF16)
        grad_v[rows, :] = d_value.astype(BF16)
        change = queries[rows, :].astype(F32) * d_query - key * d_key
        summed = dot_exact(upper, change, NN) + carry
        grad_g[rows, :] = summed
        carry = summed[0:1, :]
        after = after * jnp.exp(end) + back[c]


def backward(
    queries, keys, values, cumulative, ends, d_mixed, states, back, inside, after, books
):
    pieces, insides = after
    return vmem_call(
        backward_body,
        [
            jax.ShapeDtypeStruct(queries.shape, BF16),
            jax.ShapeDtypeStruct(keys.shape, BF16),
            jax.ShapeDtypeStruct(values.shape, BF16),
            jax.ShapeDtypeStruct(queries.shape, F32),
        ],
    )(queries, keys, values, cumulative, ends, d_mixed, states, back, *inside, *pieces, *insides, *books)


BOOK_WHOLE, BOOK_OWN, BOOK_ROWS = 8, 16, 24


def stage_weights(logs, index, reverse):
    count = len(logs)
    place = [lax.rem(index - k + count, count) for k in range(count)]
    none = jnp.zeros_like(logs[0])

    def summed(condition):
        total = none
        for log, at in zip(logs, place):
            total = total + jnp.where(condition(at), log, 0.0)
        return total

    if reverse:
        passed = lambda at: at > index
        inner = lambda start: lambda at: (at < start) & (at > index)
        outer = lambda start: lambda at: at < start
    else:
        passed = lambda at: at < index
        inner = lambda start: lambda at: (at > start) & (at < index)
        outer = lambda start: lambda at: at > start
    near = [jnp.where(passed(at), jnp.exp(summed(inner(at))), 0.0) for at in place]
    whole = [jnp.exp(summed(outer(at))) for at in place]
    return near, whole, jnp.exp(summed(passed))


def weighted(pieces, weights):
    total = pieces[0].astype(F32) * weights[0]
    for piece, weight in zip(pieces[1:], weights[1:]):
        total = total + piece.astype(F32) * weight
    return total


def opened(pieces, index, book):
    width = pieces[0].shape[0] - 8
    logs = [piece[width : width + 1, :] for piece in pieces]
    states = [piece[0:width, :] for piece in pieces]
    near, whole, own = stage_weights(logs, index, True)
    for k in range(len(logs)):
        book[k : k + 1, :] = near[k]
        book[BOOK_WHOLE + k : BOOK_WHOLE + k + 1, :] = whole[k]
    book[BOOK_OWN : BOOK_OWN + 1, :] = own
    return states, logs, stage_weights(logs, index, False)


def stage_before_body(index, *refs):
    *pieces, inside, payload, book = refs
    states, logs, (near, whole, own) = opened(pieces, index[0], book)
    width = inside.shape[0]
    book[BOOK_OWN + 1 : BOOK_OWN + 2, :] = own
    inside[...] = weighted(states, near)
    payload[0:width, :] = weighted(states, whole)
    total = logs[0]
    for log in logs[1:]:
        total = total + log
    payload[width:, :] = jnp.where(grid_of((8, total.shape[1]), 0) == 0, total, 0.0)


def stage_after_body(*refs):
    *pieces, book, inside, total = refs
    pieces = [piece[...] for piece in pieces]
    inside[...] = weighted(pieces, [book[k : k + 1, :] for k in range(len(pieces))])
    wholes = [book[BOOK_WHOLE + k : BOOK_WHOLE + k + 1, :] for k in range(len(pieces))]
    total[...] = weighted(pieces, wholes).astype(BF16)


def everyone(x, axis):
    return [x] + [shifted(x, axis, k) for k in range(1, lax.axis_size(axis))]


def states_before(payload):
    rows, channels = payload.shape
    insides, books = [], []
    for axis in reversed(SP):
        pieces = everyone(payload, axis)
        index = lax.axis_index(axis).reshape(1)
        if axis == SP[0]:
            return pieces, index, insides, books
        inside, payload, book = vmem_call(
            stage_before_body,
            [
                jax.ShapeDtypeStruct((rows - 8, channels), F32),
                jax.ShapeDtypeStruct((rows, channels), F32),
                jax.ShapeDtypeStruct((BOOK_ROWS, channels), F32),
            ],
            in_specs=[SMEM] + [VMEM] * len(pieces),
        )(index, *pieces)
        insides.append(inside)
        books.append(book)


def states_after(part, books):
    insides = []
    for axis, book in zip(reversed(SP), books):
        pieces = everyone(part, axis)
        if axis == SP[0]:
            return pieces, insides
        inside, part = vmem_call(
            stage_after_body,
            [jax.ShapeDtypeStruct(part.shape, F32), jax.ShapeDtypeStruct(part.shape, BF16)],
        )(*pieces, book)
        insides.append(inside)


def local(
    d_out,
    route_expert,
    route_weight,
    expert_inputs,
    w_gate,
    w_up,
    w_down,
    w_out,
    queries,
    keys,
    values,
    log_decay,
):
    tok_rows, model_width = d_out.shape
    experts = lax.axis_size(SP)
    capacity = expert_inputs.shape[1] // experts
    cut = PAD * 2
    tail = -(-(capacity - cut) // PAD) * PAD
    slots = experts * (cut + tail)
    quarter = model_width // lax.axis_size("tp")
    place = lax.axis_index("tp").reshape(1)
    chosen, weight = route_expert.T, route_weight.T

    def exchanged(box):
        rows, width = box.shape
        box = box.reshape(experts, rows // experts, width)
        box = lax.all_to_all(box, SP, split_axis=0, concat_axis=0, tiled=True)
        return box.reshape(rows, width)

    outbox_q, ranks = vmem_call(
        functools.partial(route_body, experts=experts, most=cut),
        [
            jax.ShapeDtypeStruct((experts * cut, quarter), BF16),
            jax.ShapeDtypeStruct((2, tok_rows), jnp.int32),
        ],
        mebibytes=20,
        in_specs=[SMEM] + [VMEM] * 3,
    )(place, d_out, chosen, weight)
    tile = exchanged(outbox_q)
    routed_q = [tile]
    for k in range(1, lax.axis_size("tp")):
        routed_q.append(shifted(tile, "tp", k))

    outbox_d, pick = vmem_call(
        functools.partial(refill_body, least=cut, most=capacity, tail=tail),
        [
            jax.ShapeDtypeStruct((experts * tail, model_width), BF16),
            jax.ShapeDtypeStruct((slots, tok_rows), BF16),
        ],
        mebibytes=20,
    )(d_out, chosen, weight, ranks)
    routed_d = exchanged(outbox_d)

    gate_w, up_w, down_w = w_gate[0].T, w_up[0].T, w_down[0]
    rows_in, active, slope, hidden = expert_forward(
        expert_inputs[0], gate_w, up_w, experts, capacity, cut, tail
    )

    query, key, value, decay = queries[:, 0], keys[:, 0], values[:, 0], log_decay[:, 0]
    cumulative, ends, gain, produced = local_states(key, value, decay)
    before = states_before(produced)
    mixed, states, scores, book = forward(query, key, value, cumulative, ends, gain, before)
    books = (*before[3], book)

    weights = (active, slope, down_w, gate_w, up_w)
    *whole, keep_a, send_a, keep_b, send_b = expert_cotangents(
        place, routed_q, *weights, 0, ()
    )
    parts_q = (keep_a, send_a, keep_b, send_b)
    routed, d_gate, d_up, *parts_d = expert_cotangents(
        place, (routed_d,), *weights, experts * cut, whole
    )
    summed = jnp.concatenate(
        [
            summed_over_tp(*parts_q).reshape(experts, cut, quarter),
            summed_over_tp(*parts_d).reshape(experts, tail, quarter),
        ],
        axis=1,
    )
    returned = exchanged(summed.reshape(slots, quarter))
    grad_gate, grad_up = weight_grads(d_gate, d_up, rows_in)
    grad_down = dot(hidden, routed, TN).astype(BF16)

    own_cols = lax.dynamic_slice_in_dim(d_out, place[0] * quarter, quarter, 1)
    picked = own_cols.astype(F32) + dot(pick, returned, TN)
    tiles = gathered_ring(picked.astype(BF16))

    d_mixed, back, own_term = cotangents(place, tiles, w_out, query, cumulative, ends)
    after = states_after(own_term, books)
    inside = inside_blocks(query, key, value, cumulative, scores, d_mixed)
    grad_q, grad_k, grad_v, grad_g = backward(
        query, key, value, cumulative, ends, d_mixed, states, back, inside, after, books
    )

    proj = projection(place, tiles, mixed).reshape(experts, model_width // experts, -1)
    proj = lax.all_to_all(proj, SP, 0, 0, tiled=True)
    grad_proj = jnp.sum(proj.astype(F32), axis=0)
    return (
        grad_gate.T[None],
        grad_up.T[None],
        grad_down[None],
        grad_proj,
        grad_q[:, None],
        grad_k[:, None],
        grad_v[:, None],
        grad_g[:, None],
    )


def solution(mesh):
    finer = Mesh(mesh.devices.reshape(4, 4, 2, mesh.shape["tp"]), ("sp_0", "sp_1", "sp_2", "tp"))
    return jax.shard_map(
        local,
        mesh=finer,
        in_specs=(
            P(SP, None),
            P(SP, None),
            P(SP, None),
            P(SP, None, None),
            P(SP, None, "tp"),
            P(SP, None, "tp"),
            P(SP, "tp", None),
            P(None, "tp"),
            P(SP, "tp", None),
            P(SP, "tp", None),
            P(SP, "tp", None),
            P(SP, "tp", None),
        ),
        out_specs=(
            P(SP, None, "tp"),
            P(SP, None, "tp"),
            P(SP, "tp", None),
            P(SP, "tp"),
            P(SP, "tp", None),
            P(SP, "tp", None),
            P(SP, "tp", None),
            P(SP, "tp", None),
        ),
        check_vma=False,
    )
```

```python
import functools

import jax
import jax.numpy as jnp
from jax import lax
from jax.experimental import pallas as pl
from jax.experimental.pallas import tpu as pltpu
from jax.sharding import Mesh
from jax.sharding import PartitionSpec as P


BLK = 64
PAD = 8
SP = ("sp_0", "sp_1", "sp_2")
F32 = jnp.float32
BF16 = jnp.bfloat16

NN = (((1,), (0,)), ((), ()))
NT = (((1,), (1,)), ((), ()))
TN = (((0,), (0,)), ((), ()))


def dot(a, b, dims):
    return lax.dot_general(a, b, dims, preferred_element_type=F32)


def halves(x):
    high = x.astype(BF16)
    return high, (x - high.astype(F32)).astype(BF16)


def thirds(x):
    high = x.astype(BF16)
    rest = x - high.astype(F32)
    middle = rest.astype(BF16)
    return high, middle, (rest - middle.astype(F32)).astype(BF16)


def dot_parts(a, b, dims):
    out = dot(a[0], b[0], dims)
    if len(a) > 1:
        out = out + dot(a[1], b[0], dims)
    if len(b) > 1:
        out = out + dot(a[0], b[1], dims)
    return out


def dot_exact(mask, x, dims):
    high, middle, low = thirds(x)
    return dot(mask, high, dims) + (dot(mask, middle, dims) + dot(mask, low, dims))


def grid_of(shape, dim):
    return lax.broadcasted_iota(jnp.int32, shape, dim)


SMEM = pl.BlockSpec(memory_space=pltpu.SMEM)
VMEM = pl.BlockSpec(memory_space=pltpu.VMEM)


def limit(mebibytes):
    return pltpu.CompilerParams(vmem_limit_bytes=mebibytes * 1024 * 1024)


def vmem_call(kernel, outs, mebibytes=12, **options):
    return pl.pallas_call(kernel, out_shape=outs, compiler_params=limit(mebibytes), **options)


def fill_outbox(rows, weight, slot_a, slot_b, outbox):
    weights_a = jnp.concatenate(thirds(weight[0:1, :]), axis=0)
    weights_b = jnp.concatenate(thirds(weight[1:2, :]), axis=0)
    step = 256
    for start in range(0, outbox.shape[0], step):
        slot = grid_of((step, rows.shape[0]), 0) + start
        one_a = jnp.where(slot == slot_a, 1.0, 0.0).astype(BF16)
        one_b = jnp.where(slot == slot_b, 1.0, 0.0).astype(BF16)
        factor = dot(one_a, weights_a, NT) + dot(one_b, weights_b, NT)
        factor = jnp.sum(factor, axis=1, keepdims=True)
        outbox[start : start + step, :] = (dot(one_a + one_b, rows, NN) * factor).astype(BF16)


def slots_of(chosen, ranks, least, most, stride):
    inside = (ranks >= least) & (ranks < most)
    return jnp.where(inside, chosen * stride + ranks - least, -1)


def route_body(place, d_out, chosen, weight, outbox, ranks, *, experts, most):
    tokens = d_out.shape[0]
    first, second = chosen[0:1, :], chosen[1:2, :]
    ids = grid_of((experts, tokens), 0)
    is_first, is_second = ids == first, ids == second
    named = jnp.where(is_first | is_second, 1.0, 0.0).astype(BF16)
    earlier = jnp.where(
        grid_of((tokens, tokens), 0) < grid_of((tokens, tokens), 1), 1.0, 0.0
    ).astype(BF16)
    before = dot(named, earlier, NN)
    rank_a = jnp.sum(jnp.where(is_first, before, 0.0), axis=0, keepdims=True).astype(jnp.int32)
    rank_b = jnp.sum(jnp.where(is_second, before, 0.0), axis=0, keepdims=True).astype(jnp.int32)
    ranks[0:1, :] = rank_a
    ranks[1:2, :] = rank_b
    slot_a = slots_of(first, rank_a, 0, most, most)
    slot_b = slots_of(second, rank_b, 0, most, most)
    width = outbox.shape[1]
    rows = d_out[:, pl.ds(pl.multiple_of(place[0] * width, width), width)]
    fill_outbox(rows, weight, slot_a, slot_b, outbox)


def refill_body(d_out, chosen, weight, ranks, outbox, pick, *, least, most, tail):
    first, second = chosen[0:1, :], chosen[1:2, :]
    rank_a, rank_b = ranks[0:1, :], ranks[1:2, :]
    slot_a = slots_of(first, rank_a, least, most, tail)
    slot_b = slots_of(second, rank_b, least, most, tail)
    fill_outbox(d_out[...], weight, slot_a, slot_b, outbox)
    slot_a = first * (least + tail) + rank_a
    slot_b = second * (least + tail) + rank_b
    step = 256
    for start in range(0, pick.shape[0], step):
        slot = grid_of((step, pick.shape[1]), 0) + start
        found = (slot == slot_a) | (slot == slot_b)
        pick[start : start + step, :] = jnp.where(found, 1.0, 0.0).astype(BF16)


def slot_order(group, capacity, cut, tail):
    def placed(rows, stride, width, first):
        row, col = grid_of((rows, group * capacity), 0), grid_of((rows, group * capacity), 1)
        found = row < 0
        for source in range(group):
            start = source * stride
            here = (row >= start) & (row < start + width)
            found = found | (here & (col == row + (source * capacity + first - start)))
        return jnp.where(found, 1.0, 0.0).astype(BF16)

    return placed(group * cut, cut, cut, 0), placed(group * tail, tail, capacity - cut, cut)


def expert_forward_body(inputs, gate_w, up_w, *outs, orders):
    order = jnp.concatenate(slot_order(*orders), axis=0)
    moved = dot(order, inputs[...], NN).astype(BF16)
    split = outs[0].shape[0]
    rows_q, rows_d = outs[0:2]
    rows_q[...] = moved[:split]
    rows_d[...] = moved[split:]
    units = gate_w.shape[0]
    for first in range(0, units, 256):
        cols = slice(first, min(first + 256, units))
        gate = dot(moved, gate_w[cols, :], NT)
        up = dot(moved, up_w[cols, :], NT)
        sigmoid = 1.0 / (1.0 + jnp.exp(-gate))
        silu = gate * sigmoid
        slope = up * sigmoid * (1.0 + gate * (1.0 - sigmoid))
        for i, value in enumerate((silu, slope, silu * up)):
            value = value.astype(BF16)
            outs[2 + 2 * i][:, cols] = value[:split]
            outs[3 + 2 * i][:, cols] = value[split:]


def expert_forward(inputs, gate_w, up_w, experts, capacity, cut, tail):
    group = 8
    width, units = inputs.shape[1], gate_w.shape[0]
    sizes = (group * cut, group * tail)
    by_row = lambda i: (i, 0)
    whole = pl.BlockSpec((units, width), lambda i: (0, 0))
    widths = [width] * 2 + [units] * 6
    return pl.pallas_call(
        functools.partial(expert_forward_body, orders=(group, capacity, cut, tail)),
        grid=(experts // group,),
        in_specs=[pl.BlockSpec((group * capacity, width), by_row), whole, whole],
        out_specs=[pl.BlockSpec((sizes[i % 2], w), by_row) for i, w in enumerate(widths)],
        out_shape=[
            jax.ShapeDtypeStruct((experts // group * sizes[i % 2], w), BF16)
            for i, w in enumerate(widths)
        ],
        compiler_params=limit(56),
    )(inputs, gate_w, up_w)


def expert_body(place, *refs, tiles):
    routed, (active, slope, down_w, gate_w, up_w) = refs[:tiles], refs[tiles : tiles + 5]
    *routed_out, d_gate, d_up, keep_a, send_a, keep_b, send_b = refs[tiles + 5 : -4]
    down_v, gate_v, up_v, loaded = refs[-4:]
    copies = [
        pltpu.make_async_copy(source, target, loaded.at[i])
        for i, (source, target) in enumerate(((down_w, down_v), (gate_w, gate_v), (up_w, up_v)))
    ]

    @pl.when(pl.program_id(0) == 0)
    def _():
        for copy in copies:
            copy.start()
        copies[0].wait()

    d_hidden = 0.0
    for k, tile in enumerate(routed):
        wide = tile.shape[1]
        cols = slice(None)
        if tiles > 1:
            cols = pl.ds(pl.multiple_of(((place[0] + tiles - k) & (tiles - 1)) * wide, wide), wide)
            routed_out[0][:, cols] = tile[...]
        d_hidden = d_hidden + dot(tile[...], down_v[:, cols], NT)

    @pl.when(pl.program_id(0) == 0)
    def _():
        copies[1].wait()
        copies[2].wait()

    to_gate = (d_hidden * slope[...].astype(F32)).astype(BF16)
    to_up = (d_hidden * active[...].astype(F32)).astype(BF16)
    d_gate[...] = to_gate
    d_up[...] = to_up
    half = keep_a.shape[2]
    homes = (
        ((keep_a, 0), (keep_b, 0)),
        ((send_a, 0), (keep_b, 1)),
        ((send_a, 1), (send_b, 1)),
        ((keep_a, 1), (send_b, 0)),
    )
    for k, (home_a, home_b) in enumerate(homes):
        start = pl.multiple_of((place[0] ^ k) * (2 * half), 2 * half)
        cols = pl.ds(start, 2 * half)
        term = dot(to_gate, gate_v[:, cols], NN) + dot(to_up, up_v[:, cols], NN)
        term = term.astype(BF16)
        home_a[0][home_a[1]] = term[:, :half]
        home_b[0][home_b[1]] = term[:, half:]


def expert_cotangents(place, routed, active, slope, down_w, gate_w, up_w):
    rows, wide = routed[0].shape
    tiles = len(routed)
    units, width = down_w.shape
    step = 256
    half = width // 8
    by_row = lambda i, *_: (i, 0)
    pair = pl.BlockSpec((2, step, half), lambda i, *_: (0, i, 0))
    rebuilt = [width] if tiles > 1 else []
    return pl.pallas_call(
        functools.partial(expert_body, tiles=tiles),
        grid_spec=pltpu.PrefetchScalarGridSpec(
            num_scalar_prefetch=1,
            grid=(rows // step,),
            in_specs=[pl.BlockSpec((step, wide), by_row)] * tiles
            + [pl.BlockSpec((step, units), by_row)] * 2
            + [pl.BlockSpec(memory_space=pl.ANY)] * 3,
            out_specs=[pl.BlockSpec((step, w), by_row) for w in rebuilt + [units] * 2]
            + [pair] * 4,
            scratch_shapes=[pltpu.VMEM((units, width), BF16)] * 3
            + [pltpu.SemaphoreType.DMA((3,))],
        ),
        out_shape=[jax.ShapeDtypeStruct((rows, w), BF16) for w in rebuilt + [units] * 2]
        + [jax.ShapeDtypeStruct((2, rows, half), BF16)] * 4,
        compiler_params=limit(56),
    )(place, *routed, active, slope, down_w, gate_w, up_w)


def weight_grads_body(*refs):
    *parts, rows_q, rows_d = refs[: len(refs) - (len(refs) - 2) // 3]
    for i, out in enumerate(refs[len(refs) - len(parts) // 2 :]):
        total = dot(parts[2 * i][...], rows_q[...], TN)
        out[...] = (total + dot(parts[2 * i + 1][...], rows_d[...], TN)).astype(BF16)


def weight_grads(pairs, rows):
    width = rows[0].shape[1]
    units = pairs[0][0].shape[1]
    step = 512
    parts = [part for pair in pairs for part in pair]
    by_col = lambda i: (0, i)
    return pl.pallas_call(
        weight_grads_body,
        grid=(width // step,),
        in_specs=[pl.BlockSpec(part.shape, lambda i: (0, 0)) for part in parts]
        + [pl.BlockSpec((part.shape[0], step), by_col) for part in rows],
        out_specs=[pl.BlockSpec((units, step), by_col)] * len(pairs),
        out_shape=[jax.ShapeDtypeStruct((units, width), BF16)] * len(pairs),
        compiler_params=limit(58),
    )(*parts, *rows)


def swapped(x, flip):
    count = lax.axis_size("tp")
    return lax.ppermute(x, "tp", [(i, i ^ flip) for i in range(count)])


def plus(*terms):
    total = terms[0].astype(F32)
    for term in terms[1:]:
        total = total + term.astype(F32)
    return total.astype(BF16)


def final_sum_body(keep_a, got_a, last_a, keep_b, got_b, last_b, out):
    half = keep_a.shape[2]
    for start, keep, got, last in ((0, keep_a, got_a, last_a), (half, keep_b, got_b, last_b)):
        total = keep[0].astype(F32) + got[0].astype(F32) + last[...].astype(F32)
        out[:, start : start + half] = total.astype(BF16)


def final_sum(keep_a, got_a, last_a, keep_b, got_b, last_b):
    _, rows, half = keep_a.shape
    first = pl.BlockSpec((1, rows, half), lambda i: (0, 0, 0))
    whole = pl.BlockSpec((rows, half), lambda i: (0, 0))
    return pl.pallas_call(
        final_sum_body,
        grid=(1,),
        in_specs=[first, first, whole] * 2,
        out_specs=pl.BlockSpec((rows, 2 * half), lambda i: (0, 0)),
        out_shape=jax.ShapeDtypeStruct((rows, 2 * half), BF16),
        compiler_params=limit(12),
    )(keep_a, got_a, last_a, keep_b, got_b, last_b)


def summed_over_tp(keep_a, send_a, keep_b, send_b):
    got_a = swapped(send_a, 1)
    got_b = swapped(send_b, 3)
    last_a, last_b = plus(keep_a[1], got_a[1]), plus(keep_b[1], got_b[1])
    last_a = swapped(last_a, 3)
    last_b = swapped(last_b, 1)
    return final_sum(keep_a, got_a, last_a, keep_b, got_b, last_b)


def shifted(x, axis, by):
    count = lax.axis_size(axis)
    return lax.ppermute(x, axis, [(i, (i + by) % count) for i in range(count)])


def gathered_ring(x):
    half = x.shape[0] // 2
    below = shifted(x, "tp", 1)
    above = shifted(x, "tp", -1)
    across = jnp.concatenate(
        [shifted(below[:half], "tp", 1), shifted(above[half:], "tp", -1)], axis=0
    )
    return x, below, above, across


def triangle(reverse):
    row, col = grid_of((BLK, BLK), 0), grid_of((BLK, BLK), 1)
    return jnp.where((row <= col) if reverse else (row >= col), 1.0, 0.0).astype(BF16)


def local_state_body(keys, values, decay, cumulative, ends, gain, produced):
    blocks = gain.shape[0]
    lower = triangle(False)
    for c in range(blocks):
        rows = slice(c * BLK, (c + 1) * BLK)
        cum = dot_exact(lower, decay[rows, :], NN)
        cumulative[rows, :] = cum
        end = cum[BLK - 1 : BLK, :]
        ends[c : c + 1, :] = end
        faded = keys[rows, :].astype(F32) * jnp.exp(end - cum)
        gain[c] = dot_parts((values[rows, :],), halves(faded), TN)
    state = gain[0]
    total = ends[0:1, :]
    for c in range(1, blocks):
        state = state * jnp.exp(ends[c : c + 1, :]) + gain[c]
        total = total + ends[c : c + 1, :]
    width = state.shape[0]
    produced[0:width, :] = state
    spare = produced.shape[0] - width
    produced[width:, :] = jnp.where(grid_of((spare, total.shape[1]), 0) == 0, total, 0.0)


def local_states(keys, values, decay):
    tokens, channels = keys.shape
    width = values.shape[1]
    blocks = tokens // BLK
    return vmem_call(
        local_state_body,
        [
            jax.ShapeDtypeStruct((tokens, channels), F32),
            jax.ShapeDtypeStruct((blocks, channels), F32),
            jax.ShapeDtypeStruct((blocks, width, channels), F32),
            jax.ShapeDtypeStruct((width + 8, channels), F32),
        ],
    )(keys, values, decay)


def forward_body(index, queries, keys, values, cumulative, ends, gain, *refs):
    *pieces, inside_0, inside_1, book_0, book_1, mixed, states, scores, book = refs
    blocks = gain.shape[0]
    far, _, (near, _, _) = opened(pieces, index[0], book)
    own = slice(BOOK_OWN + 1, BOOK_OWN + 2)
    start = inside_0[...] + book_0[own, :] * (inside_1[...] + book_1[own, :] * weighted(far, near))
    scale = queries.shape[1] ** (-0.5)
    causal = grid_of((BLK, BLK), 0) >= grid_of((BLK, BLK), 1)
    state = start
    for c in range(blocks):
        rows = slice(c * BLK, (c + 1) * BLK)
        cum = cumulative[rows, :]
        middle = cum[BLK // 2 - 1 : BLK // 2, :]
        query = queries[rows, :].astype(F32) * scale
        near_q = halves(query * jnp.exp(cum - middle))
        near_k = halves(keys[rows, :].astype(F32) * jnp.exp(middle - cum))
        score = jnp.where(causal, dot_parts(near_q, near_k, NT), 0.0)
        scores[rows, :] = score
        states[c] = state
        out = dot_parts(halves(query * jnp.exp(cum)), halves(state), NT)
        out = out + dot_parts(halves(score), (values[rows, :],), NN)
        mixed[rows, :] = out.astype(BF16)
        state = state * jnp.exp(ends[c : c + 1, :]) + gain[c]
    states[blocks] = state


def forward(queries, keys, values, cumulative, ends, gain, before):
    pieces, index, insides, books = before
    tokens, channels = keys.shape
    width = values.shape[1]
    blocks = tokens // BLK
    operands = (*pieces, *insides, *books)
    return vmem_call(
        forward_body,
        [
            jax.ShapeDtypeStruct((tokens, width), BF16),
            jax.ShapeDtypeStruct((blocks + 1, width, channels), F32),
            jax.ShapeDtypeStruct((tokens, BLK), F32),
            jax.ShapeDtypeStruct((BOOK_ROWS, channels), F32),
        ],
        in_specs=[SMEM] + [VMEM] * (6 + len(operands)),
    )(index, queries, keys, values, cumulative, ends, gain, *operands)


def cotangent_body(place, a, b, c, d, w_out, queries, cumulative, ends, d_mixed, back, own):
    blocks = back.shape[0]
    scale = queries.shape[1] ** (-0.5)
    quarter = a.shape[1]
    total = None
    for tile, offset in ((a, 0), (b, 3), (c, 1), (d, 2)):
        start = pl.multiple_of(((place[0] + offset) & 3) * quarter, quarter)
        term = dot(tile[...], w_out[pl.ds(start, quarter), :], NN)
        total = term if total is None else total + term
    d_mixed[...] = total
    for c in range(blocks):
        rows = slice(c * BLK, (c + 1) * BLK)
        query = queries[rows, :].astype(F32) * (scale * jnp.exp(cumulative[rows, :]))
        back[c] = dot_parts(halves(d_mixed[rows, :]), halves(query), TN)
    state = back[blocks - 1]
    for c in reversed(range(blocks - 1)):
        state = state * jnp.exp(ends[c : c + 1, :]) + back[c]
    own[...] = state.astype(BF16)


def cotangents(place, tiles, w_out, queries, cumulative, ends):
    tokens, channels = queries.shape
    width = w_out.shape[1]
    blocks = tokens // BLK
    return vmem_call(
        cotangent_body,
        [
            jax.ShapeDtypeStruct((tokens, width), F32),
            jax.ShapeDtypeStruct((blocks, width, channels), F32),
            jax.ShapeDtypeStruct((width, channels), BF16),
        ],
        in_specs=[SMEM] + [VMEM] * 8,
    )(place, *tiles, w_out, queries, cumulative, ends)


def projection_body(place, a, b, c, d, mixed, out):
    quarter = a.shape[1]
    for tile, offset in ((a, 0), (b, 3), (c, 1), (d, 2)):
        start = pl.multiple_of(((place[0] + offset) & 3) * quarter, quarter)
        out[pl.ds(start, quarter), :] = dot(tile[...], mixed[...], TN).astype(BF16)


def projection(place, tiles, mixed):
    return vmem_call(
        projection_body,
        jax.ShapeDtypeStruct((4 * tiles[0].shape[1], mixed.shape[1]), BF16),
        in_specs=[SMEM] + [VMEM] * 5,
    )(place, *tiles, mixed)


def inside_body(queries, keys, values, cumulative, scores, d_mixed, to_q, to_k, to_v):
    blocks = queries.shape[0] // BLK
    scale = queries.shape[1] ** (-0.5)
    causal = grid_of((BLK, BLK), 0) >= grid_of((BLK, BLK), 1)
    for c in range(blocks):
        rows = slice(c * BLK, (c + 1) * BLK)
        cum = cumulative[rows, :]
        middle = cum[BLK // 2 - 1 : BLK // 2, :]
        rising, falling = jnp.exp(cum - middle), jnp.exp(middle - cum)
        near_q = halves(queries[rows, :].astype(F32) * scale * rising)
        near_k = halves(keys[rows, :].astype(F32) * falling)
        incoming = halves(d_mixed[rows, :])
        d_score = jnp.where(causal, dot_parts(incoming, (values[rows, :],), NT), 0.0)
        d_score = halves(d_score)
        to_q[rows, :] = rising * dot_parts(d_score, near_k, NN)
        to_k[rows, :] = falling * dot_parts(d_score, near_q, TN)
        to_v[rows, :] = dot_parts(halves(scores[rows, :]), incoming, TN)


def inside_blocks(queries, keys, values, cumulative, scores, d_mixed):
    tokens, channels = queries.shape
    return vmem_call(
        inside_body,
        [
            jax.ShapeDtypeStruct((tokens, channels), F32),
            jax.ShapeDtypeStruct((tokens, channels), F32),
            jax.ShapeDtypeStruct(values.shape, F32),
        ],
    )(queries, keys, values, cumulative, scores, d_mixed)


def backward_body(
    queries, keys, values, cumulative, ends, d_mixed, states, back, to_q, to_k, to_v, *refs
):
    *pieces, inside_0, inside_1, book_0, book_1, book, grad_q, grad_k, grad_v, grad_g = refs
    own = slice(BOOK_OWN, BOOK_OWN + 1)
    later = weighted([x[...] for x in pieces], [book[k : k + 1, :] for k in range(len(pieces))])
    later = inside_0[...] + book_0[own, :] * (inside_1[...] + book_1[own, :] * later)
    blocks = back.shape[0]
    scale = queries.shape[1] ** (-0.5)
    upper = triangle(True)
    after = later
    carry = jnp.sum(after * states[blocks], axis=0, keepdims=True)
    for c in reversed(range(blocks)):
        rows = slice(c * BLK, (c + 1) * BLK)
        cum = cumulative[rows, :]
        end = ends[c : c + 1, :]
        fading = jnp.exp(end - cum)
        key = keys[rows, :].astype(F32)
        after_parts = halves(after)
        d_query = jnp.exp(cum) * dot_parts(halves(d_mixed[rows, :]), halves(states[c]), NN)
        d_query = (d_query + to_q[rows, :]) * scale
        d_key = fading * dot_parts((values[rows, :],), after_parts, NN) + to_k[rows, :]
        d_value = dot_parts(halves(key * fading), after_parts, NT) + to_v[rows, :]
        grad_q[rows, :] = d_query.astype(BF16)
        grad_k[rows, :] = d_key.astype(BF16)
        grad_v[rows, :] = d_value.astype(BF16)
        change = queries[rows, :].astype(F32) * d_query - key * d_key
        summed = dot_exact(upper, change, NN) + carry
        grad_g[rows, :] = summed
        carry = summed[0:1, :]
        after = after * jnp.exp(end) + back[c]


def backward(
    queries, keys, values, cumulative, ends, d_mixed, states, back, inside, after, books
):
    pieces, insides = after
    return vmem_call(
        backward_body,
        [
            jax.ShapeDtypeStruct(queries.shape, BF16),
            jax.ShapeDtypeStruct(keys.shape, BF16),
            jax.ShapeDtypeStruct(values.shape, BF16),
            jax.ShapeDtypeStruct(queries.shape, F32),
        ],
    )(queries, keys, values, cumulative, ends, d_mixed, states, back, *inside, *pieces, *insides, *books)


BOOK_WHOLE, BOOK_OWN, BOOK_ROWS = 8, 16, 24


def stage_weights(logs, index, reverse):
    count = len(logs)
    place = [lax.rem(index - k + count, count) for k in range(count)]
    none = jnp.zeros_like(logs[0])

    def summed(condition):
        total = none
        for log, at in zip(logs, place):
            total = total + jnp.where(condition(at), log, 0.0)
        return total

    if reverse:
        passed = lambda at: at > index
        inner = lambda start: lambda at: (at < start) & (at > index)
        outer = lambda start: lambda at: at < start
    else:
        passed = lambda at: at < index
        inner = lambda start: lambda at: (at > start) & (at < index)
        outer = lambda start: lambda at: at > start
    near = [jnp.where(passed(at), jnp.exp(summed(inner(at))), 0.0) for at in place]
    whole = [jnp.exp(summed(outer(at))) for at in place]
    return near, whole, jnp.exp(summed(passed))


def weighted(pieces, weights):
    total = pieces[0].astype(F32) * weights[0]
    for piece, weight in zip(pieces[1:], weights[1:]):
        total = total + piece.astype(F32) * weight
    return total


def opened(pieces, index, book):
    width = pieces[0].shape[0] - 8
    logs = [piece[width : width + 1, :] for piece in pieces]
    states = [piece[0:width, :] for piece in pieces]
    near, whole, own = stage_weights(logs, index, True)
    for k in range(len(logs)):
        book[k : k + 1, :] = near[k]
        book[BOOK_WHOLE + k : BOOK_WHOLE + k + 1, :] = whole[k]
    book[BOOK_OWN : BOOK_OWN + 1, :] = own
    return states, logs, stage_weights(logs, index, False)


def stage_before_body(index, *refs):
    *pieces, inside, payload, book = refs
    states, logs, (near, whole, own) = opened(pieces, index[0], book)
    width = inside.shape[0]
    book[BOOK_OWN + 1 : BOOK_OWN + 2, :] = own
    inside[...] = weighted(states, near)
    payload[0:width, :] = weighted(states, whole)
    total = logs[0]
    for log in logs[1:]:
        total = total + log
    payload[width:, :] = jnp.where(grid_of((8, total.shape[1]), 0) == 0, total, 0.0)


def stage_after_body(*refs):
    *pieces, book, inside, total = refs
    pieces = [piece[...] for piece in pieces]
    inside[...] = weighted(pieces, [book[k : k + 1, :] for k in range(len(pieces))])
    wholes = [book[BOOK_WHOLE + k : BOOK_WHOLE + k + 1, :] for k in range(len(pieces))]
    total[...] = weighted(pieces, wholes).astype(BF16)


def everyone(x, axis):
    return [x] + [shifted(x, axis, k) for k in range(1, lax.axis_size(axis))]


def states_before(payload):
    rows, channels = payload.shape
    insides, books = [], []
    for axis in reversed(SP):
        pieces = everyone(payload, axis)
        index = lax.axis_index(axis).reshape(1)
        if axis == SP[0]:
            return pieces, index, insides, books
        inside, payload, book = vmem_call(
            stage_before_body,
            [
                jax.ShapeDtypeStruct((rows - 8, channels), F32),
                jax.ShapeDtypeStruct((rows, channels), F32),
                jax.ShapeDtypeStruct((BOOK_ROWS, channels), F32),
            ],
            in_specs=[SMEM] + [VMEM] * len(pieces),
        )(index, *pieces)
        insides.append(inside)
        books.append(book)


def states_after(part, books):
    insides = []
    for axis, book in zip(reversed(SP), books):
        pieces = everyone(part, axis)
        if axis == SP[0]:
            return pieces, insides
        inside, part = vmem_call(
            stage_after_body,
            [jax.ShapeDtypeStruct(part.shape, F32), jax.ShapeDtypeStruct(part.shape, BF16)],
        )(*pieces, book)
        insides.append(inside)


def local(
    d_out,
    route_expert,
    route_weight,
    expert_inputs,
    w_gate,
    w_up,
    w_down,
    w_out,
    queries,
    keys,
    values,
    log_decay,
):
    tok_rows, model_width = d_out.shape
    experts = lax.axis_size(SP)
    capacity = expert_inputs.shape[1] // experts
    cut = PAD * 2
    tail = -(-(capacity - cut) // PAD) * PAD
    slots = experts * (cut + tail)
    quarter = model_width // lax.axis_size("tp")
    place = lax.axis_index("tp").reshape(1)
    chosen, weight = route_expert.T, route_weight.T

    def exchanged(box):
        rows, width = box.shape
        box = box.reshape(experts, rows // experts, width)
        box = lax.all_to_all(box, SP, split_axis=0, concat_axis=0, tiled=True)
        return box.reshape(rows, width)

    outbox_q, ranks = vmem_call(
        functools.partial(route_body, experts=experts, most=cut),
        [
            jax.ShapeDtypeStruct((experts * cut, quarter), BF16),
            jax.ShapeDtypeStruct((2, tok_rows), jnp.int32),
        ],
        mebibytes=20,
        in_specs=[SMEM] + [VMEM] * 3,
    )(place, d_out, chosen, weight)
    tile = exchanged(outbox_q)
    routed_q = [tile]
    for k in range(1, lax.axis_size("tp")):
        routed_q.append(shifted(tile, "tp", k))

    outbox_d, pick = vmem_call(
        functools.partial(refill_body, least=cut, most=capacity, tail=tail),
        [
            jax.ShapeDtypeStruct((experts * tail, model_width), BF16),
            jax.ShapeDtypeStruct((slots, tok_rows), BF16),
        ],
        mebibytes=20,
    )(d_out, chosen, weight, ranks)
    routed_d = exchanged(outbox_d)

    gate_w, up_w, down_w = w_gate[0].T, w_up[0].T, w_down[0]
    rows_q, rows_d, active_q, active_d, slope_q, slope_d, hidden_q, hidden_d = expert_forward(
        expert_inputs[0], gate_w, up_w, experts, capacity, cut, tail
    )

    query, key, value, decay = queries[:, 0], keys[:, 0], values[:, 0], log_decay[:, 0]
    cumulative, ends, gain, produced = local_states(key, value, decay)
    before = states_before(produced)
    mixed, states, scores, book = forward(query, key, value, cumulative, ends, gain, before)
    books = (*before[3], book)

    weights = (down_w, gate_w, up_w)
    routed_q, gate_q, up_q, *parts_q = expert_cotangents(
        place, routed_q, active_q, slope_q, *weights
    )
    gate_d, up_d, *parts_d = expert_cotangents(
        place, (routed_d,), active_d, slope_d, *weights
    )
    summed = jnp.concatenate(
        [
            summed_over_tp(*parts_q).reshape(experts, cut, quarter),
            summed_over_tp(*parts_d).reshape(experts, tail, quarter),
        ],
        axis=1,
    )
    returned = exchanged(summed.reshape(slots, quarter))
    grad_gate, grad_up = weight_grads(((gate_q, gate_d), (up_q, up_d)), (rows_q, rows_d))
    (grad_down,) = weight_grads(((hidden_q, hidden_d),), (routed_q, routed_d))

    own_cols = lax.dynamic_slice_in_dim(d_out, place[0] * quarter, quarter, 1)
    picked = own_cols.astype(F32) + dot(pick, returned, TN)
    tiles = gathered_ring(picked.astype(BF16))

    d_mixed, back, own_term = cotangents(place, tiles, w_out, query, cumulative, ends)
    after = states_after(own_term, books)
    inside = inside_blocks(query, key, value, cumulative, scores, d_mixed)
    grad_q, grad_k, grad_v, grad_g = backward(
        query, key, value, cumulative, ends, d_mixed, states, back, inside, after, books
    )

    proj = projection(place, tiles, mixed).reshape(experts, model_width // experts, -1)
    proj = lax.all_to_all(proj, SP, 0, 0, tiled=True)
    grad_proj = jnp.sum(proj.astype(F32), axis=0)
    return (
        grad_gate.T[None],
        grad_up.T[None],
        grad_down[None],
        grad_proj,
        grad_q[:, None],
        grad_k[:, None],
        grad_v[:, None],
        grad_g[:, None],
    )


def solution(mesh):
    finer = Mesh(mesh.devices.reshape(4, 4, 2, mesh.shape["tp"]), ("sp_0", "sp_1", "sp_2", "tp"))
    return jax.shard_map(
        local,
        mesh=finer,
        in_specs=(
            P(SP, None),
            P(SP, None),
            P(SP, None),
            P(SP, None, None),
            P(SP, None, "tp"),
            P(SP, None, "tp"),
            P(SP, "tp", None),
            P(None, "tp"),
            P(SP, "tp", None),
            P(SP, "tp", None),
            P(SP, "tp", None),
            P(SP, "tp", None),
        ),
        out_specs=(
            P(SP, None, "tp"),
            P(SP, None, "tp"),
            P(SP, "tp", None),
            P(SP, "tp"),
            P(SP, "tp", None),
            P(SP, "tp", None),
            P(SP, "tp", None),
            P(SP, "tp", None),
        ),
        check_vma=False,
    )
```

```python
import functools

import jax
import jax.numpy as jnp
from jax import lax
from jax.experimental import pallas as pl
from jax.experimental.pallas import tpu as pltpu
from jax.sharding import Mesh
from jax.sharding import PartitionSpec as P


BLK = 64
PAD = 8
SP = ("sp_0", "sp_1", "sp_2")
TP = "tp"
F32 = jnp.float32
BF16 = jnp.bfloat16

NN = (((1,), (0,)), ((), ()))
NT = (((1,), (1,)), ((), ()))
TN = (((0,), (0,)), ((), ()))


def dot(a, b, dims):
    return lax.dot_general(a, b, dims, preferred_element_type=F32)


def halves(x):
    high = x.astype(BF16)
    return high, (x - high.astype(F32)).astype(BF16)


def thirds(x):
    high = x.astype(BF16)
    rest = x - high.astype(F32)
    middle = rest.astype(BF16)
    return high, middle, (rest - middle.astype(F32)).astype(BF16)


def dot_parts(a, b, dims):
    out = dot(a[0], b[0], dims)
    if len(a) > 1:
        out = out + dot(a[1], b[0], dims)
    if len(b) > 1:
        out = out + dot(a[0], b[1], dims)
    return out


def dot_exact(mask, x, dims):
    high, middle, low = thirds(x)
    return dot(mask, high, dims) + (dot(mask, middle, dims) + dot(mask, low, dims))


def grid_of(shape, dim):
    return lax.broadcasted_iota(jnp.int32, shape, dim)


SMEM = pl.BlockSpec(memory_space=pltpu.SMEM)
VMEM = pl.BlockSpec(memory_space=pltpu.VMEM)


def limit(mebibytes):
    return pltpu.CompilerParams(vmem_limit_bytes=mebibytes * 1024 * 1024)


def vmem_call(kernel, outs, mebibytes=12, **options):
    return pl.pallas_call(kernel, out_shape=outs, compiler_params=limit(mebibytes), **options)


def fill_outbox(rows, weight, slot_a, slot_b, outbox):
    weights_a = jnp.concatenate(thirds(weight[0:1, :]), axis=0)
    weights_b = jnp.concatenate(thirds(weight[1:2, :]), axis=0)
    step = 256
    for start in range(0, outbox.shape[0], step):
        slot = grid_of((step, rows.shape[0]), 0) + start
        one_a = jnp.where(slot == slot_a, 1.0, 0.0).astype(BF16)
        one_b = jnp.where(slot == slot_b, 1.0, 0.0).astype(BF16)
        factor = dot(one_a, weights_a, NT) + dot(one_b, weights_b, NT)
        factor = jnp.sum(factor, axis=1, keepdims=True)
        outbox[start : start + step, :] = (dot(one_a + one_b, rows, NN) * factor).astype(BF16)


def slots_of(chosen, ranks, least, most, stride):
    inside = (ranks >= least) & (ranks < most)
    return jnp.where(inside, chosen * stride + ranks - least, -1)


def route_body(place, d_out, chosen, weight, outbox, ranks, rows, loaded, *, experts, most):
    tokens, width = rows.shape
    start = pl.multiple_of(place[0] * width, width)
    copy = pltpu.make_async_copy(d_out.at[:, pl.ds(start, width)], rows, loaded)
    copy.start()
    first, second = chosen[0:1, :], chosen[1:2, :]
    ids = grid_of((experts, tokens), 0)
    is_first, is_second = ids == first, ids == second
    named = jnp.where(is_first | is_second, 1.0, 0.0).astype(BF16)
    earlier = jnp.where(
        grid_of((tokens, tokens), 0) < grid_of((tokens, tokens), 1), 1.0, 0.0
    ).astype(BF16)
    before = dot(named, earlier, NN)
    rank_a = jnp.sum(jnp.where(is_first, before, 0.0), axis=0, keepdims=True).astype(jnp.int32)
    rank_b = jnp.sum(jnp.where(is_second, before, 0.0), axis=0, keepdims=True).astype(jnp.int32)
    ranks[0:1, :] = rank_a
    ranks[1:2, :] = rank_b
    slot_a = slots_of(first, rank_a, 0, most, most)
    slot_b = slots_of(second, rank_b, 0, most, most)
    copy.wait()
    fill_outbox(rows[...], weight, slot_a, slot_b, outbox)


def refill_body(d_out, chosen, weight, ranks, outbox, pick, *, least, most, tail):
    first, second = chosen[0:1, :], chosen[1:2, :]
    rank_a, rank_b = ranks[0:1, :], ranks[1:2, :]
    slot_a = slots_of(first, rank_a, least, most, tail)
    slot_b = slots_of(second, rank_b, least, most, tail)
    fill_outbox(d_out[...], weight, slot_a, slot_b, outbox)
    slot_a = first * (least + tail) + rank_a
    slot_b = second * (least + tail) + rank_b
    step = 256
    for start in range(0, pick.shape[0], step):
        slot = grid_of((step, pick.shape[1]), 0) + start
        found = (slot == slot_a) | (slot == slot_b)
        pick[start : start + step, :] = jnp.where(found, 1.0, 0.0).astype(BF16)


def slot_order(group, capacity, cut, tail):
    def placed(rows, stride, width, first):
        row, col = grid_of((rows, group * capacity), 0), grid_of((rows, group * capacity), 1)
        found = row < 0
        for source in range(group):
            start = source * stride
            here = (row >= start) & (row < start + width)
            found = found | (here & (col == row + (source * capacity + first - start)))
        return jnp.where(found, 1.0, 0.0).astype(BF16)

    return placed(group * cut, cut, cut, 0), placed(group * tail, tail, capacity - cut, cut)


def expert_forward_body(inputs, gate_w, up_w, *outs, orders):
    order = jnp.concatenate(slot_order(*orders), axis=0)
    moved = dot(order, inputs[...], NN).astype(BF16)
    split = outs[0].shape[0]
    rows_q, rows_d = outs[0:2]
    rows_q[...] = moved[:split]
    rows_d[...] = moved[split:]
    units = gate_w.shape[0]
    for first in range(0, units, 256):
        cols = slice(first, min(first + 256, units))
        gate = dot(moved, gate_w[cols, :], NT)
        up = dot(moved, up_w[cols, :], NT)
        sigmoid = 1.0 / (1.0 + jnp.exp(-gate))
        silu = gate * sigmoid
        slope = up * sigmoid * (1.0 + gate * (1.0 - sigmoid))
        for i, value in enumerate((silu, slope, silu * up)):
            value = value.astype(BF16)
            outs[2 + 2 * i][:, cols] = value[:split]
            outs[3 + 2 * i][:, cols] = value[split:]


def expert_forward(inputs, gate_w, up_w, experts, capacity, cut, tail):
    group = 8
    width, units = inputs.shape[1], gate_w.shape[0]
    sizes = (group * cut, group * tail)
    by_row = lambda i: (i, 0)
    whole = pl.BlockSpec((units, width), lambda i: (0, 0))
    widths = [width] * 2 + [units] * 6
    return pl.pallas_call(
        functools.partial(expert_forward_body, orders=(group, capacity, cut, tail)),
        grid=(experts // group,),
        in_specs=[pl.BlockSpec((group * capacity, width), by_row), whole, whole],
        out_specs=[pl.BlockSpec((sizes[i % 2], w), by_row) for i, w in enumerate(widths)],
        out_shape=[
            jax.ShapeDtypeStruct((experts // group * sizes[i % 2], w), BF16)
            for i, w in enumerate(widths)
        ],
        compiler_params=limit(56),
    )(inputs, gate_w, up_w)


def expert_body(place, *refs, tiles):
    routed, (active, slope, down_w, gate_w, up_w) = refs[:tiles], refs[tiles : tiles + 5]
    *routed_out, d_gate, d_up, keep_a, send_a, keep_b, send_b = refs[tiles + 5 : -4]
    down_v, gate_v, up_v, loaded = refs[-4:]
    copies = [
        pltpu.make_async_copy(source, target, loaded.at[i])
        for i, (source, target) in enumerate(((down_w, down_v), (gate_w, gate_v), (up_w, up_v)))
    ]

    @pl.when(pl.program_id(0) == 0)
    def _():
        for copy in copies:
            copy.start()
        copies[0].wait()

    d_hidden = 0.0
    for k, tile in enumerate(routed):
        wide = tile.shape[1]
        cols = slice(None)
        if tiles > 1:
            cols = pl.ds(pl.multiple_of(((place[0] + tiles - k) & (tiles - 1)) * wide, wide), wide)
            routed_out[0][:, cols] = tile[...]
        d_hidden = d_hidden + dot(tile[...], down_v[:, cols], NT)

    @pl.when(pl.program_id(0) == 0)
    def _():
        copies[1].wait()
        copies[2].wait()

    to_gate = (d_hidden * slope[...].astype(F32)).astype(BF16)
    to_up = (d_hidden * active[...].astype(F32)).astype(BF16)
    d_gate[...] = to_gate
    d_up[...] = to_up
    half = keep_a.shape[2]
    homes = (
        ((keep_a, 0), (keep_b, 0)),
        ((send_a, 0), (keep_b, 1)),
        ((send_a, 1), (send_b, 1)),
        ((keep_a, 1), (send_b, 0)),
    )
    for k, (home_a, home_b) in enumerate(homes):
        start = pl.multiple_of((place[0] ^ k) * (2 * half), 2 * half)
        cols = pl.ds(start, 2 * half)
        term = dot(to_gate, gate_v[:, cols], NN) + dot(to_up, up_v[:, cols], NN)
        term = term.astype(BF16)
        home_a[0][home_a[1]] = term[:, :half]
        home_b[0][home_b[1]] = term[:, half:]


def expert_cotangents(place, routed, active, slope, down_w, gate_w, up_w):
    rows, wide = routed[0].shape
    tiles = len(routed)
    units, width = down_w.shape
    step = 256
    half = width // 8
    by_row = lambda i, *_: (i, 0)
    pair = pl.BlockSpec((2, step, half), lambda i, *_: (0, i, 0))
    rebuilt = [width] if tiles > 1 else []
    return pl.pallas_call(
        functools.partial(expert_body, tiles=tiles),
        grid_spec=pltpu.PrefetchScalarGridSpec(
            num_scalar_prefetch=1,
            grid=(rows // step,),
            in_specs=[pl.BlockSpec((step, wide), by_row)] * tiles
            + [pl.BlockSpec((step, units), by_row)] * 2
            + [pl.BlockSpec(memory_space=pl.ANY)] * 3,
            out_specs=[pl.BlockSpec((step, w), by_row) for w in rebuilt + [units] * 2]
            + [pair] * 4,
            scratch_shapes=[pltpu.VMEM((units, width), BF16)] * 3
            + [pltpu.SemaphoreType.DMA((3,))],
        ),
        out_shape=[jax.ShapeDtypeStruct((rows, w), BF16) for w in rebuilt + [units] * 2]
        + [jax.ShapeDtypeStruct((2, rows, half), BF16)] * 4,
        compiler_params=limit(56),
    )(place, *routed, active, slope, down_w, gate_w, up_w)


def weight_grads_body(*refs):
    *parts, rows_q, rows_d = refs[: len(refs) - (len(refs) - 2) // 3]
    for i, out in enumerate(refs[len(refs) - len(parts) // 2 :]):
        total = dot(parts[2 * i][...], rows_q[...], TN)
        out[...] = (total + dot(parts[2 * i + 1][...], rows_d[...], TN)).astype(BF16)


def weight_grads(pairs, rows):
    width = rows[0].shape[1]
    units = pairs[0][0].shape[1]
    step = 512
    parts = [part for pair in pairs for part in pair]
    by_col = lambda i: (0, i)
    return pl.pallas_call(
        weight_grads_body,
        grid=(width // step,),
        in_specs=[pl.BlockSpec(part.shape, lambda i: (0, 0)) for part in parts]
        + [pl.BlockSpec((part.shape[0], step), by_col) for part in rows],
        out_specs=[pl.BlockSpec((units, step), by_col)] * len(pairs),
        out_shape=[jax.ShapeDtypeStruct((units, width), BF16)] * len(pairs),
        compiler_params=limit(58),
    )(*parts, *rows)


def swapped(x, flip):
    count = lax.axis_size(TP)
    return lax.ppermute(x, TP, [(i, i ^ flip) for i in range(count)])


def plus(*terms):
    total = terms[0].astype(F32)
    for term in terms[1:]:
        total = total + term.astype(F32)
    return total.astype(BF16)


def final_sum_body(keep_a, got_a, last_a, keep_b, got_b, last_b, out):
    half = keep_a.shape[2]
    for start, keep, got, last in ((0, keep_a, got_a, last_a), (half, keep_b, got_b, last_b)):
        total = keep[0].astype(F32) + got[0].astype(F32) + last[...].astype(F32)
        out[:, start : start + half] = total.astype(BF16)


def final_sum(keep_a, got_a, last_a, keep_b, got_b, last_b):
    _, rows, half = keep_a.shape
    first = pl.BlockSpec((1, rows, half), lambda i: (0, 0, 0))
    whole = pl.BlockSpec((rows, half), lambda i: (0, 0))
    return pl.pallas_call(
        final_sum_body,
        grid=(1,),
        in_specs=[first, first, whole] * 2,
        out_specs=pl.BlockSpec((rows, 2 * half), lambda i: (0, 0)),
        out_shape=jax.ShapeDtypeStruct((rows, 2 * half), BF16),
        compiler_params=limit(12),
    )(keep_a, got_a, last_a, keep_b, got_b, last_b)


def summed_over_tp(keep_a, send_a, keep_b, send_b):
    got_a = swapped(send_a, 1)
    got_b = swapped(send_b, 3)
    last_a, last_b = plus(keep_a[1], got_a[1]), plus(keep_b[1], got_b[1])
    last_a = swapped(last_a, 3)
    last_b = swapped(last_b, 1)
    return final_sum(keep_a, got_a, last_a, keep_b, got_b, last_b)


def shifted(x, axis, by):
    count = lax.axis_size(axis)
    return lax.ppermute(x, axis, [(i, (i + by) % count) for i in range(count)])


def gathered_ring(x):
    half = x.shape[0] // 2
    below = shifted(x, TP, 1)
    above = shifted(x, TP, -1)
    across = jnp.concatenate(
        [shifted(below[:half], TP, 1), shifted(above[half:], TP, -1)], axis=0
    )
    return x, below, above, across


def triangle(reverse):
    row, col = grid_of((BLK, BLK), 0), grid_of((BLK, BLK), 1)
    return jnp.where((row <= col) if reverse else (row >= col), 1.0, 0.0).astype(BF16)


def local_state_body(keys, values, decay, cumulative, ends, gain, produced):
    blocks = gain.shape[0]
    lower = triangle(False)
    for c in range(blocks):
        rows = slice(c * BLK, (c + 1) * BLK)
        cum = dot_exact(lower, decay[rows, :], NN)
        cumulative[rows, :] = cum
        end = cum[BLK - 1 : BLK, :]
        ends[c : c + 1, :] = end
        faded = keys[rows, :].astype(F32) * jnp.exp(end - cum)
        gain[c] = dot_parts((values[rows, :],), halves(faded), TN)
    state = gain[0]
    total = ends[0:1, :]
    for c in range(1, blocks):
        state = state * jnp.exp(ends[c : c + 1, :]) + gain[c]
        total = total + ends[c : c + 1, :]
    width = state.shape[0]
    produced[0:width, :] = state
    spare = produced.shape[0] - width
    produced[width:, :] = jnp.where(grid_of((spare, total.shape[1]), 0) == 0, total, 0.0)


def local_states(keys, values, decay):
    tokens, channels = keys.shape
    width = values.shape[1]
    blocks = tokens // BLK
    return vmem_call(
        local_state_body,
        [
            jax.ShapeDtypeStruct((tokens, channels), F32),
            jax.ShapeDtypeStruct((blocks, channels), F32),
            jax.ShapeDtypeStruct((blocks, width, channels), F32),
            jax.ShapeDtypeStruct((width + 8, channels), F32),
        ],
    )(keys, values, decay)


def forward_body(index, queries, keys, values, cumulative, ends, gain, *refs):
    *pieces, inside_0, inside_1, book_0, book_1, mixed, states, scores, book = refs
    blocks = gain.shape[0]
    far, _, (near, _, _) = opened(pieces, index[0], book)
    own = slice(BOOK_OWN + 1, BOOK_OWN + 2)
    start = inside_0[...] + book_0[own, :] * (inside_1[...] + book_1[own, :] * weighted(far, near))
    scale = queries.shape[1] ** (-0.5)
    causal = grid_of((BLK, BLK), 0) >= grid_of((BLK, BLK), 1)
    state = start
    for c in range(blocks):
        rows = slice(c * BLK, (c + 1) * BLK)
        cum = cumulative[rows, :]
        middle = cum[BLK // 2 - 1 : BLK // 2, :]
        query = queries[rows, :].astype(F32) * scale
        near_q = halves(query * jnp.exp(cum - middle))
        near_k = halves(keys[rows, :].astype(F32) * jnp.exp(middle - cum))
        score = jnp.where(causal, dot_parts(near_q, near_k, NT), 0.0)
        scores[rows, :] = score
        states[c] = state
        out = dot_parts(halves(query * jnp.exp(cum)), halves(state), NT)
        out = out + dot_parts(halves(score), (values[rows, :],), NN)
        mixed[rows, :] = out.astype(BF16)
        state = state * jnp.exp(ends[c : c + 1, :]) + gain[c]
    states[blocks] = state


def forward(queries, keys, values, cumulative, ends, gain, before):
    pieces, index, insides, books = before
    tokens, channels = keys.shape
    width = values.shape[1]
    blocks = tokens // BLK
    operands = (*pieces, *insides, *books)
    return vmem_call(
        forward_body,
        [
            jax.ShapeDtypeStruct((tokens, width), BF16),
            jax.ShapeDtypeStruct((blocks + 1, width, channels), F32),
            jax.ShapeDtypeStruct((tokens, BLK), F32),
            jax.ShapeDtypeStruct((BOOK_ROWS, channels), F32),
        ],
        in_specs=[SMEM] + [VMEM] * (6 + len(operands)),
    )(index, queries, keys, values, cumulative, ends, gain, *operands)


def cotangent_body(place, a, b, c, d, w_out, queries, cumulative, ends, d_mixed, back, own):
    blocks = back.shape[0]
    scale = queries.shape[1] ** (-0.5)
    quarter = a.shape[1]
    total = None
    for tile, offset in ((a, 0), (b, 3), (c, 1), (d, 2)):
        start = pl.multiple_of(((place[0] + offset) & 3) * quarter, quarter)
        term = dot(tile[...], w_out[pl.ds(start, quarter), :], NN)
        total = term if total is None else total + term
    d_mixed[...] = total
    for c in range(blocks):
        rows = slice(c * BLK, (c + 1) * BLK)
        query = queries[rows, :].astype(F32) * (scale * jnp.exp(cumulative[rows, :]))
        back[c] = dot_parts(halves(d_mixed[rows, :]), halves(query), TN)
    state = back[blocks - 1]
    for c in reversed(range(blocks - 1)):
        state = state * jnp.exp(ends[c : c + 1, :]) + back[c]
    own[...] = state.astype(BF16)


def cotangents(place, tiles, w_out, queries, cumulative, ends):
    tokens, channels = queries.shape
    width = w_out.shape[1]
    blocks = tokens // BLK
    return vmem_call(
        cotangent_body,
        [
            jax.ShapeDtypeStruct((tokens, width), F32),
            jax.ShapeDtypeStruct((blocks, width, channels), F32),
            jax.ShapeDtypeStruct((width, channels), BF16),
        ],
        in_specs=[SMEM] + [VMEM] * 8,
    )(place, *tiles, w_out, queries, cumulative, ends)


def projection_body(place, a, b, c, d, mixed, out):
    quarter = a.shape[1]
    for tile, offset in ((a, 0), (b, 3), (c, 1), (d, 2)):
        start = pl.multiple_of(((place[0] + offset) & 3) * quarter, quarter)
        out[pl.ds(start, quarter), :] = dot(tile[...], mixed[...], TN).astype(BF16)


def projection(place, tiles, mixed):
    return vmem_call(
        projection_body,
        jax.ShapeDtypeStruct((4 * tiles[0].shape[1], mixed.shape[1]), BF16),
        in_specs=[SMEM] + [VMEM] * 5,
    )(place, *tiles, mixed)


def inside_body(queries, keys, values, cumulative, scores, d_mixed, to_q, to_k, to_v):
    blocks = queries.shape[0] // BLK
    scale = queries.shape[1] ** (-0.5)
    causal = grid_of((BLK, BLK), 0) >= grid_of((BLK, BLK), 1)
    for c in range(blocks):
        rows = slice(c * BLK, (c + 1) * BLK)
        cum = cumulative[rows, :]
        middle = cum[BLK // 2 - 1 : BLK // 2, :]
        rising, falling = jnp.exp(cum - middle), jnp.exp(middle - cum)
        near_q = halves(queries[rows, :].astype(F32) * scale * rising)
        near_k = halves(keys[rows, :].astype(F32) * falling)
        incoming = halves(d_mixed[rows, :])
        d_score = jnp.where(causal, dot_parts(incoming, (values[rows, :],), NT), 0.0)
        d_score = halves(d_score)
        to_q[rows, :] = rising * dot_parts(d_score, near_k, NN)
        to_k[rows, :] = falling * dot_parts(d_score, near_q, TN)
        to_v[rows, :] = dot_parts(halves(scores[rows, :]), incoming, TN)


def inside_blocks(queries, keys, values, cumulative, scores, d_mixed):
    tokens, channels = queries.shape
    return vmem_call(
        inside_body,
        [
            jax.ShapeDtypeStruct((tokens, channels), F32),
            jax.ShapeDtypeStruct((tokens, channels), F32),
            jax.ShapeDtypeStruct(values.shape, F32),
        ],
    )(queries, keys, values, cumulative, scores, d_mixed)


def backward_body(
    queries, keys, values, cumulative, ends, d_mixed, states, back, to_q, to_k, to_v, *refs
):
    *pieces, inside_0, inside_1, book_0, book_1, book, grad_q, grad_k, grad_v, grad_g = refs
    own = slice(BOOK_OWN, BOOK_OWN + 1)
    later = weighted([x[...] for x in pieces], [book[k : k + 1, :] for k in range(len(pieces))])
    later = inside_0[...] + book_0[own, :] * (inside_1[...] + book_1[own, :] * later)
    blocks = back.shape[0]
    scale = queries.shape[1] ** (-0.5)
    upper = triangle(True)
    after = later
    carry = jnp.sum(after * states[blocks], axis=0, keepdims=True)
    for c in reversed(range(blocks)):
        rows = slice(c * BLK, (c + 1) * BLK)
        cum = cumulative[rows, :]
        end = ends[c : c + 1, :]
        fading = jnp.exp(end - cum)
        key = keys[rows, :].astype(F32)
        after_parts = halves(after)
        d_query = jnp.exp(cum) * dot_parts(halves(d_mixed[rows, :]), halves(states[c]), NN)
        d_query = (d_query + to_q[rows, :]) * scale
        d_key = fading * dot_parts((values[rows, :],), after_parts, NN) + to_k[rows, :]
        d_value = dot_parts(halves(key * fading), after_parts, NT) + to_v[rows, :]
        grad_q[rows, :] = d_query.astype(BF16)
        grad_k[rows, :] = d_key.astype(BF16)
        grad_v[rows, :] = d_value.astype(BF16)
        change = queries[rows, :].astype(F32) * d_query - key * d_key
        summed = dot_exact(upper, change, NN) + carry
        grad_g[rows, :] = summed
        carry = summed[0:1, :]
        after = after * jnp.exp(end) + back[c]


def backward(
    queries, keys, values, cumulative, ends, d_mixed, states, back, inside, after, books
):
    pieces, insides = after
    return vmem_call(
        backward_body,
        [
            jax.ShapeDtypeStruct(queries.shape, BF16),
            jax.ShapeDtypeStruct(keys.shape, BF16),
            jax.ShapeDtypeStruct(values.shape, BF16),
            jax.ShapeDtypeStruct(queries.shape, F32),
        ],
    )(queries, keys, values, cumulative, ends, d_mixed, states, back, *inside, *pieces, *insides, *books)


BOOK_WHOLE, BOOK_OWN, BOOK_ROWS = 8, 16, 24


def stage_weights(logs, index, reverse):
    count = len(logs)
    place = [lax.rem(index - k + count, count) for k in range(count)]
    none = jnp.zeros_like(logs[0])

    def summed(condition):
        total = none
        for log, at in zip(logs, place):
            total = total + jnp.where(condition(at), log, 0.0)
        return total

    if reverse:
        passed = lambda at: at > index
        inner = lambda start: lambda at: (at < start) & (at > index)
        outer = lambda start: lambda at: at < start
    else:
        passed = lambda at: at < index
        inner = lambda start: lambda at: (at > start) & (at < index)
        outer = lambda start: lambda at: at > start
    near = [jnp.where(passed(at), jnp.exp(summed(inner(at))), 0.0) for at in place]
    whole = [jnp.exp(summed(outer(at))) for at in place]
    return near, whole, jnp.exp(summed(passed))


def weighted(pieces, weights):
    total = pieces[0].astype(F32) * weights[0]
    for piece, weight in zip(pieces[1:], weights[1:]):
        total = total + piece.astype(F32) * weight
    return total


def opened(pieces, index, book):
    width = pieces[0].shape[0] - 8
    logs = [piece[width : width + 1, :] for piece in pieces]
    states = [piece[0:width, :] for piece in pieces]
    near, whole, own = stage_weights(logs, index, True)
    for k in range(len(logs)):
        book[k : k + 1, :] = near[k]
        book[BOOK_WHOLE + k : BOOK_WHOLE + k + 1, :] = whole[k]
    book[BOOK_OWN : BOOK_OWN + 1, :] = own
    return states, logs, stage_weights(logs, index, False)


def stage_before_body(index, *refs):
    *pieces, inside, payload, book = refs
    states, logs, (near, whole, own) = opened(pieces, index[0], book)
    width = inside.shape[0]
    book[BOOK_OWN + 1 : BOOK_OWN + 2, :] = own
    inside[...] = weighted(states, near)
    payload[0:width, :] = weighted(states, whole)
    total = logs[0]
    for log in logs[1:]:
        total = total + log
    payload[width:, :] = jnp.where(grid_of((8, total.shape[1]), 0) == 0, total, 0.0)


def stage_after_body(*refs):
    *pieces, book, inside, total = refs
    pieces = [piece[...] for piece in pieces]
    inside[...] = weighted(pieces, [book[k : k + 1, :] for k in range(len(pieces))])
    wholes = [book[BOOK_WHOLE + k : BOOK_WHOLE + k + 1, :] for k in range(len(pieces))]
    total[...] = weighted(pieces, wholes).astype(BF16)


def everyone(x, axis):
    return [x] + [shifted(x, axis, k) for k in range(1, lax.axis_size(axis))]


def states_before(payload):
    rows, channels = payload.shape
    insides, books = [], []
    for axis in reversed(SP):
        pieces = everyone(payload, axis)
        index = lax.axis_index(axis).reshape(1)
        if axis == SP[0]:
            return pieces, index, insides, books
        inside, payload, book = vmem_call(
            stage_before_body,
            [
                jax.ShapeDtypeStruct((rows - 8, channels), F32),
                jax.ShapeDtypeStruct((rows, channels), F32),
                jax.ShapeDtypeStruct((BOOK_ROWS, channels), F32),
            ],
            in_specs=[SMEM] + [VMEM] * len(pieces),
        )(index, *pieces)
        insides.append(inside)
        books.append(book)


def states_after(part, books):
    insides = []
    for axis, book in zip(reversed(SP), books):
        pieces = everyone(part, axis)
        if axis == SP[0]:
            return pieces, insides
        inside, part = vmem_call(
            stage_after_body,
            [jax.ShapeDtypeStruct(part.shape, F32), jax.ShapeDtypeStruct(part.shape, BF16)],
        )(*pieces, book)
        insides.append(inside)


def local(
    d_out,
    route_expert,
    route_weight,
    expert_inputs,
    w_gate,
    w_up,
    w_down,
    w_out,
    queries,
    keys,
    values,
    log_decay,
):
    tok_rows, model_width = d_out.shape
    experts = lax.axis_size(SP)
    capacity = expert_inputs.shape[1] // experts
    cut = PAD * 2
    tail = -(-(capacity - cut) // PAD) * PAD
    slots = experts * (cut + tail)
    quarter = model_width // lax.axis_size(TP)
    place = lax.axis_index(TP).reshape(1)
    chosen, weight = route_expert.T, route_weight.T

    def exchanged(box):
        rows, width = box.shape
        box = box.reshape(experts, rows // experts, width)
        box = lax.all_to_all(box, SP, split_axis=0, concat_axis=0, tiled=True)
        return box.reshape(rows, width)

    outbox_q, ranks = vmem_call(
        functools.partial(route_body, experts=experts, most=cut),
        [
            jax.ShapeDtypeStruct((experts * cut, quarter), BF16),
            jax.ShapeDtypeStruct((2, tok_rows), jnp.int32),
        ],
        mebibytes=58,
        in_specs=[SMEM, pl.BlockSpec(memory_space=pltpu.HBM)] + [VMEM] * 2,
        scratch_shapes=[pltpu.VMEM((tok_rows, quarter), BF16), pltpu.SemaphoreType.DMA(())],
    )(place, d_out, chosen, weight)
    tile = exchanged(outbox_q)
    routed_q = [tile]
    for k in range(1, lax.axis_size(TP)):
        routed_q.append(shifted(tile, TP, k))

    outbox_d, pick = vmem_call(
        functools.partial(refill_body, least=cut, most=capacity, tail=tail),
        [
            jax.ShapeDtypeStruct((experts * tail, model_width), BF16),
            jax.ShapeDtypeStruct((slots, tok_rows), BF16),
        ],
        mebibytes=20,
    )(d_out, chosen, weight, ranks)
    routed_d = exchanged(outbox_d)

    gate_w, up_w, down_w = w_gate[0].T, w_up[0].T, w_down[0]
    rows_q, rows_d, active_q, active_d, slope_q, slope_d, hidden_q, hidden_d = expert_forward(
        expert_inputs[0], gate_w, up_w, experts, capacity, cut, tail
    )

    query, key, value, decay = queries[:, 0], keys[:, 0], values[:, 0], log_decay[:, 0]
    cumulative, ends, gain, produced = local_states(key, value, decay)
    before = states_before(produced)
    mixed, states, scores, book = forward(query, key, value, cumulative, ends, gain, before)
    books = (*before[3], book)

    weights = (down_w, gate_w, up_w)
    routed_q, gate_q, up_q, *parts_q = expert_cotangents(
        place, routed_q, active_q, slope_q, *weights
    )
    gate_d, up_d, *parts_d = expert_cotangents(
        place, (routed_d,), active_d, slope_d, *weights
    )
    summed = jnp.concatenate(
        [
            summed_over_tp(*parts_q).reshape(experts, cut, quarter),
            summed_over_tp(*parts_d).reshape(experts, tail, quarter),
        ],
        axis=1,
    )
    returned = exchanged(summed.reshape(slots, quarter))
    grad_gate, grad_up = weight_grads(((gate_q, gate_d), (up_q, up_d)), (rows_q, rows_d))
    (grad_down,) = weight_grads(((hidden_q, hidden_d),), (routed_q, routed_d))

    own_cols = lax.dynamic_slice_in_dim(d_out, place[0] * quarter, quarter, 1)
    picked = own_cols.astype(F32) + dot(pick, returned, TN)
    tiles = gathered_ring(picked.astype(BF16))

    d_mixed, back, own_term = cotangents(place, tiles, w_out, query, cumulative, ends)
    after = states_after(own_term, books)
    inside = inside_blocks(query, key, value, cumulative, scores, d_mixed)
    grad_q, grad_k, grad_v, grad_g = backward(
        query, key, value, cumulative, ends, d_mixed, states, back, inside, after, books
    )

    proj = projection(place, tiles, mixed).reshape(experts, model_width // experts, -1)
    proj = lax.all_to_all(proj, SP, 0, 0, tiled=True)
    grad_proj = jnp.sum(proj.astype(F32), axis=0)
    return (
        grad_gate.T[None],
        grad_up.T[None],
        grad_down[None],
        grad_proj,
        grad_q[:, None],
        grad_k[:, None],
        grad_v[:, None],
        grad_g[:, None],
    )


def solution(mesh):
    finer = Mesh(mesh.devices.reshape(4, 4, 2, mesh.shape[TP]), (*SP, TP))
    return jax.shard_map(
        local,
        mesh=finer,
        in_specs=(
            P(SP, None),
            P(SP, None),
            P(SP, None),
            P(SP, None, None),
            P(SP, None, TP),
            P(SP, None, TP),
            P(SP, TP, None),
            P(None, TP),
            P(SP, TP, None),
            P(SP, TP, None),
            P(SP, TP, None),
            P(SP, TP, None),
        ),
        out_specs=(
            P(SP, None, TP),
            P(SP, None, TP),
            P(SP, TP, None),
            P(SP, TP),
            P(SP, TP, None),
            P(SP, TP, None),
            P(SP, TP, None),
            P(SP, TP, None),
        ),
        check_vma=False,
    )
```

```python
import functools

import jax
import jax.numpy as jnp
from jax import lax
from jax.experimental import pallas as pl
from jax.experimental.pallas import tpu as pltpu
from jax.sharding import Mesh
from jax.sharding import PartitionSpec as P


BLK = 64
PAD = 8
SP = ("sp_0", "sp_1", "sp_2")
TP = "tp"
F32 = jnp.float32
BF16 = jnp.bfloat16

NN = (((1,), (0,)), ((), ()))
NT = (((1,), (1,)), ((), ()))
TN = (((0,), (0,)), ((), ()))


def dot(a, b, dims):
    return lax.dot_general(a, b, dims, preferred_element_type=F32)


def halves(x):
    high = x.astype(BF16)
    return high, (x - high.astype(F32)).astype(BF16)


def thirds(x):
    high = x.astype(BF16)
    rest = x - high.astype(F32)
    middle = rest.astype(BF16)
    return high, middle, (rest - middle.astype(F32)).astype(BF16)


def dot_parts(a, b, dims):
    out = dot(a[0], b[0], dims)
    if len(a) > 1:
        out = out + dot(a[1], b[0], dims)
    if len(b) > 1:
        out = out + dot(a[0], b[1], dims)
    return out


def dot_exact(mask, x, dims):
    high, middle, low = thirds(x)
    return dot(mask, high, dims) + (dot(mask, middle, dims) + dot(mask, low, dims))


def grid_of(shape, dim):
    return lax.broadcasted_iota(jnp.int32, shape, dim)


SMEM = pl.BlockSpec(memory_space=pltpu.SMEM)
VMEM = pl.BlockSpec(memory_space=pltpu.VMEM)


def limit(mebibytes):
    return pltpu.CompilerParams(vmem_limit_bytes=mebibytes * 1024 * 1024)


def vmem_call(kernel, outs, mebibytes=12, **options):
    return pl.pallas_call(kernel, out_shape=outs, compiler_params=limit(mebibytes), **options)


def fill_outbox(rows, weight, slot_a, slot_b, outbox):
    weights_a = jnp.concatenate(thirds(weight[0:1, :]), axis=0)
    weights_b = jnp.concatenate(thirds(weight[1:2, :]), axis=0)
    step = 256
    for start in range(0, outbox.shape[0], step):
        slot = grid_of((step, rows.shape[0]), 0) + start
        one_a = jnp.where(slot == slot_a, 1.0, 0.0).astype(BF16)
        one_b = jnp.where(slot == slot_b, 1.0, 0.0).astype(BF16)
        factor = dot(one_a, weights_a, NT) + dot(one_b, weights_b, NT)
        factor = jnp.sum(factor, axis=1, keepdims=True)
        outbox[start : start + step, :] = (dot(one_a + one_b, rows, NN) * factor).astype(BF16)


def slots_of(chosen, ranks, least, most, stride):
    inside = (ranks >= least) & (ranks < most)
    return jnp.where(inside, chosen * stride + ranks - least, -1)


def route_body(place, d_out, chosen, weight, outbox, ranks, rows, loaded, *, experts, most):
    tokens, width = rows.shape
    start = pl.multiple_of(place[0] * width, width)
    copy = pltpu.make_async_copy(d_out.at[:, pl.ds(start, width)], rows, loaded)
    copy.start()
    first, second = chosen[0:1, :], chosen[1:2, :]
    ids = grid_of((experts, tokens), 0)
    is_first, is_second = ids == first, ids == second
    named = jnp.where(is_first | is_second, 1.0, 0.0).astype(BF16)
    earlier = jnp.where(
        grid_of((tokens, tokens), 0) < grid_of((tokens, tokens), 1), 1.0, 0.0
    ).astype(BF16)
    before = dot(named, earlier, NN)
    rank_a = jnp.sum(jnp.where(is_first, before, 0.0), axis=0, keepdims=True).astype(jnp.int32)
    rank_b = jnp.sum(jnp.where(is_second, before, 0.0), axis=0, keepdims=True).astype(jnp.int32)
    ranks[0:1, :] = rank_a
    ranks[1:2, :] = rank_b
    slot_a = slots_of(first, rank_a, 0, most, most)
    slot_b = slots_of(second, rank_b, 0, most, most)
    copy.wait()
    fill_outbox(rows[...], weight, slot_a, slot_b, outbox)


def refill_body(d_out, chosen, weight, ranks, outbox, pick, *, least, most, tail):
    first, second = chosen[0:1, :], chosen[1:2, :]
    rank_a, rank_b = ranks[0:1, :], ranks[1:2, :]
    slot_a = slots_of(first, rank_a, least, most, tail)
    slot_b = slots_of(second, rank_b, least, most, tail)
    fill_outbox(d_out[...], weight, slot_a, slot_b, outbox)
    slot_a = first * (least + tail) + rank_a
    slot_b = second * (least + tail) + rank_b
    step = 256
    for start in range(0, pick.shape[0], step):
        slot = grid_of((step, pick.shape[1]), 0) + start
        found = (slot == slot_a) | (slot == slot_b)
        pick[start : start + step, :] = jnp.where(found, 1.0, 0.0).astype(BF16)


def slot_order(group, capacity, cut, tail):
    def placed(rows, stride, width, first):
        row, col = grid_of((rows, group * capacity), 0), grid_of((rows, group * capacity), 1)
        found = row < 0
        for source in range(group):
            start = source * stride
            here = (row >= start) & (row < start + width)
            found = found | (here & (col == row + (source * capacity + first - start)))
        return jnp.where(found, 1.0, 0.0).astype(BF16)

    return placed(group * cut, cut, cut, 0), placed(group * tail, tail, capacity - cut, cut)


def expert_forward_body(inputs, gate_w, up_w, *outs, orders):
    order = jnp.concatenate(slot_order(*orders), axis=0)
    moved = dot(order, inputs[...], NN).astype(BF16)
    split = outs[0].shape[0]
    rows_q, rows_d = outs[0:2]
    rows_q[...] = moved[:split]
    rows_d[...] = moved[split:]
    units = gate_w.shape[0]
    for first in range(0, units, 256):
        cols = slice(first, min(first + 256, units))
        gate = dot(moved, gate_w[cols, :], NT)
        up = dot(moved, up_w[cols, :], NT)
        sigmoid = 1.0 / (1.0 + jnp.exp(-gate))
        silu = gate * sigmoid
        slope = up * sigmoid * (1.0 + gate * (1.0 - sigmoid))
        for i, value in enumerate((silu, slope, silu * up)):
            value = value.astype(BF16)
            outs[2 + 2 * i][:, cols] = value[:split]
            outs[3 + 2 * i][:, cols] = value[split:]


def expert_forward(inputs, gate_w, up_w, experts, capacity, cut, tail):
    group = 8
    width, units = inputs.shape[1], gate_w.shape[0]
    sizes = (group * cut, group * tail)
    by_row = lambda i: (i, 0)
    whole = pl.BlockSpec((units, width), lambda i: (0, 0))
    widths = [width] * 2 + [units] * 6
    return pl.pallas_call(
        functools.partial(expert_forward_body, orders=(group, capacity, cut, tail)),
        grid=(experts // group,),
        in_specs=[pl.BlockSpec((group * capacity, width), by_row), whole, whole],
        out_specs=[pl.BlockSpec((sizes[i % 2], w), by_row) for i, w in enumerate(widths)],
        out_shape=[
            jax.ShapeDtypeStruct((experts // group * sizes[i % 2], w), BF16)
            for i, w in enumerate(widths)
        ],
        compiler_params=limit(56),
    )(inputs, gate_w, up_w)


def expert_body(place, *refs, tiles):
    routed, (active, slope, down_w, gate_w, up_w) = refs[:tiles], refs[tiles : tiles + 5]
    *routed_out, d_gate, d_up, keep_a, send_a, keep_b, send_b = refs[tiles + 5 :]
    d_hidden = 0.0
    for k, tile in enumerate(routed):
        wide = tile.shape[1]
        cols = slice(None)
        if tiles > 1:
            cols = pl.ds(pl.multiple_of(((place[0] + tiles - k) & (tiles - 1)) * wide, wide), wide)
            routed_out[0][:, cols] = tile[...]
        d_hidden = d_hidden + dot(tile[...], down_w[:, cols], NT)

    to_gate = (d_hidden * slope[...].astype(F32)).astype(BF16)
    to_up = (d_hidden * active[...].astype(F32)).astype(BF16)
    d_gate[...] = to_gate
    d_up[...] = to_up
    half = keep_a.shape[2]
    homes = (
        ((keep_a, 0), (keep_b, 0)),
        ((send_a, 0), (keep_b, 1)),
        ((send_a, 1), (send_b, 1)),
        ((keep_a, 1), (send_b, 0)),
    )
    for k, (home_a, home_b) in enumerate(homes):
        start = pl.multiple_of((place[0] ^ k) * (2 * half), 2 * half)
        cols = pl.ds(start, 2 * half)
        term = dot(to_gate, gate_w[:, cols], NN) + dot(to_up, up_w[:, cols], NN)
        term = term.astype(BF16)
        home_a[0][home_a[1]] = term[:, :half]
        home_b[0][home_b[1]] = term[:, half:]


def expert_cotangents(place, routed, active, slope, down_w, gate_w, up_w):
    rows, wide = routed[0].shape
    tiles = len(routed)
    units, width = down_w.shape
    step = 256
    half = width // 8
    by_row = lambda i, *_: (i, 0)
    pair = pl.BlockSpec((2, step, half), lambda i, *_: (0, i, 0))
    rebuilt = [width] if tiles > 1 else []
    return pl.pallas_call(
        functools.partial(expert_body, tiles=tiles),
        grid_spec=pltpu.PrefetchScalarGridSpec(
            num_scalar_prefetch=1,
            grid=(rows // step,),
            in_specs=[pl.BlockSpec((step, wide), by_row)] * tiles
            + [pl.BlockSpec((step, units), by_row)] * 2
            + [VMEM] * 3,
            out_specs=[pl.BlockSpec((step, w), by_row) for w in rebuilt + [units] * 2]
            + [pair] * 4,
        ),
        out_shape=[jax.ShapeDtypeStruct((rows, w), BF16) for w in rebuilt + [units] * 2]
        + [jax.ShapeDtypeStruct((2, rows, half), BF16)] * 4,
        compiler_params=limit(53),
    )(place, *routed, active, slope, down_w, gate_w, up_w)


def weight_grads_body(*refs):
    *parts, rows_q, rows_d = refs[: len(refs) - (len(refs) - 2) // 3]
    for i, out in enumerate(refs[len(refs) - len(parts) // 2 :]):
        total = dot(parts[2 * i][...], rows_q[...], TN)
        out[...] = (total + dot(parts[2 * i + 1][...], rows_d[...], TN)).astype(BF16)


def weight_grads(pairs, rows):
    width = rows[0].shape[1]
    units = pairs[0][0].shape[1]
    step = 512
    parts = [part for pair in pairs for part in pair]
    by_col = lambda i: (0, i)
    return pl.pallas_call(
        weight_grads_body,
        grid=(width // step,),
        in_specs=[pl.BlockSpec(part.shape, lambda i: (0, 0)) for part in parts]
        + [pl.BlockSpec((part.shape[0], step), by_col) for part in rows],
        out_specs=[pl.BlockSpec((units, step), by_col)] * len(pairs),
        out_shape=[jax.ShapeDtypeStruct((units, width), BF16)] * len(pairs),
        compiler_params=limit(58),
    )(*parts, *rows)


def swapped(x, flip):
    count = lax.axis_size(TP)
    return lax.ppermute(x, TP, [(i, i ^ flip) for i in range(count)])


def plus(*terms):
    total = terms[0].astype(F32)
    for term in terms[1:]:
        total = total + term.astype(F32)
    return total.astype(BF16)


def final_sum_body(keep_a, got_a, last_a, keep_b, got_b, last_b, out):
    half = keep_a.shape[2]
    for start, keep, got, last in ((0, keep_a, got_a, last_a), (half, keep_b, got_b, last_b)):
        total = keep[0].astype(F32) + got[0].astype(F32) + last[...].astype(F32)
        out[:, start : start + half] = total.astype(BF16)


def final_sum(keep_a, got_a, last_a, keep_b, got_b, last_b):
    _, rows, half = keep_a.shape
    first = pl.BlockSpec((1, rows, half), lambda i: (0, 0, 0))
    whole = pl.BlockSpec((rows, half), lambda i: (0, 0))
    return pl.pallas_call(
        final_sum_body,
        grid=(1,),
        in_specs=[first, first, whole] * 2,
        out_specs=pl.BlockSpec((rows, 2 * half), lambda i: (0, 0)),
        out_shape=jax.ShapeDtypeStruct((rows, 2 * half), BF16),
        compiler_params=limit(12),
    )(keep_a, got_a, last_a, keep_b, got_b, last_b)


def summed_over_tp(keep_a, send_a, keep_b, send_b):
    got_a = swapped(send_a, 1)
    got_b = swapped(send_b, 3)
    last_a, last_b = plus(keep_a[1], got_a[1]), plus(keep_b[1], got_b[1])
    last_a = swapped(last_a, 3)
    last_b = swapped(last_b, 1)
    return final_sum(keep_a, got_a, last_a, keep_b, got_b, last_b)


def shifted(x, axis, by):
    count = lax.axis_size(axis)
    return lax.ppermute(x, axis, [(i, (i + by) % count) for i in range(count)])


def gathered_ring(x):
    half = x.shape[0] // 2
    below = shifted(x, TP, 1)
    above = shifted(x, TP, -1)
    across = jnp.concatenate(
        [shifted(below[:half], TP, 1), shifted(above[half:], TP, -1)], axis=0
    )
    return x, below, above, across


def triangle(reverse):
    row, col = grid_of((BLK, BLK), 0), grid_of((BLK, BLK), 1)
    return jnp.where((row <= col) if reverse else (row >= col), 1.0, 0.0).astype(BF16)


def local_state_body(keys, values, decay, cumulative, ends, gain, produced):
    blocks = gain.shape[0]
    lower = triangle(False)
    for c in range(blocks):
        rows = slice(c * BLK, (c + 1) * BLK)
        cum = dot_exact(lower, decay[rows, :], NN)
        cumulative[rows, :] = cum
        end = cum[BLK - 1 : BLK, :]
        ends[c : c + 1, :] = end
        faded = keys[rows, :].astype(F32) * jnp.exp(end - cum)
        gain[c] = dot_parts((values[rows, :],), halves(faded), TN)
    state = gain[0]
    total = ends[0:1, :]
    for c in range(1, blocks):
        state = state * jnp.exp(ends[c : c + 1, :]) + gain[c]
        total = total + ends[c : c + 1, :]
    width = state.shape[0]
    produced[0:width, :] = state
    spare = produced.shape[0] - width
    produced[width:, :] = jnp.where(grid_of((spare, total.shape[1]), 0) == 0, total, 0.0)


def local_states(keys, values, decay):
    tokens, channels = keys.shape
    width = values.shape[1]
    blocks = tokens // BLK
    return vmem_call(
        local_state_body,
        [
            jax.ShapeDtypeStruct((tokens, channels), F32),
            jax.ShapeDtypeStruct((blocks, channels), F32),
            jax.ShapeDtypeStruct((blocks, width, channels), F32),
            jax.ShapeDtypeStruct((width + 8, channels), F32),
        ],
    )(keys, values, decay)


def forward_body(index, queries, keys, values, cumulative, ends, gain, *refs):
    *pieces, inside_0, inside_1, book_0, book_1, mixed, states, scores, book = refs
    blocks = gain.shape[0]
    far, _, (near, _, _) = opened(pieces, index[0], book)
    own = slice(BOOK_OWN + 1, BOOK_OWN + 2)
    start = inside_0[...] + book_0[own, :] * (inside_1[...] + book_1[own, :] * weighted(far, near))
    scale = queries.shape[1] ** (-0.5)
    causal = grid_of((BLK, BLK), 0) >= grid_of((BLK, BLK), 1)
    state = start
    for c in range(blocks):
        rows = slice(c * BLK, (c + 1) * BLK)
        cum = cumulative[rows, :]
        middle = cum[BLK // 2 - 1 : BLK // 2, :]
        query = queries[rows, :].astype(F32) * scale
        near_q = halves(query * jnp.exp(cum - middle))
        near_k = halves(keys[rows, :].astype(F32) * jnp.exp(middle - cum))
        score = jnp.where(causal, dot_parts(near_q, near_k, NT), 0.0)
        scores[rows, :] = score
        states[c] = state
        out = dot_parts(halves(query * jnp.exp(cum)), halves(state), NT)
        out = out + dot_parts(halves(score), (values[rows, :],), NN)
        mixed[rows, :] = out.astype(BF16)
        state = state * jnp.exp(ends[c : c + 1, :]) + gain[c]
    states[blocks] = state


def forward(queries, keys, values, cumulative, ends, gain, before):
    pieces, index, insides, books = before
    tokens, channels = keys.shape
    width = values.shape[1]
    blocks = tokens // BLK
    operands = (*pieces, *insides, *books)
    return vmem_call(
        forward_body,
        [
            jax.ShapeDtypeStruct((tokens, width), BF16),
            jax.ShapeDtypeStruct((blocks + 1, width, channels), F32),
            jax.ShapeDtypeStruct((tokens, BLK), F32),
            jax.ShapeDtypeStruct((BOOK_ROWS, channels), F32),
        ],
        in_specs=[SMEM] + [VMEM] * (6 + len(operands)),
    )(index, queries, keys, values, cumulative, ends, gain, *operands)


def cotangent_body(place, a, b, c, d, w_out, queries, cumulative, ends, d_mixed, back, own):
    blocks = back.shape[0]
    scale = queries.shape[1] ** (-0.5)
    quarter = a.shape[1]
    total = None
    for tile, offset in ((a, 0), (b, 3), (c, 1), (d, 2)):
        start = pl.multiple_of(((place[0] + offset) & 3) * quarter, quarter)
        term = dot(tile[...], w_out[pl.ds(start, quarter), :], NN)
        total = term if total is None else total + term
    d_mixed[...] = total
    for c in range(blocks):
        rows = slice(c * BLK, (c + 1) * BLK)
        query = queries[rows, :].astype(F32) * (scale * jnp.exp(cumulative[rows, :]))
        back[c] = dot_parts(halves(d_mixed[rows, :]), halves(query), TN)
    state = back[blocks - 1]
    for c in reversed(range(blocks - 1)):
        state = state * jnp.exp(ends[c : c + 1, :]) + back[c]
    own[...] = state.astype(BF16)


def cotangents(place, tiles, w_out, queries, cumulative, ends):
    tokens, channels = queries.shape
    width = w_out.shape[1]
    blocks = tokens // BLK
    return vmem_call(
        cotangent_body,
        [
            jax.ShapeDtypeStruct((tokens, width), F32),
            jax.ShapeDtypeStruct((blocks, width, channels), F32),
            jax.ShapeDtypeStruct((width, channels), BF16),
        ],
        in_specs=[SMEM] + [VMEM] * 8,
    )(place, *tiles, w_out, queries, cumulative, ends)


def projection_body(place, a, b, c, d, mixed, out):
    quarter = a.shape[1]
    for tile, offset in ((a, 0), (b, 3), (c, 1), (d, 2)):
        start = pl.multiple_of(((place[0] + offset) & 3) * quarter, quarter)
        out[pl.ds(start, quarter), :] = dot(tile[...], mixed[...], TN).astype(BF16)


def projection(place, tiles, mixed):
    return vmem_call(
        projection_body,
        jax.ShapeDtypeStruct((4 * tiles[0].shape[1], mixed.shape[1]), BF16),
        in_specs=[SMEM] + [VMEM] * 5,
    )(place, *tiles, mixed)


def inside_body(queries, keys, values, cumulative, scores, d_mixed, to_q, to_k, to_v):
    blocks = queries.shape[0] // BLK
    scale = queries.shape[1] ** (-0.5)
    causal = grid_of((BLK, BLK), 0) >= grid_of((BLK, BLK), 1)
    for c in range(blocks):
        rows = slice(c * BLK, (c + 1) * BLK)
        cum = cumulative[rows, :]
        middle = cum[BLK // 2 - 1 : BLK // 2, :]
        rising, falling = jnp.exp(cum - middle), jnp.exp(middle - cum)
        near_q = halves(queries[rows, :].astype(F32) * scale * rising)
        near_k = halves(keys[rows, :].astype(F32) * falling)
        incoming = halves(d_mixed[rows, :])
        d_score = jnp.where(causal, dot_parts(incoming, (values[rows, :],), NT), 0.0)
        d_score = halves(d_score)
        to_q[rows, :] = rising * dot_parts(d_score, near_k, NN)
        to_k[rows, :] = falling * dot_parts(d_score, near_q, TN)
        to_v[rows, :] = dot_parts(halves(scores[rows, :]), incoming, TN)


def inside_blocks(queries, keys, values, cumulative, scores, d_mixed):
    tokens, channels = queries.shape
    return vmem_call(
        inside_body,
        [
            jax.ShapeDtypeStruct((tokens, channels), F32),
            jax.ShapeDtypeStruct((tokens, channels), F32),
            jax.ShapeDtypeStruct(values.shape, F32),
        ],
    )(queries, keys, values, cumulative, scores, d_mixed)


def backward_body(
    queries, keys, values, cumulative, ends, d_mixed, states, back, to_q, to_k, to_v, *refs
):
    *pieces, inside_0, inside_1, book_0, book_1, book, grad_q, grad_k, grad_v, grad_g = refs
    own = slice(BOOK_OWN, BOOK_OWN + 1)
    later = weighted([x[...] for x in pieces], [book[k : k + 1, :] for k in range(len(pieces))])
    later = inside_0[...] + book_0[own, :] * (inside_1[...] + book_1[own, :] * later)
    blocks = back.shape[0]
    scale = queries.shape[1] ** (-0.5)
    upper = triangle(True)
    after = later
    carry = jnp.sum(after * states[blocks], axis=0, keepdims=True)
    for c in reversed(range(blocks)):
        rows = slice(c * BLK, (c + 1) * BLK)
        cum = cumulative[rows, :]
        end = ends[c : c + 1, :]
        fading = jnp.exp(end - cum)
        key = keys[rows, :].astype(F32)
        after_parts = halves(after)
        d_query = jnp.exp(cum) * dot_parts(halves(d_mixed[rows, :]), halves(states[c]), NN)
        d_query = (d_query + to_q[rows, :]) * scale
        d_key = fading * dot_parts((values[rows, :],), after_parts, NN) + to_k[rows, :]
        d_value = dot_parts(halves(key * fading), after_parts, NT) + to_v[rows, :]
        grad_q[rows, :] = d_query.astype(BF16)
        grad_k[rows, :] = d_key.astype(BF16)
        grad_v[rows, :] = d_value.astype(BF16)
        change = queries[rows, :].astype(F32) * d_query - key * d_key
        summed = dot_exact(upper, change, NN) + carry
        grad_g[rows, :] = summed
        carry = summed[0:1, :]
        after = after * jnp.exp(end) + back[c]


def backward(
    queries, keys, values, cumulative, ends, d_mixed, states, back, inside, after, books
):
    pieces, insides = after
    return vmem_call(
        backward_body,
        [
            jax.ShapeDtypeStruct(queries.shape, BF16),
            jax.ShapeDtypeStruct(keys.shape, BF16),
            jax.ShapeDtypeStruct(values.shape, BF16),
            jax.ShapeDtypeStruct(queries.shape, F32),
        ],
    )(queries, keys, values, cumulative, ends, d_mixed, states, back, *inside, *pieces, *insides, *books)


BOOK_WHOLE, BOOK_OWN, BOOK_ROWS = 8, 16, 24


def stage_weights(logs, index, reverse):
    count = len(logs)
    place = [lax.rem(index - k + count, count) for k in range(count)]
    none = jnp.zeros_like(logs[0])

    def summed(condition):
        total = none
        for log, at in zip(logs, place):
            total = total + jnp.where(condition(at), log, 0.0)
        return total

    if reverse:
        passed = lambda at: at > index
        inner = lambda start: lambda at: (at < start) & (at > index)
        outer = lambda start: lambda at: at < start
    else:
        passed = lambda at: at < index
        inner = lambda start: lambda at: (at > start) & (at < index)
        outer = lambda start: lambda at: at > start
    near = [jnp.where(passed(at), jnp.exp(summed(inner(at))), 0.0) for at in place]
    whole = [jnp.exp(summed(outer(at))) for at in place]
    return near, whole, jnp.exp(summed(passed))


def weighted(pieces, weights):
    total = pieces[0].astype(F32) * weights[0]
    for piece, weight in zip(pieces[1:], weights[1:]):
        total = total + piece.astype(F32) * weight
    return total


def opened(pieces, index, book):
    width = pieces[0].shape[0] - 8
    logs = [piece[width : width + 1, :] for piece in pieces]
    states = [piece[0:width, :] for piece in pieces]
    near, whole, own = stage_weights(logs, index, True)
    for k in range(len(logs)):
        book[k : k + 1, :] = near[k]
        book[BOOK_WHOLE + k : BOOK_WHOLE + k + 1, :] = whole[k]
    book[BOOK_OWN : BOOK_OWN + 1, :] = own
    return states, logs, stage_weights(logs, index, False)


def stage_before_body(index, *refs):
    *pieces, inside, payload, book = refs
    states, logs, (near, whole, own) = opened(pieces, index[0], book)
    width = inside.shape[0]
    book[BOOK_OWN + 1 : BOOK_OWN + 2, :] = own
    inside[...] = weighted(states, near)
    payload[0:width, :] = weighted(states, whole)
    total = logs[0]
    for log in logs[1:]:
        total = total + log
    payload[width:, :] = jnp.where(grid_of((8, total.shape[1]), 0) == 0, total, 0.0)


def stage_after_body(*refs):
    *pieces, book, inside, total = refs
    pieces = [piece[...] for piece in pieces]
    inside[...] = weighted(pieces, [book[k : k + 1, :] for k in range(len(pieces))])
    wholes = [book[BOOK_WHOLE + k : BOOK_WHOLE + k + 1, :] for k in range(len(pieces))]
    total[...] = weighted(pieces, wholes).astype(BF16)


def everyone(x, axis):
    return [x] + [shifted(x, axis, k) for k in range(1, lax.axis_size(axis))]


def states_before(payload):
    rows, channels = payload.shape
    insides, books = [], []
    for axis in reversed(SP):
        pieces = everyone(payload, axis)
        index = lax.axis_index(axis).reshape(1)
        if axis == SP[0]:
            return pieces, index, insides, books
        inside, payload, book = vmem_call(
            stage_before_body,
            [
                jax.ShapeDtypeStruct((rows - 8, channels), F32),
                jax.ShapeDtypeStruct((rows, channels), F32),
                jax.ShapeDtypeStruct((BOOK_ROWS, channels), F32),
            ],
            in_specs=[SMEM] + [VMEM] * len(pieces),
        )(index, *pieces)
        insides.append(inside)
        books.append(book)


def states_after(part, books):
    insides = []
    for axis, book in zip(reversed(SP), books):
        pieces = everyone(part, axis)
        if axis == SP[0]:
            return pieces, insides
        inside, part = vmem_call(
            stage_after_body,
            [jax.ShapeDtypeStruct(part.shape, F32), jax.ShapeDtypeStruct(part.shape, BF16)],
        )(*pieces, book)
        insides.append(inside)


def local(
    d_out,
    route_expert,
    route_weight,
    expert_inputs,
    w_gate,
    w_up,
    w_down,
    w_out,
    queries,
    keys,
    values,
    log_decay,
):
    tok_rows, model_width = d_out.shape
    experts = lax.axis_size(SP)
    capacity = expert_inputs.shape[1] // experts
    cut = PAD * 2
    tail = -(-(capacity - cut) // PAD) * PAD
    slots = experts * (cut + tail)
    quarter = model_width // lax.axis_size(TP)
    place = lax.axis_index(TP).reshape(1)
    chosen, weight = route_expert.T, route_weight.T

    def exchanged(box):
        rows, width = box.shape
        box = box.reshape(experts, rows // experts, width)
        box = lax.all_to_all(box, SP, split_axis=0, concat_axis=0, tiled=True)
        return box.reshape(rows, width)

    outbox_q, ranks = vmem_call(
        functools.partial(route_body, experts=experts, most=cut),
        [
            jax.ShapeDtypeStruct((experts * cut, quarter), BF16),
            jax.ShapeDtypeStruct((2, tok_rows), jnp.int32),
        ],
        mebibytes=58,
        in_specs=[SMEM, pl.BlockSpec(memory_space=pltpu.HBM)] + [VMEM] * 2,
        scratch_shapes=[pltpu.VMEM((tok_rows, quarter), BF16), pltpu.SemaphoreType.DMA(())],
    )(place, d_out, chosen, weight)
    tile = exchanged(outbox_q)
    routed_q = [tile]
    for k in range(1, lax.axis_size(TP)):
        routed_q.append(shifted(tile, TP, k))

    outbox_d, pick = vmem_call(
        functools.partial(refill_body, least=cut, most=capacity, tail=tail),
        [
            jax.ShapeDtypeStruct((experts * tail, model_width), BF16),
            jax.ShapeDtypeStruct((slots, tok_rows), BF16),
        ],
        mebibytes=20,
    )(d_out, chosen, weight, ranks)
    routed_d = exchanged(outbox_d)

    gate_w, up_w, down_w = w_gate[0].T, w_up[0].T, w_down[0]
    rows_q, rows_d, active_q, active_d, slope_q, slope_d, hidden_q, hidden_d = expert_forward(
        expert_inputs[0], gate_w, up_w, experts, capacity, cut, tail
    )

    query, key, value, decay = queries[:, 0], keys[:, 0], values[:, 0], log_decay[:, 0]
    cumulative, ends, gain, produced = local_states(key, value, decay)
    before = states_before(produced)
    mixed, states, scores, book = forward(query, key, value, cumulative, ends, gain, before)
    books = (*before[3], book)

    weights = (down_w, gate_w, up_w)
    routed_q, gate_q, up_q, *parts_q = expert_cotangents(
        place, routed_q, active_q, slope_q, *weights
    )
    gate_d, up_d, *parts_d = expert_cotangents(
        place, (routed_d,), active_d, slope_d, *weights
    )
    summed = jnp.concatenate(
        [
            summed_over_tp(*parts_q).reshape(experts, cut, quarter),
            summed_over_tp(*parts_d).reshape(experts, tail, quarter),
        ],
        axis=1,
    )
    returned = exchanged(summed.reshape(slots, quarter))
    grad_gate, grad_up = weight_grads(((gate_q, gate_d), (up_q, up_d)), (rows_q, rows_d))
    (grad_down,) = weight_grads(((hidden_q, hidden_d),), (routed_q, routed_d))

    own_cols = lax.dynamic_slice_in_dim(d_out, place[0] * quarter, quarter, 1)
    picked = own_cols.astype(F32) + dot(pick, returned, TN)
    tiles = gathered_ring(picked.astype(BF16))

    d_mixed, back, own_term = cotangents(place, tiles, w_out, query, cumulative, ends)
    after = states_after(own_term, books)
    inside = inside_blocks(query, key, value, cumulative, scores, d_mixed)
    grad_q, grad_k, grad_v, grad_g = backward(
        query, key, value, cumulative, ends, d_mixed, states, back, inside, after, books
    )

    proj = projection(place, tiles, mixed).reshape(experts, model_width // experts, -1)
    proj = lax.all_to_all(proj, SP, 0, 0, tiled=True)
    grad_proj = jnp.sum(proj.astype(F32), axis=0)
    return (
        grad_gate.T[None],
        grad_up.T[None],
        grad_down[None],
        grad_proj,
        grad_q[:, None],
        grad_k[:, None],
        grad_v[:, None],
        grad_g[:, None],
    )


def solution(mesh):
    finer = Mesh(mesh.devices.reshape(4, 4, 2, mesh.shape[TP]), (*SP, TP))
    return jax.shard_map(
        local,
        mesh=finer,
        in_specs=(
            P(SP, None),
            P(SP, None),
            P(SP, None),
            P(SP, None, None),
            P(SP, None, TP),
            P(SP, None, TP),
            P(SP, TP, None),
            P(None, TP),
            P(SP, TP, None),
            P(SP, TP, None),
            P(SP, TP, None),
            P(SP, TP, None),
        ),
        out_specs=(
            P(SP, None, TP),
            P(SP, None, TP),
            P(SP, TP, None),
            P(SP, TP),
            P(SP, TP, None),
            P(SP, TP, None),
            P(SP, TP, None),
            P(SP, TP, None),
        ),
        check_vma=False,
    )
```
